32 devices in a mesh: sp: 8 (over z, x), tp: 4 (over y, core).
Axes of the slice: x: 2, y: 2, z: 4, core: 2. Of those that a mesh axis runs over, the one named last changes fastest.
Arguments:
- residual: bfloat16 [4096, 2048], P(('sp', 'tp')), may hold values from -6 to 6
- conv_value: bfloat16 [4096, 1024], P('sp', 'tp'), may hold values from -6 to 6
- conv_gate: bfloat16 [4096, 1024], P('sp', 'tp'), may hold values from -9 to 9
- segments: int32 [4096], P('sp'), may hold values from 0 to 3, never falling along the last dimension, each value on 1 to 2048 neighbouring positions
- conv_weight: float32 [31, 1024], P(None, 'tp'), may hold values from -1 to 1
- norm_gain: float32 [1024], P('tp'), may hold values from 0.1 to 1.9
- norm_shift: float32 [1024], P('tp'), may hold values from -3 to 3
- out_weight: bfloat16 [1024, 2048], replicated, may hold values from -0.1875 to 0.1875
- ffn_gain: float32 [2048], replicated, may hold values from 0.1 to 1.9
- routes: int32 [4096, 2], P('sp'), may hold values from 0 to 7, all different within a row; in each aligned block of 128 rows (0 to 127, 128 to 255, ...) at most 64 rows name the same one
- route_weights: float32 [4096, 2], P('sp'), may hold values from 0.2 to 1
- w_gate: bfloat16 [8, 2048, 1024], P('sp', None, 'tp'), may hold values from -0.125 to 0.125
- w_up: bfloat16 [8, 2048, 1024], P('sp', None, 'tp'), may hold values from -0.125 to 0.125
- w_down: bfloat16 [8, 1024, 2048], P('sp', 'tp'), may hold values from -0.1875 to 0.1875
Outputs:
- layer_out: bfloat16 [4096, 2048], P(('sp', 'tp'))
The draws below stay inside these ranges and needn't reach their ends.
Inputs may be any that keep to these rules, and one draw needn't show every extreme that they name: `routes`: within the rows of one device (aligned blocks of 512 / 4 rows), no expert is named more than 64 times; the two experts of a row differ. `segments`: document numbers never fall along the sequence.
All inputs are finite; a program needn't handle non-finite values.
Results may differ from the reference program's by a relative error of at most 0.007.
Values may be sent and summed in bfloat16 or wider, within the bound.
A program may use at most 128 MiB of HBM per device.

```python
import math
import jax
import jax.numpy as jnp
import numpy as np
from jax import lax

D = 2048
DC = 1024
FF = 1024
CONV_WIDTH = 31
CONV_GROUPS = 8
TOPK = 2
TOK_DEV = 512
TOKENS = 4096
EXPERTS = 8
CAP = 64
N_SP = 8
N_TP = 4


def steps_of(stream_key, shape, cuts, low, largest):
    level = 1.0
    for dim, shards_of in cuts:
        heights = jax.random.uniform(jax.random.fold_in(jax.random.fold_in(stream_key, 6), dim), (shards_of,), jnp.float32, low / len(cuts), largest / len(cuts))
        level = level * jnp.repeat(jnp.exp(heights), shape[dim] // shards_of).reshape((-1,) + (1,) * (len(shape) - 1 - dim))
    return level


def profile(amount, total, bound, slope):
    weights = [(1 << 20) // math.isqrt(grade ** slope) + 1 for grade in range(2, amount + 1)]
    spare, given = total - bound - (amount - 1), [1] * (amount - 1)
    while spare > 0:
        candidates = [i for i in range(amount - 1) if given[i] < bound]
        pool, left = sum([weights[i] for i in candidates]), spare
        for i in candidates:
            more = min(bound - given[i], max(1, left * weights[i] // pool), spare)
            given[i] = given[i] + more
            spare = spare - more
    return np.array([bound] + given)


def uneven(key, number_of, total, most, lean):
    if number_of == 2:
        one = jax.random.randint(key, (), max(1, total - most), min(most, total - 1) + 1)
        return jnp.stack([one, total - one])
    sizes = jnp.asarray(profile(number_of, total, most, lean), jnp.int32)
    couples = (number_of - 1) // 2
    donor, sink = sizes[1:1 + 2 * couples:2], sizes[2:2 + 2 * couples:2]
    margin = jnp.minimum(donor - 1, most - sink)
    shifted = jax.random.randint(jax.random.fold_in(key, 1), (couples,), 0, 1 << 20) % (margin + 1)
    sizes = sizes.at[1:1 + 2 * couples:2].set(donor - shifted).at[2:2 + 2 * couples:2].set(sink + shifted)
    return sizes[jax.random.permutation(jax.random.fold_in(key, 2), number_of)]


def assign_block(key, own, number, rows, count, top, most, lean):
    sequence = jax.random.permutation(key, count)
    crowded, usual = portions_of(count, rows * top, most, lean, True), portions_of(count, rows * top, most, lean, False)
    places = jnp.arange(count)

    def named(tallies, turn):
        used = int((tallies > 0).sum())
        fixed = max(1, used // 4)
        passed = fixed + (places - fixed + turn * (used - fixed)) % max(1, count - fixed)
        return jnp.zeros((count,), jnp.int32).at[sequence[jnp.where(places < fixed, places, passed)]].set(jnp.asarray(tallies, jnp.int32))

    tallies = jnp.where(number % 4 == 0, named(crowded, number // 4), named(usual, number - number // 4 - 1))
    mixed = jax.random.permutation(jax.random.fold_in(own, 3), count)
    donor, taker = mixed[0:count // 2 * 2:2], mixed[1:count // 2 * 2:2]
    slack = jnp.minimum(tallies[donor] - 1, most - tallies[taker]) // 2
    slack = jnp.where((donor == sequence[0]) | (taker == sequence[0]) | (tallies[taker] == 0), 0, jnp.maximum(slack, 0))
    passed = jax.random.randint(jax.random.fold_in(own, 4), (count // 2,), 0, 1 << 20) % (slack + 1)
    tallies = tallies.at[donor].add(-passed).at[taker].add(passed)
    items = jnp.searchsorted(jnp.cumsum(tallies), jnp.arange(rows * top), side="right").astype(jnp.int32)
    table = items.reshape(top, rows).T
    table = table[jax.random.permutation(jax.random.fold_in(own, 1), rows)]
    turn = jax.random.randint(jax.random.fold_in(own, 2), (rows, 1), 0, top)
    return jnp.take_along_axis(table, (jnp.arange(top)[None, :] + turn) % top, axis=1)


def portions_of(count, total, limit, slope, full):
    loads = [(1 << 20) // math.isqrt(standing ** slope) + 1 for standing in range(1, count + 1)]
    largest = limit if full else min(limit, max(-(-total // count), total * loads[0] // sum(loads)))
    least = 1 if total - largest >= count - 1 else 0
    holding, rest = [largest] + [least] * (count - 1), total - largest - least * (count - 1)
    while rest > 0:
        movable = [i for i in range(1, count) if holding[i] < largest] or [i for i in range(1, count) if holding[i] < limit]
        pool, budget = sum([loads[i] for i in movable]), rest
        for i in movable:
            addition = min(limit - holding[i], max(1, budget * loads[i] // pool), rest)
            holding[i] = holding[i] + addition
            rest = rest - addition
    return np.array(holding)


def gaussian(stream_key, extent, scale, most, cuts=(), kind=jnp.bfloat16):
    result = scale * jax.random.normal(stream_key, extent, jnp.float32)
    if cuts:
        result = result * steps_of(stream_key, extent, cuts, -0.22, 0.18)
    return jnp.clip(result, -most, most).astype(kind)


def setup_inputs(seed: int = 0) -> dict:
    arg_keys = jax.random.split(jax.random.key(seed), 15)
    residual = gaussian(arg_keys[0], (TOKENS, D), 1.0, 6.0, ((0, 32),))
    conv_value = gaussian(arg_keys[1], (TOKENS, DC), 1.0, 6.0, ((0, 8), (1, 4)))
    conv_gate = gaussian(arg_keys[2], (TOKENS, DC), 1.5, 9.0, ((0, 8), (1, 4)))
    segments = jnp.searchsorted(jnp.cumsum(uneven(arg_keys[3], N_SP // 2, TOKENS, 4 * TOK_DEV, 0)), jnp.arange(TOKENS), side="right").astype(jnp.int32)
    conv_weight = gaussian(arg_keys[4], (CONV_WIDTH, DC), CONV_WIDTH ** -0.5, 1.0, ((1, 4),), jnp.float32)
    norm_gain = jnp.clip(1.0 + 0.18 * jax.random.normal(arg_keys[5], (DC,), jnp.float32), 0.1, 1.9)
    norm_shift = gaussian(arg_keys[6], (DC,), 0.5, 3.0, ((0, 4),), jnp.float32)
    out_weight = gaussian(arg_keys[7], (DC, D), DC ** -0.5, 0.1875)
    ffn_gain = jnp.clip(1.0 + 0.18 * jax.random.normal(arg_keys[8], (D,), jnp.float32), 0.1, 1.9)
    routes_keys = jax.random.split(jax.random.fold_in(arg_keys[9], 1), TOKENS // (TOK_DEV // N_TP))
    routes_turns = jax.random.permutation(jax.random.fold_in(arg_keys[9], 3), TOKENS // (TOK_DEV // N_TP))
    routes = jax.vmap(lambda own, number: assign_block(jax.random.fold_in(arg_keys[9], 2), own, number, TOK_DEV // N_TP, EXPERTS, TOPK, CAP, 2))(routes_keys, routes_turns).reshape((TOKENS, TOPK))
    route_weights = jnp.clip(0.2 + 0.8 * jax.random.uniform(arg_keys[10], (TOKENS, TOPK), jnp.float32) ** steps_of(arg_keys[10], (TOKENS, TOPK), ((0, 8),), -0.2, 0.2), 0.2, 1.0)
    w_gate = gaussian(arg_keys[11], (EXPERTS, D, FF), D ** -0.5, 0.125, ((0, 8), (2, 4)))
    w_up = gaussian(arg_keys[12], (EXPERTS, D, FF), D ** -0.5, 0.125, ((0, 8), (2, 4)))
    w_down = gaussian(arg_keys[13], (EXPERTS, FF, D), FF ** -0.5, 0.1875, ((0, 8), (1, 4)))
    return dict(residual=residual, conv_value=conv_value, conv_gate=conv_gate, segments=segments, conv_weight=conv_weight, norm_gain=norm_gain, norm_shift=norm_shift, out_weight=out_weight, ffn_gain=ffn_gain, routes=routes, route_weights=route_weights, w_gate=w_gate, w_up=w_up, w_down=w_down)


def reference(residual, conv_value, conv_gate, segments, conv_weight, norm_gain, norm_shift, out_weight, ffn_gain, routes, route_weights, w_gate, w_up, w_down):
    gated = (conv_value.astype(jnp.float32) * jax.nn.sigmoid(conv_gate.astype(jnp.float32))).astype(jnp.bfloat16)
    reach = CONV_WIDTH - 1
    padded = jnp.concatenate([jnp.zeros((reach, DC), jnp.bfloat16), gated], 0).astype(jnp.float32)
    seg_padded = jnp.concatenate([jnp.full((reach,), -1, jnp.int32), segments.astype(jnp.int32)], 0)
    convolved = jnp.zeros((TOKENS, DC), jnp.float32)
    for offset in range(CONV_WIDTH):
        same_doc = (seg_padded[offset:offset + TOKENS] == segments)[:, None]
        convolved = convolved + jnp.where(same_doc, padded[offset:offset + TOKENS] * conv_weight[offset], 0.0)
    grouped = convolved.reshape(TOKENS, CONV_GROUPS, DC // CONV_GROUPS)
    group_mean = lax.optimization_barrier(jnp.mean(grouped, axis=-1, keepdims=True))
    group_var = lax.optimization_barrier(jnp.mean(jnp.square(grouped - group_mean), axis=-1, keepdims=True))
    scaled = ((grouped - group_mean) * lax.rsqrt(group_var + 1e-05)).reshape(TOKENS, DC) * norm_gain + norm_shift
    conv_out = jax.nn.silu(scaled).astype(jnp.bfloat16)
    mixed = jnp.dot(conv_out, out_weight, preferred_element_type=jnp.float32).astype(jnp.bfloat16)
    stream = residual.astype(jnp.float32) + lax.optimization_barrier(mixed).astype(jnp.float32)
    normed = (stream * lax.rsqrt(lax.optimization_barrier(jnp.mean(stream * stream, axis=-1, keepdims=True)) + 1e-06) * ffn_gain).astype(jnp.bfloat16)
    rows_dev = TOK_DEV // N_TP
    blocks = TOKENS // rows_dev
    route_pairs = routes.reshape(blocks, rows_dev * TOPK)
    onehot = (route_pairs[..., None] == jnp.arange(EXPERTS, dtype=jnp.int32)).astype(jnp.int32)
    slot_rank = lax.optimization_barrier(jnp.sum((jnp.cumsum(onehot, axis=1) - onehot) * onehot, axis=2)).reshape(TOKENS, TOPK)
    token_id = jnp.broadcast_to(jnp.arange(TOKENS, dtype=jnp.int32)[:, None], (TOKENS, TOPK))
    block_id = token_id // rows_dev
    owners = jnp.full((EXPERTS, blocks, CAP), TOKENS, jnp.int32).at[routes, block_id, slot_rank].set(token_id)
    weight_table = jnp.zeros((EXPERTS, blocks, CAP), jnp.float32).at[routes, block_id, slot_rank].set(route_weights)
    rows_pad = jnp.concatenate([normed, jnp.zeros((1, D), jnp.bfloat16)], 0)

    def one_expert(totals, inputs):
        gate_w, up_w, down_w, expert_owners, expert_weights = inputs
        row_index = expert_owners.reshape(-1)
        picked = rows_pad[row_index]
        gate_act = jnp.dot(picked, gate_w, preferred_element_type=jnp.float32)
        up_act = jnp.dot(picked, up_w, preferred_element_type=jnp.float32)
        hidden = (jax.nn.silu(gate_act) * up_act).astype(jnp.bfloat16)
        summed = jnp.dot(hidden, down_w, preferred_element_type=jnp.float32)
        expert_out = lax.optimization_barrier(summed.astype(jnp.bfloat16)).astype(jnp.float32)
        totals = totals.at[row_index].add(expert_weights.reshape(-1)[:, None] * expert_out)
        return (totals, None)
    totals, _ = lax.scan(one_expert, jnp.zeros((TOKENS + 1, D), jnp.float32), (w_gate, w_up, w_down, owners, weight_table))
    return (stream + totals[:TOKENS]).astype(jnp.bfloat16)
```

```python
import functools

import jax
import jax.numpy as jnp
from jax import lax
from jax.experimental import pallas as pl
from jax.experimental.pallas import tpu as pltpu
from jax.sharding import PartitionSpec as P

DC = 1024
CONV_GROUPS = 8
MESH = pl.DeviceIdType.MESH
RIM = 32


def passed_along(value, axis, steps):
    count = lax.axis_size(axis)
    initial, last = (max(0, -steps), min(count, count - steps))
    return lax.ppermute(value, axis, [(source, source + steps) for source in range(initial, last)])


def slot_numbers(block_routes, capacity, experts_n):
    route_pairs = block_routes.reshape(block_routes.shape[:-2] + (-1,))
    onehot = (route_pairs[..., None] == jnp.arange(experts_n, dtype=jnp.int32)).astype(jnp.int32)
    slot_rank = jnp.sum((jnp.cumsum(onehot, axis=-2) - onehot) * onehot, axis=-1)
    return (route_pairs * capacity + slot_rank).reshape(block_routes.shape)


def dispatch_matrix(slot_ids, slot_total):
    numbers = jnp.arange(slot_total, dtype=jnp.int32)[:, None, None]
    matches = jnp.any(numbers == slot_ids[..., None, :, :], axis=-1)
    return matches.astype(jnp.bfloat16)


def plain_shards(
    residual,
    conv_value,
    conv_gate,
    segments,
    conv_weight,
    norm_gain,
    norm_shift,
    out_weight,
    ffn_gain,
    routes,
    route_weights,
    w_gate,
    w_up,
    w_down,
):
    tok_dev, local_channels = conv_value.shape
    reach = conv_weight.shape[0] - 1
    whole_gate, whole_up = (
        lax.all_gather(w_gate[0], "tp", axis=1, tiled=True),
        lax.all_gather(w_up[0], "tp", axis=1, tiled=True),
    )
    whole_down = lax.all_gather(w_down[0], "tp", axis=0, tiled=True)
    gated = (conv_value.astype(jnp.float32) * jax.nn.sigmoid(conv_gate.astype(jnp.float32))).astype(
        jnp.bfloat16
    )
    rim_prev, seg_prev = passed_along(
        (gated[tok_dev - reach :], segments[tok_dev - reach :]), "sp", 1
    )
    extended = jnp.concatenate([rim_prev, gated], 0).astype(jnp.float32)
    seg_ext = jnp.concatenate([seg_prev, segments], 0)
    convolved = jnp.zeros((tok_dev, local_channels), jnp.float32)
    for offset in range(reach + 1):
        same_doc = (seg_ext[offset : offset + tok_dev] == segments)[:, None]
        convolved = convolved + jnp.where(
            same_doc, extended[offset : offset + tok_dev] * conv_weight[offset], 0.0
        )
    group_size = DC // CONV_GROUPS
    grouped = convolved.reshape(tok_dev, local_channels // group_size, group_size)
    group_mean = jnp.mean(grouped, axis=-1, keepdims=True)
    group_var = jnp.mean(jnp.square(grouped - group_mean), axis=-1, keepdims=True)
    scaled = ((grouped - group_mean) * lax.rsqrt(group_var + 1e-05)).reshape(
        tok_dev, local_channels
    ) * norm_gain + norm_shift
    conv_out = jax.nn.silu(scaled).astype(jnp.bfloat16)
    columns = lax.axis_size("tp")
    column = lax.axis_index("tp")
    rows_own = tok_dev // columns
    own_conv = lax.all_to_all(conv_out, "tp", split_axis=0, concat_axis=1, tiled=True)
    mixed = jnp.dot(own_conv, out_weight, preferred_element_type=jnp.float32)
    stream = residual.astype(jnp.float32) + lax.optimization_barrier(
        mixed.astype(jnp.bfloat16)
    ).astype(jnp.float32)
    normed = (
        stream * lax.rsqrt(jnp.mean(stream * stream, axis=-1, keepdims=True) + 1e-06) * ffn_gain
    ).astype(jnp.bfloat16)
    experts_n = lax.axis_size("sp")
    top_count = routes.shape[1]
    model_width = normed.shape[1]
    capacity = max(2, 2 * tok_dev * top_count // (columns * experts_n))
    slot_total = experts_n * capacity
    own_routes = lax.dynamic_slice_in_dim(routes, column * rows_own, rows_own, 0)
    own_weights = lax.dynamic_slice_in_dim(route_weights, column * rows_own, rows_own, 0)
    own_slots = slot_numbers(own_routes, capacity, experts_n)
    routing_table = dispatch_matrix(own_slots, slot_total)
    outgoing = jnp.dot(routing_table, normed, preferred_element_type=jnp.float32).astype(
        jnp.bfloat16
    )
    outgoing = outgoing.reshape(experts_n, capacity, model_width)
    arrived = lax.all_to_all(outgoing, "sp", split_axis=0, concat_axis=1, tiled=True).reshape(
        slot_total, model_width
    )
    gate_act = jnp.dot(arrived, whole_gate, preferred_element_type=jnp.float32)
    up_act = jnp.dot(arrived, whole_up, preferred_element_type=jnp.float32)
    hidden = (jax.nn.silu(gate_act) * up_act).astype(jnp.bfloat16)
    summed = jnp.dot(hidden, whole_down, preferred_element_type=jnp.float32)
    expert_out = summed.astype(jnp.bfloat16).reshape(experts_n, capacity, model_width)
    returned = lax.all_to_all(expert_out, "sp", split_axis=0, concat_axis=0, tiled=True).reshape(
        slot_total, model_width
    )
    combined = stream
    for member in range(top_count):
        chosen = jnp.take(returned, own_slots[:, member], axis=0).astype(jnp.float32)
        combined = combined + own_weights[:, member : member + 1] * chosen
    return combined.astype(jnp.bfloat16)


def flipped(index, mask):
    bit = 1
    while bit <= mask:
        if mask & bit:
            index = index + bit * (1 - 2 * ((index // bit) % 2))
        bit *= 2
    return index


def layer_kernel(
    experts_n, columns, capacity, blocks,
    residual_hbm, value_hbm, gate_hbm, seg_ref, conv_w_ref, gain_ref, shift_ref, ow_hbm, ffn_ref,
    routes_ref, route_w_ref, wg_hbm, wu_hbm, wd_hbm,
    out_ref,
    residual, value, gate, ow, wg, wu, wd, wg_in, wu_in, wd_in, rim, seg_in, seg_ext, ext, win, seg_win,
    conv_out, conv_in, stream, normed, outgoing, arrived, rows_in, relay_out, hidden, partial,
    results, returned, relay_in, relay_sum, far_in, tables, picks, shares, routes_in, route_w_in,
    load_sem, y_send, y_recv, c_send, c_recv, f_send, f_recv, rim_send, rim_recv, x_send, x_recv,
    t_send, t_recv, far_send, far_recv, d_send, d_recv, rd_send,
    rb_send, rb_recv, r_send, r_recv, sum_send, sum_recv,
):
    me_s, me_t = lax.axis_index("sp"), lax.axis_index("tp")
    tok_dev, local = value.shape
    width = residual.shape[1]
    rows_own = tok_dev // columns
    taps = conv_w_ref.shape[0]
    halves = normed.shape[0]
    half = width // halves
    band = width // blocks
    near_n = experts_n // 2
    near_slots = near_n * capacity
    next_s = (me_s + 1) % experts_n
    tile = 512
    group = DC // CONV_GROUPS
    level = me_s // 2
    levels = experts_n // 2
    in_middle = jnp.logical_or(level == levels // 2 - 1, level == levels // 2)
    at_end = jnp.logical_not(in_middle)

    def tp_peer(mask):
        return (me_s, flipped(me_t, mask))

    def sp_peer(mask):
        return (flipped(me_s, mask), me_t)

    loads = [
        pltpu.make_async_copy(src, dst, load_sem.at[i])
        for i, (src, dst) in enumerate((
            (value_hbm, value), (gate_hbm, gate), (residual_hbm, residual), (ow_hbm, ow),
            (wg_hbm, wg), (wu_hbm, wu), (wd_hbm, wd),
        ))
    ]
    barrier = pltpu.get_barrier_semaphore()
    peers = [tp_peer(mask) for mask in range(1, columns)]
    peers += [sp_peer(mask) for mask in range(1, experts_n)]
    for peer in peers:
        pl.semaphore_signal(barrier, inc=1, device_id=peer, device_id_type=MESH)
    for load in loads:
        load.start()
    pl.semaphore_wait(barrier, len(peers))

    def remote(src, dst, send, recv, peer):
        return pltpu.make_async_remote_copy(
            src_ref=src, dst_ref=dst, send_sem=send, recv_sem=recv,
            device_id=peer, device_id_type=MESH,
        )

    last = pl.ds(tok_dev - RIM, RIM)
    rim_copies = [
        remote(ref, dst, rim_send.at[i], rim_recv.at[i], (next_s, me_t))
        for i, (ref, dst) in enumerate(
            ((value_hbm.at[last], rim.at[0]), (gate_hbm.at[last], rim.at[1]), (seg_ref, seg_in))
        )
    ]
    for copy in rim_copies:
        copy.start()

    def across_piece(i, own, into, rows, cols):
        return (
            remote(own.at[rows, cols], into.at[1, rows, cols], y_send.at[i], y_recv.at[i], tp_peer(2)),
            remote(into.at[1, rows, cols], into.at[2, rows, cols], f_send.at[i], f_recv.at[i], tp_peer(1)),
        )

    every, first_rows = pl.ds(0, local), width // 4
    pieces = [
        (wg_hbm, wg_in, pl.ds(0, first_rows), every),
        (wg_hbm, wg_in, pl.ds(first_rows, width - first_rows), every),
        (wu_hbm, wu_in, pl.ds(0, width // 2), every),
        (wu_hbm, wu_in, pl.ds(width // 2, width // 2), every),
    ]
    up_done = len(pieces)
    pieces += [(wd_hbm, wd_in, every, pl.ds(j * band, band)) for j in range(blocks)]
    across, forward = zip(*[across_piece(i, *piece) for i, piece in enumerate(pieces)])
    beside = [
        remote(own, into.at[0], c_send.at[i], c_recv.at[i], tp_peer(1))
        for i, (own, into) in enumerate(((wg_hbm, wg_in), (wu_hbm, wu_in), (wd_hbm, wd_in)))
    ]
    across[0].start()

    relay = jnp.where(in_middle, flipped(me_s, 6), flipped(me_s, 4))
    relay_slot = jnp.where(in_middle, 0, 1)
    route_copies = [
        remote(ref, dst.at[relay_slot], t_send.at[i], t_recv.at[relay_slot, i], (relay, me_t))
        for i, (ref, dst) in enumerate(((routes_ref, routes_in), (route_w_ref, route_w_in)))
    ]
    for copy in route_copies:
        copy.start()

    def gated_of(v, g):
        v, g = v.astype(jnp.float32), g.astype(jnp.float32)
        product = v * (1.0 / (1.0 + jnp.exp(-g)))
        return product.astype(jnp.bfloat16).astype(jnp.float32)

    def gate_rows(i, carry):
        row = pl.multiple_of(i * 64, 64)
        ext[pl.ds(row + RIM, 64), :] = gated_of(value[pl.ds(row, 64), :], gate[pl.ds(row, 64), :])
        return carry

    for load in loads[:2]:
        load.wait()
    lax.fori_loop(0, tok_dev // 64, gate_rows, 0)
    lanes_n = seg_ref.shape[1]

    def column(row):
        return jnp.broadcast_to(row.astype(jnp.float32), (lanes_n, lanes_n)).T

    for i in range(seg_ref.shape[0]):
        seg_ext[RIM + i * lanes_n : RIM + (i + 1) * lanes_n, :] = column(seg_ref[i : i + 1, :])

    for copy in rim_copies:
        copy.wait_recv()
    ext[pl.ds(0, RIM), :] = gated_of(rim[0], rim[1])
    before = column(seg_in[seg_ref.shape[0] - 1 : seg_ref.shape[0], :])[lanes_n - RIM :, :]
    seg_ext[0:RIM, :] = jnp.where(me_s == 0, -1.0, before)

    block = 64
    lead = RIM - (taps - 1)

    def conv_rows(row):
        win[...] = ext[pl.ds(row, RIM + block), :]
        seg_win[...] = seg_ext[pl.ds(row, RIM + block), :]
        own_seg = seg_win[RIM:, :]
        sums = [jnp.zeros((block, group), jnp.float32) for _ in range(local // group)]
        for tap in range(taps):
            at = lead + tap
            same_doc = seg_win[at : at + block, :] == own_seg
            for g in range(local // group):
                lanes = slice(g * group, (g + 1) * group)
                term = win[at : at + block, lanes] * conv_w_ref[tap : tap + 1, lanes]
                sums[g] = sums[g] + jnp.where(same_doc, term, 0.0)
        for g in range(local // group):
            lanes = slice(g * group, (g + 1) * group)
            mean = jnp.mean(sums[g], axis=-1, keepdims=True)
            centred = sums[g] - mean
            deviation = jnp.mean(centred * centred, axis=-1, keepdims=True)
            scaled = centred * lax.rsqrt(deviation + 1e-05) * gain_ref[:, lanes] + shift_ref[:, lanes]
            conv_out[pl.ds(row, block), lanes] = (scaled / (1.0 + jnp.exp(-scaled))).astype(jnp.bfloat16)

    exchange = {}
    for mask in (3, 2, 1, 0):
        peer_row = pl.multiple_of(flipped(me_t, mask) * rows_own, rows_own)

        def conv_step(i, carry):
            conv_rows(pl.multiple_of(peer_row + i * block, block))
            return carry

        lax.fori_loop(0, rows_own // block, conv_step, 0)
        if mask:
            exchange[mask] = remote(
                conv_out.at[pl.ds(peer_row, rows_own)], conv_in.at[mask],
                x_send.at[mask], x_recv.at[mask], tp_peer(mask),
            )
            exchange[mask].start()
        else:
            conv_in[0] = conv_out[pl.ds(peer_row, rows_own), :]
        if mask == 2:
            for copy in across[1:]:
                copy.start()

    for copy in beside:
        copy.start()
    numbers = lax.broadcasted_iota(jnp.int32, (rows_own, lanes_n), 1).astype(jnp.float32)
    earlier = jnp.where(
        lax.broadcasted_iota(jnp.int32, (rows_own, rows_own), 0)
        > lax.broadcasted_iota(jnp.int32, (rows_own, rows_own), 1), 1.0, 0.0,
    ).astype(jnp.bfloat16)
    slot_places = lax.broadcasted_iota(jnp.int32, (rows_own, near_slots), 1)
    own_lanes = pl.ds(pl.multiple_of(me_t * rows_own, rows_own), rows_own)
    top_count = routes_ref.shape[0]

    def make_tables(which, route_row, weight_row):
        names = [column(route_row(m)) for m in range(top_count)]
        marks = [jnp.where(name == numbers, 1.0, 0.0) for name in names]
        counts = jnp.dot(earlier, sum(marks).astype(jnp.bfloat16), preferred_element_type=jnp.float32)
        total = jnp.zeros((rows_own, near_slots), jnp.float32)
        for m, mark in enumerate(marks):
            rank = jnp.sum(counts * mark, axis=-1, keepdims=True).astype(jnp.int32)
            slot = (names[m][:, 0:1].astype(jnp.int32) ^ me_s) * capacity + rank
            table = jnp.where(slot_places == slot, 1.0, 0.0)
            tables[which, m] = table.astype(jnp.bfloat16)
            total = total + table
            shares[which, m] = column(weight_row(m))
        picks[which] = total.T.astype(jnp.bfloat16)

    make_tables(
        0, lambda m: routes_ref[m : m + 1, own_lanes], lambda m: route_w_ref[m : m + 1, own_lanes]
    )

    @pl.when(in_middle)
    def _():
        for slot in range(2):
            for i, ref in enumerate((routes_ref, route_w_ref)):
                dst = (routes_in, route_w_in)[i].at[slot]
                remote(ref, dst, t_send.at[i], t_recv.at[slot, i], (relay, me_t)).wait_recv()
            make_tables(
                1 + slot,
                lambda m: routes_in[slot, m : m + 1, own_lanes],
                lambda m: route_w_in[slot, m : m + 1, own_lanes],
            )

    across[0].wait_recv()
    forward[0].start()
    for load in loads[2:4]:
        load.wait()
    for mask in (1, 2, 3):
        exchange[mask].wait_recv()

    squares = jnp.zeros((rows_own, 1), jnp.float32)
    for col in range(0, width, tile):
        cols = slice(col, col + tile)
        mixed = jnp.zeros((rows_own, tile), jnp.float32)
        for mask in range(columns):
            w_rows = pl.ds(pl.multiple_of(flipped(me_t, mask) * local, local), local)
            mixed = mixed + jnp.dot(conv_in[mask], ow[w_rows, cols], preferred_element_type=jnp.float32)
        part = residual[:, cols].astype(jnp.float32) + mixed.astype(jnp.bfloat16).astype(jnp.float32)
        stream[:, cols] = part
        squares = squares + jnp.sum(part * part, axis=-1, keepdims=True)
    scale = lax.rsqrt(squares / width + 1e-06)
    far_rows = []
    for h in range(halves):
        cols = slice(h * half, (h + 1) * half)
        normed[h] = (stream[:, cols] * scale * ffn_ref[:, cols]).astype(jnp.bfloat16)
        far_rows.append(remote(
            normed.at[h], rows_in.at[relay_slot, h], far_send.at[h], far_recv.at[relay_slot, h], (relay, me_t)
        ))
        far_rows[h].start()

    def packet(mask):
        return pl.ds(mask * capacity, capacity)

    dispatch = {}
    for h in range(halves):
        for col in range(0, half, tile):
            cols = slice(col, col + tile)
            outgoing[h, :, cols] = jnp.dot(
                picks[0], normed[h, :, cols], preferred_element_type=jnp.float32
            ).astype(jnp.bfloat16)
        for mask in range(near_n - 1, 0, -1):
            dispatch[mask, h] = remote(
                outgoing.at[h, packet(mask)], arrived.at[h, packet(mask)],
                d_send.at[mask, h], d_recv.at[mask, h], sp_peer(mask),
            )
            dispatch[mask, h].start()
        arrived[h, 0:capacity, :] = outgoing[h, 0:capacity, :]

    relay_masks = ((6, 7, 4, 5), (4, 5, 6, 7))

    def relayed(slot, m, h):
        return remote(
            relay_out.at[slot, h, packet(m)], arrived.at[h, packet(relay_masks[slot][m])],
            rd_send.at[slot, m, h], d_recv.at[relay_masks[slot][m], h], sp_peer(m),
        )

    def relay_half(h):
        @pl.when(in_middle)
        def _():
            for slot in range(2):
                remote(
                    normed.at[h], rows_in.at[slot, h], far_send.at[h], far_recv.at[slot, h], (relay, me_t)
                ).wait_recv()
                for col in range(0, half, tile):
                    cols = slice(col, col + tile)
                    relay_out[slot, h, :, cols] = jnp.dot(
                        picks[1 + slot], rows_in[slot, h, :, cols], preferred_element_type=jnp.float32
                    ).astype(jnp.bfloat16)
                for m in (2, 3, 1):
                    relayed(slot, m, h).start()
                place = relay_masks[slot][0] * capacity
                arrived[h, place : place + capacity, :] = relay_out[slot, h, 0:capacity, :]

    def d_wait(mask, h):
        remote(
            outgoing.at[h, packet(0)], arrived.at[h, packet(mask)],
            d_send.at[0, h], d_recv.at[mask, h], sp_peer(1),
        ).wait_recv()

    relay_half(0)

    for load in loads[4:]:
        load.wait()
    for copy in beside:
        copy.wait_recv()
    across[1].wait_recv()
    forward[1].start()

    for h in range(1, halves):
        relay_half(h)

    for h in range(halves):
        for mask in range(1, near_n):
            d_wait(mask, h)

    near, far = slice(0, near_slots), slice(near_slots, 2 * near_slots)
    whole = slice(0, 2 * near_slots)

    def hidden_units(mask, rows):
        g = wg if mask == 0 else wg_in.at[mask - 1]
        u = wu if mask == 0 else wu_in.at[mask - 1]

        def act(w):
            return sum(
                jnp.dot(arrived[h, rows, :], w[h * half : (h + 1) * half, :], preferred_element_type=jnp.float32)
                for h in range(halves)
            )

        gate_act, up_act = act(g), act(u)
        hidden[mask, rows, :] = (gate_act / (1.0 + jnp.exp(-gate_act)) * up_act).astype(jnp.bfloat16)

    hidden_units(0, near)
    hidden_units(1, near)

    across[2].wait_recv()
    forward[2].start()

    for h in range(halves):
        for mask in range(near_n + 1, experts_n, 2):
            d_wait(mask, h)

    @pl.when(at_end)
    def _():
        for h in range(halves):
            for mask in range(near_n, experts_n, 2):
                d_wait(mask, h)

    hidden_units(0, far)
    hidden_units(1, far)

    across[3].wait_recv()
    forward[3].start()

    hidden_units(2, whole)

    for i in range(up_done):
        forward[i].wait_recv()

    hidden_units(3, whole)

    def to_relay(mask, m, slot, j):
        return remote(
            results.at[j, packet(mask)], relay_in.at[slot, j, packet(m)],
            rb_send.at[mask, j], rb_recv.at[slot, m, j], sp_peer(m),
        )

    from_middle = ((7, 1, 0), (5, 1, 1))
    from_end = ((4, 2, 0), (6, 2, 1), (5, 3, 0), (7, 3, 1))
    kept = ((6, 0), (4, 1))
    give_back = {
        (mask, j): remote(
            results.at[j, packet(mask)], returned.at[j, packet(mask)],
            r_send.at[mask, j], r_recv.at[mask, j], sp_peer(mask),
        )
        for j in range(blocks) for mask in range(1, near_n)
    }

    def band_results(j):
        cols = slice(j * band, (j + 1) * band)
        across[up_done + j].wait_recv()
        forward[up_done + j].start()

        def down(mask):
            w = wd[:, cols] if mask == 0 else wd_in[mask - 1, :, cols]
            return jnp.dot(hidden[mask], w, preferred_element_type=jnp.float32)

        partial[...] = down(0) + down(1) + down(2)
        forward[up_done + j].wait_recv()
        results[j] = (partial[...] + down(3)).astype(jnp.bfloat16)

        @pl.when(in_middle)
        def _():
            for mask, m, slot in from_middle:
                to_relay(mask, m, slot, j).start()
            for mask, slot in kept:
                relay_in[slot, j, 0:capacity, :] = results[j, mask * capacity : (mask + 1) * capacity, :]

        @pl.when(at_end)
        def _():
            for mask, m, slot in from_end:
                to_relay(mask, m, slot, j).start()

        returned[j, 0:capacity, :] = results[j, 0:capacity, :]

    def direct(j):
        for mask in range(near_n - 1, 0, -1):
            give_back[mask, j].start()

    def summed_up(slot, j):
        return remote(
            relay_sum.at[slot, j], far_in.at[j], sum_send.at[slot, j], sum_recv.at[j],
            sp_peer((6, 4)[slot]),
        )

    def weighed(which, packets):
        return sum(
            shares[which, m][:, 0:1] * jnp.dot(tables[which, m], packets, preferred_element_type=jnp.float32)
            for m in range(top_count)
        )

    def relay_band(j):
        @pl.when(in_middle)
        def _():
            for slot in range(2):
                for m in range(1, near_n):
                    remote(
                        results.at[j, packet(0)], relay_in.at[slot, j, packet(m)],
                        rb_send.at[near_n, j], rb_recv.at[slot, m, j], sp_peer(m),
                    ).wait_recv()
                relay_sum[slot, j] = weighed(1 + slot, relay_in[slot, j]).astype(jnp.bfloat16)
                summed_up(slot, j).start()

    band_results(0)
    direct(0)
    band_results(1)
    relay_band(0)
    band_results(2)
    relay_band(1)
    band_results(3)
    for j in range(1, blocks):
        direct(j)
    relay_band(2)
    relay_band(3)

    def finish(j):
        cols = slice(j * band, (j + 1) * band)
        for mask in range(1, near_n):
            give_back[mask, j].wait_recv()
        remote(
            relay_sum.at[0, j], far_in.at[j], sum_send.at[0, j], sum_recv.at[j], (relay, me_t)
        ).wait_recv()
        total = stream[:, cols] + weighed(0, returned[j]) + far_in[j].astype(jnp.float32)
        out_ref[:, cols] = total.astype(jnp.bfloat16)

    finish(0)
    finish(1)
    finish(2)
    finish(3)

    own_copies = rim_copies + route_copies + list(across) + list(forward) + beside + far_rows
    for copy in own_copies + list(exchange.values()) + list(dispatch.values()) + list(give_back.values()):
        copy.wait_send()

    @pl.when(in_middle)
    def _():
        for slot in range(2):
            for h in range(halves):
                for m in range(1, near_n):
                    relayed(slot, m, h).wait_send()
            for j in range(blocks):
                summed_up(slot, j).wait_send()
        for j in range(blocks):
            for mask, m, slot in from_middle:
                to_relay(mask, m, slot, j).wait_send()

    @pl.when(at_end)
    def _():
        for j in range(blocks):
            for mask, m, slot in from_end:
                to_relay(mask, m, slot, j).wait_send()


def shards(*args):
    (residual, conv_value, conv_gate, segments, conv_weight, norm_gain, norm_shift, out_weight,
     ffn_gain, routes, route_weights, w_gate, w_up, w_down) = args
    tok_dev, local = conv_value.shape
    width = residual.shape[1]
    experts_n, columns = lax.axis_size("sp"), lax.axis_size("tp")
    top_count = routes.shape[1]
    capacity = max(2, 2 * tok_dev * top_count // (columns * experts_n))
    if capacity % 32 or columns != 4 or tok_dev != columns * 128 or experts_n != 8:
        return plain_shards(*args)
    rows_own = tok_dev // columns
    lanes = DC // CONV_GROUPS
    slot_total = experts_n * capacity
    near_slots = slot_total // 2
    halves, blocks = 2, 4
    half, band = width // halves, width // blocks
    bf16, f32 = jnp.bfloat16, jnp.float32
    vmem, dma = pltpu.VMEM, pltpu.SemaphoreType.DMA
    spec, anywhere = pl.BlockSpec(memory_space=pltpu.VMEM), pl.BlockSpec(memory_space=pl.ANY)
    specs = [spec] * 14
    for i in (0, 1, 2, 7, 11, 12, 13):
        specs[i] = anywhere
    routes_t, route_weights_t = routes.T, route_weights.T
    return pl.pallas_call(
        functools.partial(layer_kernel, experts_n, columns, capacity, blocks),
        out_shape=jax.ShapeDtypeStruct((rows_own, width), bf16),
        in_specs=specs,
        out_specs=spec,
        scratch_shapes=[
            vmem((rows_own, width), bf16), vmem((tok_dev, local), bf16), vmem((tok_dev, local), bf16),
            vmem(out_weight.shape, bf16),
            vmem((width, local), bf16), vmem((width, local), bf16), vmem((local, width), bf16),
            vmem((3, width, local), bf16), vmem((3, width, local), bf16), vmem((3, local, width), bf16),
            vmem((2, RIM, local), bf16), vmem((tok_dev // lanes, lanes), jnp.int32),
            vmem((RIM + tok_dev, lanes), f32), vmem((RIM + tok_dev, local), f32),
            vmem((RIM + 64, local), f32), vmem((RIM + 64, lanes), f32),
            vmem((tok_dev, local), bf16), vmem((columns, rows_own, local), bf16),
            vmem((rows_own, width), f32), vmem((halves, rows_own, half), bf16),
            vmem((halves, near_slots, half), bf16), vmem((halves, slot_total, half), bf16),
            vmem((2, halves, rows_own, half), bf16), vmem((2, halves, near_slots, half), bf16),
            vmem((columns, slot_total, local), bf16), vmem((slot_total, band), f32),
            vmem((blocks, slot_total, band), bf16), vmem((blocks, near_slots, band), bf16),
            vmem((2, blocks, near_slots, band), bf16), vmem((2, blocks, rows_own, band), bf16),
            vmem((blocks, rows_own, band), bf16),
            vmem((3, top_count, rows_own, near_slots), bf16), vmem((3, near_slots, rows_own), bf16),
            vmem((3, top_count, rows_own, rows_own), f32),
            vmem((2, *routes_t.shape), routes.dtype), vmem((2, *route_weights_t.shape), route_weights.dtype),
            dma((7,)), dma((4 + blocks,)), dma((4 + blocks,)), dma((3,)), dma((3,)),
            dma((4 + blocks,)), dma((4 + blocks,)), dma((3,)), dma((3,)), dma((columns,)), dma((columns,)),
            dma((2,)), dma((2, 2)), dma((halves,)), dma((2, halves)),
            dma((experts_n // 2, halves)), dma((experts_n, halves)), dma((2, experts_n // 2, halves)),
            dma((experts_n, blocks)), dma((2, experts_n // 2, blocks)),
            dma((experts_n // 2, blocks)), dma((experts_n // 2, blocks)), dma((2, blocks)), dma((blocks,)),
        ],
        compiler_params=pltpu.CompilerParams(
            collective_id=0, has_side_effects=True, vmem_limit_bytes=60 * 1024 * 1024
        ),
    )(
        residual, conv_value, conv_gate,
        segments.reshape(-1, lanes), conv_weight,
        norm_gain[None], norm_shift[None], out_weight, ffn_gain[None],
        routes_t, route_weights_t, w_gate[0], w_up[0], w_down[0],
    )


def solution(mesh):
    return jax.shard_map(
        shards,
        mesh=mesh,
        in_specs=(
            P(("sp", "tp"), None),
            P("sp", "tp"),
            P("sp", "tp"),
            P("sp"),
            P(None, "tp"),
            P("tp"),
            P("tp"),
            P(),
            P(),
            P("sp", None),
            P("sp", None),
            P("sp", None, "tp"),
            P("sp", None, "tp"),
            P("sp", "tp", None),
        ),
        out_specs=P(("sp", "tp"), None),
        check_vma=False,
    )
```

```python
import functools

import jax
import jax.numpy as jnp
from jax import lax
from jax.experimental import pallas as pl
from jax.experimental.pallas import tpu as pltpu
from jax.sharding import PartitionSpec as P

DC = 1024
CONV_GROUPS = 8
MESH = pl.DeviceIdType.MESH
RIM = 32


def passed_along(value, axis, steps):
    count = lax.axis_size(axis)
    initial, last = (max(0, -steps), min(count, count - steps))
    return lax.ppermute(value, axis, [(source, source + steps) for source in range(initial, last)])


def slot_numbers(block_routes, capacity, experts_n):
    route_pairs = block_routes.reshape(block_routes.shape[:-2] + (-1,))
    onehot = (route_pairs[..., None] == jnp.arange(experts_n, dtype=jnp.int32)).astype(jnp.int32)
    slot_rank = jnp.sum((jnp.cumsum(onehot, axis=-2) - onehot) * onehot, axis=-1)
    return (route_pairs * capacity + slot_rank).reshape(block_routes.shape)


def dispatch_matrix(slot_ids, slot_total):
    numbers = jnp.arange(slot_total, dtype=jnp.int32)[:, None, None]
    matches = jnp.any(numbers == slot_ids[..., None, :, :], axis=-1)
    return matches.astype(jnp.bfloat16)


def plain_shards(
    residual,
    conv_value,
    conv_gate,
    segments,
    conv_weight,
    norm_gain,
    norm_shift,
    out_weight,
    ffn_gain,
    routes,
    route_weights,
    w_gate,
    w_up,
    w_down,
):
    tok_dev, local_channels = conv_value.shape
    reach = conv_weight.shape[0] - 1
    whole_gate, whole_up = (
        lax.all_gather(w_gate[0], "tp", axis=1, tiled=True),
        lax.all_gather(w_up[0], "tp", axis=1, tiled=True),
    )
    whole_down = lax.all_gather(w_down[0], "tp", axis=0, tiled=True)
    gated = (conv_value.astype(jnp.float32) * jax.nn.sigmoid(conv_gate.astype(jnp.float32))).astype(
        jnp.bfloat16
    )
    rim_prev, seg_prev = passed_along(
        (gated[tok_dev - reach :], segments[tok_dev - reach :]), "sp", 1
    )
    extended = jnp.concatenate([rim_prev, gated], 0).astype(jnp.float32)
    seg_ext = jnp.concatenate([seg_prev, segments], 0)
    convolved = jnp.zeros((tok_dev, local_channels), jnp.float32)
    for offset in range(reach + 1):
        same_doc = (seg_ext[offset : offset + tok_dev] == segments)[:, None]
        convolved = convolved + jnp.where(
            same_doc, extended[offset : offset + tok_dev] * conv_weight[offset], 0.0
        )
    group_size = DC // CONV_GROUPS
    grouped = convolved.reshape(tok_dev, local_channels // group_size, group_size)
    group_mean = jnp.mean(grouped, axis=-1, keepdims=True)
    group_var = jnp.mean(jnp.square(grouped - group_mean), axis=-1, keepdims=True)
    scaled = ((grouped - group_mean) * lax.rsqrt(group_var + 1e-05)).reshape(
        tok_dev, local_channels
    ) * norm_gain + norm_shift
    conv_out = jax.nn.silu(scaled).astype(jnp.bfloat16)
    columns = lax.axis_size("tp")
    column = lax.axis_index("tp")
    rows_own = tok_dev // columns
    own_conv = lax.all_to_all(conv_out, "tp", split_axis=0, concat_axis=1, tiled=True)
    mixed = jnp.dot(own_conv, out_weight, preferred_element_type=jnp.float32)
    stream = residual.astype(jnp.float32) + lax.optimization_barrier(
        mixed.astype(jnp.bfloat16)
    ).astype(jnp.float32)
    normed = (
        stream * lax.rsqrt(jnp.mean(stream * stream, axis=-1, keepdims=True) + 1e-06) * ffn_gain
    ).astype(jnp.bfloat16)
    experts_n = lax.axis_size("sp")
    top_count = routes.shape[1]
    model_width = normed.shape[1]
    capacity = max(2, 2 * tok_dev * top_count // (columns * experts_n))
    slot_total = experts_n * capacity
    own_routes = lax.dynamic_slice_in_dim(routes, column * rows_own, rows_own, 0)
    own_weights = lax.dynamic_slice_in_dim(route_weights, column * rows_own, rows_own, 0)
    own_slots = slot_numbers(own_routes, capacity, experts_n)
    routing_table = dispatch_matrix(own_slots, slot_total)
    outgoing = jnp.dot(routing_table, normed, preferred_element_type=jnp.float32).astype(
        jnp.bfloat16
    )
    outgoing = outgoing.reshape(experts_n, capacity, model_width)
    arrived = lax.all_to_all(outgoing, "sp", split_axis=0, concat_axis=1, tiled=True).reshape(
        slot_total, model_width
    )
    gate_act = jnp.dot(arrived, whole_gate, preferred_element_type=jnp.float32)
    up_act = jnp.dot(arrived, whole_up, preferred_element_type=jnp.float32)
    hidden = (jax.nn.silu(gate_act) * up_act).astype(jnp.bfloat16)
    summed = jnp.dot(hidden, whole_down, preferred_element_type=jnp.float32)
    expert_out = summed.astype(jnp.bfloat16).reshape(experts_n, capacity, model_width)
    returned = lax.all_to_all(expert_out, "sp", split_axis=0, concat_axis=0, tiled=True).reshape(
        slot_total, model_width
    )
    combined = stream
    for member in range(top_count):
        chosen = jnp.take(returned, own_slots[:, member], axis=0).astype(jnp.float32)
        combined = combined + own_weights[:, member : member + 1] * chosen
    return combined.astype(jnp.bfloat16)


def flipped(index, mask):
    bit = 1
    while bit <= mask:
        if mask & bit:
            index = index + bit * (1 - 2 * ((index // bit) % 2))
        bit *= 2
    return index


def layer_kernel(
    experts_n, columns, capacity, blocks,
    residual_hbm, value_hbm, gate_hbm, seg_hbm, conv_w_hbm, gain_hbm, shift_hbm, ow_hbm, ffn_hbm,
    routes_hbm, route_w_hbm, wg_hbm, wu_hbm, wd_hbm,
    out_hbm,
    residual, value, gate, seg_ref, conv_w_ref, gain_ref, shift_ref, ow, ffn_ref, routes_ref, route_w_ref,
    wg, wu, wd, out_ref, wg_in, wu_in, wd_in, rim, seg_in, seg_ext, ext, win, seg_win,
    conv_out, conv_in, stream, normed, outgoing, arrived, rows_in, relay_out, hidden, silu_gate, partial,
    results, returned, relay_in, relay_sum, far_in, tables, picks, shares, routes_in, route_w_in,
    load_sem, y_send, y_recv, c_send, c_recv, f_send, f_recv, rim_send, rim_recv, x_send, x_recv,
    t_send, t_recv, far_send, far_recv, d_send, d_recv, e_recv, rd_send,
    rb_send, rb_recv, r_send, r_recv, sum_send, sum_recv, out_sem,
):
    me_s, me_t = lax.axis_index("sp"), lax.axis_index("tp")
    tok_dev, local = value.shape
    width = residual.shape[1]
    rows_own = tok_dev // columns
    taps = conv_w_ref.shape[0]
    halves = normed.shape[0]
    half = width // halves
    band = width // blocks
    near_n = experts_n // 2
    near_slots = near_n * capacity
    next_s = (me_s + 1) % experts_n
    tile = 512
    group = DC // CONV_GROUPS
    level = me_s // 2
    levels = experts_n // 2
    in_middle = jnp.logical_or(level == levels // 2 - 1, level == levels // 2)
    at_end = jnp.logical_not(in_middle)

    def tp_peer(mask):
        return (me_s, flipped(me_t, mask))

    def sp_peer(mask):
        return (flipped(me_s, mask), me_t)

    loads = [
        pltpu.make_async_copy(src, dst, load_sem.at[i])
        for i, (src, dst) in enumerate((
            (value_hbm, value), (gate_hbm, gate), (seg_hbm, seg_ref), (conv_w_hbm, conv_w_ref),
            (gain_hbm, gain_ref), (shift_hbm, shift_ref), (routes_hbm, routes_ref), (route_w_hbm, route_w_ref),
            (residual_hbm, residual), (ow_hbm, ow), (ffn_hbm, ffn_ref),
            (wg_hbm, wg), (wu_hbm, wu), (wd_hbm, wd),
        ))
    ]
    conv_loads, stream_loads = 8, 11
    barrier = pltpu.get_barrier_semaphore()
    peers = [tp_peer(mask) for mask in range(1, columns)]
    peers += [sp_peer(mask) for mask in range(1, experts_n)]
    for peer in peers:
        pl.semaphore_signal(barrier, inc=1, device_id=peer, device_id_type=MESH)
    for load in loads:
        load.start()
    for load in loads[:conv_loads]:
        load.wait()
    pl.semaphore_wait(barrier, len(peers))

    def remote(src, dst, send, recv, peer):
        return pltpu.make_async_remote_copy(
            src_ref=src, dst_ref=dst, send_sem=send, recv_sem=recv,
            device_id=peer, device_id_type=MESH,
        )

    last = pl.ds(tok_dev - RIM, RIM)
    rim_copies = [
        remote(ref, dst, rim_send.at[i], rim_recv.at[i], (next_s, me_t))
        for i, (ref, dst) in enumerate(
            ((value.at[last], rim.at[0]), (gate.at[last], rim.at[1]), (seg_ref, seg_in))
        )
    ]
    for copy in rim_copies:
        copy.start()

    def across_piece(i, own, into, rows, cols):
        return (
            remote(own.at[rows, cols], into.at[1, rows, cols], y_send, y_recv.at[i], tp_peer(2)),
            remote(into.at[1, rows, cols], into.at[2, rows, cols], f_send, f_recv.at[i], tp_peer(1)),
        )

    every, first_rows = pl.ds(0, local), width // 4
    pieces = [
        (wg_hbm, wg_in, pl.ds(0, first_rows), every),
        (wg_hbm, wg_in, pl.ds(first_rows, width - first_rows), every),
        (wu_hbm, wu_in, pl.ds(0, width // 2), every),
        (wu_hbm, wu_in, pl.ds(width // 2, width // 4), every),
        (wu_hbm, wu_in, pl.ds(3 * width // 4, width // 4), every),
    ]
    up_done = len(pieces)
    pieces += [(wd_hbm, wd_in, every, pl.ds(j * band, band)) for j in range(blocks)]
    across, forward = zip(*[across_piece(i, *piece) for i, piece in enumerate(pieces)])
    beside = [
        remote(own, into.at[0], c_send, c_recv.at[i], tp_peer(1))
        for i, (own, into) in enumerate(((wg_hbm, wg_in), (wu_hbm, wu_in), (wd_hbm, wd_in)))
    ]
    across[0].start()

    relay = jnp.where(in_middle, flipped(me_s, 6), flipped(me_s, 4))
    relay_slot = jnp.where(in_middle, 0, 1)
    route_copies = [
        remote(ref, dst.at[relay_slot], t_send.at[i], t_recv.at[relay_slot, i], (relay, me_t))
        for i, (ref, dst) in enumerate(((routes_ref, routes_in), (route_w_ref, route_w_in)))
    ]
    for copy in route_copies:
        copy.start()

    def gated_of(v, g):
        v, g = v.astype(jnp.float32), g.astype(jnp.float32)
        product = v * (1.0 / (1.0 + jnp.exp(-g)))
        return product.astype(jnp.bfloat16).astype(jnp.float32)

    def gate_rows(i, carry):
        row = pl.multiple_of(i * 64, 64)
        ext[pl.ds(row + RIM, 64), :] = gated_of(value[pl.ds(row, 64), :], gate[pl.ds(row, 64), :])
        return carry

    lax.fori_loop(0, tok_dev // 64, gate_rows, 0)
    lanes_n = seg_ref.shape[1]

    def column(row):
        return jnp.broadcast_to(row.astype(jnp.float32), (lanes_n, lanes_n)).T

    for i in range(seg_ref.shape[0]):
        seg_ext[RIM + i * lanes_n : RIM + (i + 1) * lanes_n, :] = column(seg_ref[i : i + 1, :])

    block = 64
    lead = RIM - (taps - 1)

    def conv_rows(row):
        win[...] = ext[pl.ds(row, RIM + rows_own), :]
        seg_win[...] = seg_ext[pl.ds(row, RIM + rows_own), :]
        for start in range(0, rows_own, block):
            own_seg = seg_win[start + RIM : start + RIM + block, :]
            sums = [jnp.zeros((block, group), jnp.float32) for _ in range(local // group)]
            for tap in range(taps):
                at = start + lead + tap
                same_doc = seg_win[at : at + block, :] == own_seg
                for g in range(local // group):
                    lanes = slice(g * group, (g + 1) * group)
                    term = win[at : at + block, lanes] * conv_w_ref[tap : tap + 1, lanes]
                    sums[g] = sums[g] + jnp.where(same_doc, term, 0.0)
            for g in range(local // group):
                lanes = slice(g * group, (g + 1) * group)
                mean = jnp.mean(sums[g], axis=-1, keepdims=True)
                centred = sums[g] - mean
                deviation = jnp.mean(centred * centred, axis=-1, keepdims=True)
                scaled = centred * lax.rsqrt(deviation + 1e-05) * gain_ref[:, lanes] + shift_ref[:, lanes]
                conv_out[pl.ds(row + start, block), lanes] = (scaled / (1.0 + jnp.exp(-scaled))).astype(jnp.bfloat16)

    low = me_t % 2
    masks = (3 - low, 2 + low, 1, 0)

    def conv_part(i):
        peer_row = pl.multiple_of((me_t ^ masks[i]) * rows_own, rows_own)
        conv_rows(peer_row)
        if i == 3:
            conv_in[0] = conv_out[pl.ds(peer_row, rows_own), :]
            return []
        copy = remote(
            conv_out.at[pl.ds(peer_row, rows_own)], conv_in.at[masks[i]], x_send, x_recv,
            (me_s, me_t ^ masks[i]),
        )
        copy.start()
        return [copy]

    conv_part(0)

    numbers = lax.broadcasted_iota(jnp.int32, (rows_own, lanes_n), 1).astype(jnp.float32)
    earlier = jnp.where(
        lax.broadcasted_iota(jnp.int32, (rows_own, rows_own), 0)
        > lax.broadcasted_iota(jnp.int32, (rows_own, rows_own), 1), 1.0, 0.0,
    ).astype(jnp.bfloat16)
    slot_places = lax.broadcasted_iota(jnp.int32, (rows_own, near_slots), 1)
    own_lanes = pl.ds(pl.multiple_of(me_t * rows_own, rows_own), rows_own)
    top_count = routes_ref.shape[0]

    def make_tables(which, route_row, weight_row):
        names = [column(route_row(m)) for m in range(top_count)]
        marks = [jnp.where(name == numbers, 1.0, 0.0) for name in names]
        counts = jnp.dot(earlier, sum(marks).astype(jnp.bfloat16), preferred_element_type=jnp.float32)
        total = jnp.zeros((rows_own, near_slots), jnp.float32)
        for m, mark in enumerate(marks):
            rank = jnp.sum(counts * mark, axis=-1, keepdims=True).astype(jnp.int32)
            slot = (names[m][:, 0:1].astype(jnp.int32) ^ me_s) * capacity + rank
            table = jnp.where(slot_places == slot, 1.0, 0.0)
            tables[which, m] = table.astype(jnp.bfloat16)
            total = total + table
            shares[which, m] = column(weight_row(m))
        picks[which] = total.T.astype(jnp.bfloat16)

    make_tables(
        0, lambda m: routes_ref[m : m + 1, own_lanes], lambda m: route_w_ref[m : m + 1, own_lanes]
    )

    for copy in rim_copies:
        copy.wait_recv()
    ext[pl.ds(0, RIM), :] = gated_of(rim[0], rim[1])
    before = column(seg_in[seg_ref.shape[0] - 1 : seg_ref.shape[0], :])[lanes_n - RIM :, :]
    seg_ext[0:RIM, :] = jnp.where(me_s == 0, -1.0, before)

    conv_part(1)
    for copy in across[1:]:
        copy.start()
    conv_part(2)
    for copy in beside:
        copy.start()
    conv_part(3)

    @pl.when(in_middle)
    def _():
        for slot in range(2):
            for i, ref in enumerate((routes_ref, route_w_ref)):
                dst = (routes_in, route_w_in)[i].at[slot]
                remote(ref, dst, t_send.at[i], t_recv.at[slot, i], (relay, me_t)).wait_recv()
            make_tables(
                1 + slot,
                lambda m: routes_in[slot, m : m + 1, own_lanes],
                lambda m: route_w_in[slot, m : m + 1, own_lanes],
            )

    across[0].wait_recv()
    forward[0].start()
    for load in loads[conv_loads:stream_loads]:
        load.wait()
    swapped = remote(conv_in.at[pl.ds(1, columns - 1)], conv_in.at[pl.ds(1, columns - 1)], x_send, x_recv, tp_peer(1))
    swapped.wait_recv()

    squares = jnp.zeros((rows_own, 1), jnp.float32)
    for col in range(0, width, tile):
        cols = slice(col, col + tile)
        mixed = jnp.zeros((rows_own, tile), jnp.float32)
        for mask in range(columns):
            w_rows = pl.ds(pl.multiple_of(flipped(me_t, mask) * local, local), local)
            mixed = mixed + jnp.dot(conv_in[mask], ow[w_rows, cols], preferred_element_type=jnp.float32)
        part = residual[:, cols].astype(jnp.float32) + mixed.astype(jnp.bfloat16).astype(jnp.float32)
        stream[:, cols] = part
        squares = squares + jnp.sum(part * part, axis=-1, keepdims=True)
    scale = lax.rsqrt(squares / width + 1e-06)
    far_rows = []
    for h in range(halves):
        cols = slice(h * half, (h + 1) * half)
        normed[h] = (stream[:, cols] * scale * ffn_ref[:, cols]).astype(jnp.bfloat16)
        far_rows.append(remote(
            normed.at[h], rows_in.at[relay_slot, h], far_send.at[h], far_recv.at[relay_slot, h], (relay, me_t)
        ))
        far_rows[h].start()

    def packet(mask):
        return pl.ds(mask * capacity, capacity)

    others = pl.ds(capacity, near_slots - capacity)
    for h in range(halves):
        for col in range(0, half, tile):
            cols = slice(col, col + tile)
            outgoing[h, :, cols] = jnp.dot(
                picks[0], normed[h, :, cols], preferred_element_type=jnp.float32
            ).astype(jnp.bfloat16)
        for mask in range(near_n - 1, 0, -1):
            remote(
                outgoing.at[h, packet(mask)], arrived.at[h, packet(mask)], d_send, d_recv, sp_peer(mask)
            ).start()
        arrived[h, 0:capacity, :] = outgoing[h, 0:capacity, :]

    relay_masks = ((6, 7, 4, 5), (4, 5, 6, 7))

    def relayed(slot, m, h):
        return remote(
            relay_out.at[slot, h, packet(m)], arrived.at[h, packet(relay_masks[slot][m])],
            rd_send, e_recv, sp_peer(m),
        )

    def relay_half(slot, h):
        @pl.when(in_middle)
        def _():
            remote(
                normed.at[h], rows_in.at[slot, h], far_send.at[h], far_recv.at[slot, h], (relay, me_t)
            ).wait_recv()
            for col in range(0, half, tile):
                cols = slice(col, col + tile)
                relay_out[slot, h, :, cols] = jnp.dot(
                    picks[1 + slot], rows_in[slot, h, :, cols], preferred_element_type=jnp.float32
                ).astype(jnp.bfloat16)
            for m in (2, 3, 1):
                relayed(slot, m, h).start()
            place = relay_masks[slot][0] * capacity
            arrived[h, place : place + capacity, :] = relay_out[slot, h, 0:capacity, :]

    def landed(rows, recv):
        remote(arrived.at[:, rows], arrived.at[:, rows], d_send, recv, sp_peer(1)).wait_recv()

    for h in range(halves):
        relay_half(1, h)

    for load in loads[stream_loads:]:
        load.wait()
    for copy in beside:
        copy.wait_recv()
    across[1].wait_recv()
    forward[1].start()

    for h in range(halves):
        relay_half(0, h)

    landed(others, d_recv)

    near, far = slice(0, near_slots), slice(near_slots, 2 * near_slots)

    def act(w, rows):
        return sum(
            jnp.dot(arrived[h, rows, :], w[h * half : (h + 1) * half, :], preferred_element_type=jnp.float32)
            for h in range(halves)
        )

    def silu(v):
        return v / (1.0 + jnp.exp(-v))

    def hidden_units(mask, rows):
        g = wg if mask == 0 else wg_in.at[mask - 1]
        u = wu if mask == 0 else wu_in.at[mask - 1]
        hidden[mask, rows, :] = (silu(act(g, rows)) * act(u, rows)).astype(jnp.bfloat16)

    hidden_units(0, near)
    hidden_units(1, near)

    across[2].wait_recv()
    forward[2].start()

    @pl.when(in_middle)
    def _():
        landed(pl.ds(near_slots, 2 * capacity), e_recv)

    @pl.when(at_end)
    def _():
        landed(pl.ds(near_slots, 4 * capacity), e_recv)

    hidden_units(0, far)
    hidden_units(1, far)

    across[3].wait_recv()
    forward[3].start()

    for i in range(2):
        forward[i].wait_recv()
    for mask in (2, 3):
        for rows in (near, far):
            silu_gate[mask - 2, rows, :] = silu(act(wg_in.at[mask - 1], rows))

    across[4].wait_recv()
    forward[4].start()

    def finish_hidden(mask):
        for rows in (near, far):
            units = silu_gate[mask - 2, rows, :] * act(wu_in.at[mask - 1], rows)
            hidden[mask, rows, :] = units.astype(jnp.bfloat16)

    finish_hidden(2)

    for i in range(2, up_done):
        forward[i].wait_recv()

    finish_hidden(3)

    def to_relay(mask, m, slot, j):
        return remote(
            results.at[j, packet(mask)], relay_in.at[slot, j, packet(m)],
            rb_send, rb_recv.at[slot, j], sp_peer(m),
        )

    from_middle = ((7, 1, 0), (5, 1, 1))
    from_end = ((4, 2, 0), (6, 2, 1), (5, 3, 0), (7, 3, 1))
    kept = ((6, 0), (4, 1))
    give_back = {
        (mask, j): remote(
            results.at[j, packet(mask)], returned.at[j, packet(mask)],
            r_send, r_recv.at[j], sp_peer(mask),
        )
        for j in range(blocks) for mask in range(1, near_n)
    }

    def band_results(j):
        cols = slice(j * band, (j + 1) * band)
        across[up_done + j].wait_recv()
        forward[up_done + j].start()

        def down(mask):
            w = wd[:, cols] if mask == 0 else wd_in[mask - 1, :, cols]
            return jnp.dot(hidden[mask], w, preferred_element_type=jnp.float32)

        partial[...] = down(0) + down(1) + down(2)
        forward[up_done + j].wait_recv()
        results[j] = (partial[...] + down(3)).astype(jnp.bfloat16)

        @pl.when(in_middle)
        def _():
            for mask, m, slot in from_middle:
                to_relay(mask, m, slot, j).start()
            for mask, slot in kept:
                relay_in[slot, j, 0:capacity, :] = results[j, mask * capacity : (mask + 1) * capacity, :]

        @pl.when(at_end)
        def _():
            for mask, m, slot in from_end:
                to_relay(mask, m, slot, j).start()

        returned[j, 0:capacity, :] = results[j, 0:capacity, :]

    def direct(j):
        for mask in range(near_n - 1, 0, -1):
            give_back[mask, j].start()

    def summed_up(slot, j):
        return remote(
            relay_sum.at[slot, j], far_in.at[j], sum_send, sum_recv.at[j],
            sp_peer((6, 4)[slot]),
        )

    def weighed(which, packets):
        return sum(
            shares[which, m][:, 0:1] * jnp.dot(tables[which, m], packets, preferred_element_type=jnp.float32)
            for m in range(top_count)
        )

    def relay_band(j):
        @pl.when(in_middle)
        def _():
            for slot in range(2):
                remote(
                    relay_in.at[slot, j, others], relay_in.at[slot, j, others],
                    rb_send, rb_recv.at[slot, j], sp_peer(1),
                ).wait_recv()
                relay_sum[slot, j] = weighed(1 + slot, relay_in[slot, j]).astype(jnp.bfloat16)
                summed_up(slot, j).start()

    early, lag = blocks // 4, blocks // 2
    for j in range(blocks):
        band_results(j)
        if j < early:
            direct(j)
        else:
            pl.when(in_middle)(functools.partial(direct, j))
        if j >= lag:
            relay_band(j - lag)
    for j in range(early, blocks):
        pl.when(at_end)(functools.partial(direct, j))
    for j in range(blocks - lag, blocks):
        relay_band(j)

    outs = [
        pltpu.make_async_copy(
            out_ref.at[:, pl.ds(j * band, band)], out_hbm.at[:, pl.ds(j * band, band)], out_sem.at[j]
        )
        for j in range(blocks)
    ]

    def finish(j):
        cols = slice(j * band, (j + 1) * band)
        remote(
            relay_sum.at[0, j], far_in.at[j], sum_send, sum_recv.at[j], (relay, me_t)
        ).wait_recv()
        remote(
            returned.at[j, others], returned.at[j, others], r_send, r_recv.at[j], sp_peer(1)
        ).wait_recv()
        total = stream[:, cols] + weighed(0, returned[j]) + far_in[j].astype(jnp.float32)
        out_ref[:, cols] = total.astype(jnp.bfloat16)
        outs[j].start()

    for j in range(blocks // 2):
        finish(j)
    for j in range(blocks // 2, blocks):
        finish(j)

    def sent(ref, sem):
        remote(ref, ref, sem, sem, sp_peer(1)).wait_send()

    for copy in rim_copies + route_copies + far_rows:
        copy.wait_send()
    for sem in (y_send, f_send, c_send):
        sent(wg_in, sem)
    swapped.wait_send()
    sent(outgoing.at[:, others], d_send)
    sent(results.at[:, others], r_send)

    @pl.when(in_middle)
    def _():
        sent(relay_out.at[:, :, others], rd_send)
        sent(relay_sum, sum_send)
        sent(results.at[:, pl.ds(0, 2 * capacity)], rb_send)

    @pl.when(at_end)
    def _():
        sent(results.at[:, pl.ds(0, 4 * capacity)], rb_send)

    for copy in outs:
        copy.wait()


def shards(*args):
    (residual, conv_value, conv_gate, segments, conv_weight, norm_gain, norm_shift, out_weight,
     ffn_gain, routes, route_weights, w_gate, w_up, w_down) = args
    tok_dev, local = conv_value.shape
    width = residual.shape[1]
    experts_n, columns = lax.axis_size("sp"), lax.axis_size("tp")
    top_count = routes.shape[1]
    capacity = max(2, 2 * tok_dev * top_count // (columns * experts_n))
    if capacity % 32 or columns != 4 or tok_dev != columns * 128 or experts_n != 8:
        return plain_shards(*args)
    rows_own = tok_dev // columns
    lanes = DC // CONV_GROUPS
    slot_total = experts_n * capacity
    near_slots = slot_total // 2
    halves, blocks = 2, 8
    half, band = width // halves, width // blocks
    bf16, f32 = jnp.bfloat16, jnp.float32
    vmem, dma = pltpu.VMEM, pltpu.SemaphoreType.DMA
    anywhere = pl.BlockSpec(memory_space=pl.ANY)
    operands = (
        residual, conv_value, conv_gate,
        segments.reshape(-1, lanes), conv_weight,
        norm_gain[None], norm_shift[None], out_weight, ffn_gain[None],
        routes.T, route_weights.T, w_gate[0], w_up[0], w_down[0],
    )
    return pl.pallas_call(
        functools.partial(layer_kernel, experts_n, columns, capacity, blocks),
        out_shape=jax.ShapeDtypeStruct((rows_own, width), bf16),
        in_specs=[anywhere] * len(operands),
        out_specs=anywhere,
        scratch_shapes=[vmem(operand.shape, operand.dtype) for operand in operands] + [
            vmem((rows_own, width), bf16),
            vmem((3, width, local), bf16), vmem((3, width, local), bf16), vmem((3, local, width), bf16),
            vmem((2, RIM, local), bf16), vmem((tok_dev // lanes, lanes), jnp.int32),
            vmem((RIM + tok_dev, lanes), f32), vmem((RIM + tok_dev, local), f32),
            vmem((RIM + rows_own, local), f32), vmem((RIM + rows_own, lanes), f32),
            vmem((tok_dev, local), bf16), vmem((columns, rows_own, local), bf16),
            vmem((rows_own, width), f32), vmem((halves, rows_own, half), bf16),
            vmem((halves, near_slots, half), bf16), vmem((halves, slot_total, half), bf16),
            vmem((2, halves, rows_own, half), bf16), vmem((2, halves, near_slots, half), bf16),
            vmem((columns, slot_total, local), bf16), vmem((2, slot_total, local), f32),
            vmem((slot_total, band), f32),
            vmem((blocks, slot_total, band), bf16), vmem((blocks, near_slots, band), bf16),
            vmem((2, blocks, near_slots, band), bf16), vmem((2, blocks, rows_own, band), bf16),
            vmem((blocks, rows_own, band), bf16),
            vmem((3, top_count, rows_own, near_slots), bf16), vmem((3, near_slots, rows_own), bf16),
            vmem((3, top_count, rows_own, rows_own), f32),
            vmem((2, top_count, tok_dev), routes.dtype), vmem((2, top_count, tok_dev), route_weights.dtype),
            dma((len(operands),)), dma, dma((5 + blocks,)), dma, dma((3,)),
            dma, dma((5 + blocks,)), dma((3,)), dma((3,)), dma, dma,
            dma((2,)), dma((2, 2)), dma((halves,)), dma((2, halves)),
            dma, dma, dma, dma,
            dma, dma((2, blocks)), dma, dma((blocks,)), dma, dma((blocks,)), dma((blocks,)),
        ],
        compiler_params=pltpu.CompilerParams(
            collective_id=0, has_side_effects=True, vmem_limit_bytes=60 * 1024 * 1024
        ),
    )(*operands)


def solution(mesh):
    return jax.shard_map(
        shards,
        mesh=mesh,
        in_specs=(
            P(("sp", "tp"), None),
            P("sp", "tp"),
            P("sp", "tp"),
            P("sp"),
            P(None, "tp"),
            P("tp"),
            P("tp"),
            P(),
            P(),
            P("sp", None),
            P("sp", None),
            P("sp", None, "tp"),
            P("sp", None, "tp"),
            P("sp", "tp", None),
        ),
        out_specs=P(("sp", "tp"), None),
        check_vma=False,
    )
```

```python
import functools

import jax
import jax.numpy as jnp
from jax import lax
from jax.experimental import pallas as pl
from jax.experimental.pallas import tpu as pltpu
from jax.sharding import PartitionSpec as P

DC = 1024
CONV_GROUPS = 8
MESH = pl.DeviceIdType.MESH
RIM = 32


def passed_along(value, axis, steps):
    count = lax.axis_size(axis)
    initial, last = (max(0, -steps), min(count, count - steps))
    return lax.ppermute(value, axis, [(source, source + steps) for source in range(initial, last)])


def slot_numbers(block_routes, capacity, experts_n):
    route_pairs = block_routes.reshape(block_routes.shape[:-2] + (-1,))
    onehot = (route_pairs[..., None] == jnp.arange(experts_n, dtype=jnp.int32)).astype(jnp.int32)
    slot_rank = jnp.sum((jnp.cumsum(onehot, axis=-2) - onehot) * onehot, axis=-1)
    return (route_pairs * capacity + slot_rank).reshape(block_routes.shape)


def dispatch_matrix(slot_ids, slot_total):
    numbers = jnp.arange(slot_total, dtype=jnp.int32)[:, None, None]
    matches = jnp.any(numbers == slot_ids[..., None, :, :], axis=-1)
    return matches.astype(jnp.bfloat16)


def plain_shards(
    residual,
    conv_value,
    conv_gate,
    segments,
    conv_weight,
    norm_gain,
    norm_shift,
    out_weight,
    ffn_gain,
    routes,
    route_weights,
    w_gate,
    w_up,
    w_down,
):
    tok_dev, local_channels = conv_value.shape
    reach = conv_weight.shape[0] - 1
    whole_gate, whole_up = (
        lax.all_gather(w_gate[0], "tp", axis=1, tiled=True),
        lax.all_gather(w_up[0], "tp", axis=1, tiled=True),
    )
    whole_down = lax.all_gather(w_down[0], "tp", axis=0, tiled=True)
    gated = (conv_value.astype(jnp.float32) * jax.nn.sigmoid(conv_gate.astype(jnp.float32))).astype(
        jnp.bfloat16
    )
    rim_prev, seg_prev = passed_along(
        (gated[tok_dev - reach :], segments[tok_dev - reach :]), "sp", 1
    )
    extended = jnp.concatenate([rim_prev, gated], 0).astype(jnp.float32)
    seg_ext = jnp.concatenate([seg_prev, segments], 0)
    convolved = jnp.zeros((tok_dev, local_channels), jnp.float32)
    for offset in range(reach + 1):
        same_doc = (seg_ext[offset : offset + tok_dev] == segments)[:, None]
        convolved = convolved + jnp.where(
            same_doc, extended[offset : offset + tok_dev] * conv_weight[offset], 0.0
        )
    group_size = DC // CONV_GROUPS
    grouped = convolved.reshape(tok_dev, local_channels // group_size, group_size)
    group_mean = jnp.mean(grouped, axis=-1, keepdims=True)
    group_var = jnp.mean(jnp.square(grouped - group_mean), axis=-1, keepdims=True)
    scaled = ((grouped - group_mean) * lax.rsqrt(group_var + 1e-05)).reshape(
        tok_dev, local_channels
    ) * norm_gain + norm_shift
    conv_out = jax.nn.silu(scaled).astype(jnp.bfloat16)
    columns = lax.axis_size("tp")
    column = lax.axis_index("tp")
    rows_own = tok_dev // columns
    own_conv = lax.all_to_all(conv_out, "tp", split_axis=0, concat_axis=1, tiled=True)
    mixed = jnp.dot(own_conv, out_weight, preferred_element_type=jnp.float32)
    stream = residual.astype(jnp.float32) + lax.optimization_barrier(
        mixed.astype(jnp.bfloat16)
    ).astype(jnp.float32)
    normed = (
        stream * lax.rsqrt(jnp.mean(stream * stream, axis=-1, keepdims=True) + 1e-06) * ffn_gain
    ).astype(jnp.bfloat16)
    experts_n = lax.axis_size("sp")
    top_count = routes.shape[1]
    model_width = normed.shape[1]
    capacity = max(2, 2 * tok_dev * top_count // (columns * experts_n))
    slot_total = experts_n * capacity
    own_routes = lax.dynamic_slice_in_dim(routes, column * rows_own, rows_own, 0)
    own_weights = lax.dynamic_slice_in_dim(route_weights, column * rows_own, rows_own, 0)
    own_slots = slot_numbers(own_routes, capacity, experts_n)
    routing_table = dispatch_matrix(own_slots, slot_total)
    outgoing = jnp.dot(routing_table, normed, preferred_element_type=jnp.float32).astype(
        jnp.bfloat16
    )
    outgoing = outgoing.reshape(experts_n, capacity, model_width)
    arrived = lax.all_to_all(outgoing, "sp", split_axis=0, concat_axis=1, tiled=True).reshape(
        slot_total, model_width
    )
    gate_act = jnp.dot(arrived, whole_gate, preferred_element_type=jnp.float32)
    up_act = jnp.dot(arrived, whole_up, preferred_element_type=jnp.float32)
    hidden = (jax.nn.silu(gate_act) * up_act).astype(jnp.bfloat16)
    summed = jnp.dot(hidden, whole_down, preferred_element_type=jnp.float32)
    expert_out = summed.astype(jnp.bfloat16).reshape(experts_n, capacity, model_width)
    returned = lax.all_to_all(expert_out, "sp", split_axis=0, concat_axis=0, tiled=True).reshape(
        slot_total, model_width
    )
    combined = stream
    for member in range(top_count):
        chosen = jnp.take(returned, own_slots[:, member], axis=0).astype(jnp.float32)
        combined = combined + own_weights[:, member : member + 1] * chosen
    return combined.astype(jnp.bfloat16)


def flipped(index, mask):
    bit = 1
    while bit <= mask:
        if mask & bit:
            index = index + bit * (1 - 2 * ((index // bit) % 2))
        bit *= 2
    return index


def layer_kernel(
    experts_n, columns, capacity, blocks,
    residual_hbm, value_hbm, gate_hbm, seg_hbm, conv_w_hbm, gain_hbm, shift_hbm, ow_hbm, ffn_hbm,
    routes_hbm, route_w_hbm, wg_hbm, wu_hbm, wd_hbm,
    out_ref,
    residual, value, gate, seg_ref, conv_w_ref, gain_ref, shift_ref, ow, ffn_ref, routes_ref, route_w_ref,
    wg, wu, wd, wg_in, wu_in, wd_in, rim, seg_in, seg_ext, ext, win, seg_win,
    conv_out, conv_in, stream, normed, outgoing, arrived, rows_in, relay_out, hidden, silu_gate, partial,
    results, returned, relay_in, relay_sum, far_in, tables, picks, shares, routes_in, route_w_in,
    load_sem, y_send, y_recv, c_send, c_recv, f_send, f_recv, rim_send, rim_recv, x_send, x_recv,
    t_send, t_recv, far_send, far_recv, d_send, d_recv, e_recv, rd_send,
    rb_send, rb_recv, r_send, r_recv, sum_send, sum_recv,
):
    me_s, me_t = lax.axis_index("sp"), lax.axis_index("tp")
    tok_dev, local = value.shape
    width = residual.shape[1]
    rows_own = tok_dev // columns
    taps = conv_w_ref.shape[0]
    halves = normed.shape[0]
    half = width // halves
    band = width // blocks
    near_n = experts_n // 2
    near_slots = near_n * capacity
    next_s = (me_s + 1) % experts_n
    tile = 512
    group = DC // CONV_GROUPS
    level = me_s // 2
    levels = experts_n // 2
    in_middle = jnp.logical_or(level == levels // 2 - 1, level == levels // 2)
    at_end = jnp.logical_not(in_middle)

    def tp_peer(mask):
        return (me_s, flipped(me_t, mask))

    def sp_peer(mask):
        return (flipped(me_s, mask), me_t)

    loads = [
        pltpu.make_async_copy(src, dst, load_sem.at[i])
        for i, (src, dst) in enumerate((
            (value_hbm, value), (gate_hbm, gate), (seg_hbm, seg_ref), (conv_w_hbm, conv_w_ref),
            (gain_hbm, gain_ref), (shift_hbm, shift_ref), (routes_hbm, routes_ref), (route_w_hbm, route_w_ref),
            (residual_hbm, residual), (ow_hbm, ow), (ffn_hbm, ffn_ref),
            (wg_hbm, wg), (wu_hbm, wu), (wd_hbm, wd),
        ))
    ]
    conv_loads, stream_loads = 8, 11
    barrier = pltpu.get_barrier_semaphore()
    peers = [tp_peer(mask) for mask in range(1, columns)]
    peers += [sp_peer(mask) for mask in range(1, experts_n)]
    for peer in peers:
        pl.semaphore_signal(barrier, inc=1, device_id=peer, device_id_type=MESH)
    for load in loads:
        load.start()
    for load in loads[:conv_loads]:
        load.wait()
    pl.semaphore_wait(barrier, len(peers))

    def remote(src, dst, send, recv, peer):
        return pltpu.make_async_remote_copy(
            src_ref=src, dst_ref=dst, send_sem=send, recv_sem=recv,
            device_id=peer, device_id_type=MESH,
        )

    last = pl.ds(tok_dev - RIM, RIM)
    rim_copies = [
        remote(ref, dst, rim_send.at[i], rim_recv.at[i], (next_s, me_t))
        for i, (ref, dst) in enumerate(
            ((value.at[last], rim.at[0]), (gate.at[last], rim.at[1]), (seg_ref, seg_in))
        )
    ]
    for copy in rim_copies:
        copy.start()

    def across_piece(i, own, into, rows, cols):
        return (
            remote(own.at[rows, cols], into.at[1, rows, cols], y_send, y_recv.at[i], tp_peer(2)),
            remote(into.at[1, rows, cols], into.at[2, rows, cols], f_send, f_recv.at[i], tp_peer(1)),
        )

    every, first_rows, second_rows = pl.ds(0, local), width // 8, width // 16
    pieces = [
        (wg_hbm, wg_in, pl.ds(0, first_rows), every),
        (wg_hbm, wg_in, pl.ds(first_rows, second_rows), every),
        (wg_hbm, wg_in, pl.ds(first_rows + second_rows, width - first_rows - second_rows), every),
        (wu_hbm, wu_in, pl.ds(0, width // 2), every),
        (wu_hbm, wu_in, pl.ds(width // 2, width // 4), every),
        (wu_hbm, wu_in, pl.ds(3 * width // 4, width // 4), every),
    ]
    up_done = len(pieces)
    pieces += [(wd_hbm, wd_in, every, pl.ds(j * band, band)) for j in range(blocks)]
    across, forward = zip(*[across_piece(i, *piece) for i, piece in enumerate(pieces)])
    beside = [
        remote(own, into.at[0], c_send, c_recv.at[i], tp_peer(1))
        for i, (own, into) in enumerate(((wg_hbm, wg_in), (wu_hbm, wu_in), (wd_hbm, wd_in)))
    ]
    across[0].start()

    relay = jnp.where(in_middle, flipped(me_s, 6), flipped(me_s, 4))
    relay_slot = jnp.where(in_middle, 0, 1)
    route_copies = [
        remote(ref, dst.at[relay_slot], t_send.at[i], t_recv.at[relay_slot, i], (relay, me_t))
        for i, (ref, dst) in enumerate(((routes_ref, routes_in), (route_w_ref, route_w_in)))
    ]
    for copy in route_copies:
        copy.start()

    def gated_of(v, g):
        v, g = v.astype(jnp.float32), g.astype(jnp.float32)
        product = v * (1.0 / (1.0 + jnp.exp(-g)))
        return product.astype(jnp.bfloat16).astype(jnp.float32)

    def gate_rows(i, carry):
        row = pl.multiple_of(i * 64, 64)
        ext[pl.ds(row + RIM, 64), :] = gated_of(value[pl.ds(row, 64), :], gate[pl.ds(row, 64), :])
        return carry

    lax.fori_loop(0, tok_dev // 64, gate_rows, 0)
    lanes_n = seg_ref.shape[1]

    def column(row):
        return jnp.broadcast_to(row.astype(jnp.float32), (lanes_n, lanes_n)).T

    for i in range(seg_ref.shape[0]):
        seg_ext[RIM + i * lanes_n : RIM + (i + 1) * lanes_n, :] = column(seg_ref[i : i + 1, :])

    block = 64
    lead = RIM - (taps - 1)

    def conv_rows(row):
        win[...] = ext[pl.ds(row, RIM + rows_own), :]
        seg_win[...] = seg_ext[pl.ds(row, RIM + rows_own), :]
        for start in range(0, rows_own, block):
            own_seg = seg_win[start + RIM : start + RIM + block, :]
            sums = [jnp.zeros((block, group), jnp.float32) for _ in range(local // group)]
            for tap in range(taps):
                at = start + lead + tap
                same_doc = seg_win[at : at + block, :] == own_seg
                for g in range(local // group):
                    lanes = slice(g * group, (g + 1) * group)
                    term = win[at : at + block, lanes] * conv_w_ref[tap : tap + 1, lanes]
                    sums[g] = sums[g] + jnp.where(same_doc, term, 0.0)
            for g in range(local // group):
                lanes = slice(g * group, (g + 1) * group)
                mean = jnp.mean(sums[g], axis=-1, keepdims=True)
                centred = sums[g] - mean
                deviation = jnp.mean(centred * centred, axis=-1, keepdims=True)
                scaled = centred * lax.rsqrt(deviation + 1e-05) * gain_ref[:, lanes] + shift_ref[:, lanes]
                conv_out[pl.ds(row + start, block), lanes] = (scaled / (1.0 + jnp.exp(-scaled))).astype(jnp.bfloat16)

    low = me_t % 2
    masks = (3 - low, 2 + low, 1, 0)

    def conv_part(i):
        peer_row = pl.multiple_of((me_t ^ masks[i]) * rows_own, rows_own)
        conv_rows(peer_row)
        if i == 3:
            conv_in[0] = conv_out[pl.ds(peer_row, rows_own), :]
            return []
        copy = remote(
            conv_out.at[pl.ds(peer_row, rows_own)], conv_in.at[masks[i]], x_send, x_recv,
            (me_s, me_t ^ masks[i]),
        )
        copy.start()
        return [copy]

    conv_part(0)
    across[1].start()

    numbers = lax.broadcasted_iota(jnp.int32, (rows_own, lanes_n), 1).astype(jnp.float32)
    earlier = jnp.where(
        lax.broadcasted_iota(jnp.int32, (rows_own, rows_own), 0)
        > lax.broadcasted_iota(jnp.int32, (rows_own, rows_own), 1), 1.0, 0.0,
    ).astype(jnp.bfloat16)
    slot_places = lax.broadcasted_iota(jnp.int32, (rows_own, near_slots), 1)
    own_lanes = pl.ds(pl.multiple_of(me_t * rows_own, rows_own), rows_own)
    top_count = routes_ref.shape[0]

    def make_tables(which, route_row, weight_row):
        names = [column(route_row(m)) for m in range(top_count)]
        marks = [jnp.where(name == numbers, 1.0, 0.0) for name in names]
        counts = jnp.dot(earlier, sum(marks).astype(jnp.bfloat16), preferred_element_type=jnp.float32)
        total = jnp.zeros((rows_own, near_slots), jnp.float32)
        for m, mark in enumerate(marks):
            rank = jnp.sum(counts * mark, axis=-1, keepdims=True).astype(jnp.int32)
            slot = (names[m][:, 0:1].astype(jnp.int32) ^ me_s) * capacity + rank
            table = jnp.where(slot_places == slot, 1.0, 0.0)
            tables[which, m] = table.astype(jnp.bfloat16)
            total = total + table
            shares[which, m] = column(weight_row(m))
        picks[which] = total.T.astype(jnp.bfloat16)

    make_tables(
        0, lambda m: routes_ref[m : m + 1, own_lanes], lambda m: route_w_ref[m : m + 1, own_lanes]
    )

    for copy in rim_copies:
        copy.wait_recv()
    ext[pl.ds(0, RIM), :] = gated_of(rim[0], rim[1])
    before = column(seg_in[seg_ref.shape[0] - 1 : seg_ref.shape[0], :])[lanes_n - RIM :, :]
    seg_ext[0:RIM, :] = jnp.where(me_s == 0, -1.0, before)

    conv_part(1)
    for copy in across[2:]:
        copy.start()
    conv_part(2)
    for copy in beside:
        copy.start()
    conv_part(3)

    @pl.when(in_middle)
    def _():
        for slot in range(2):
            for i, ref in enumerate((routes_ref, route_w_ref)):
                dst = (routes_in, route_w_in)[i].at[slot]
                remote(ref, dst, t_send.at[i], t_recv.at[slot, i], (relay, me_t)).wait_recv()
            make_tables(
                1 + slot,
                lambda m: routes_in[slot, m : m + 1, own_lanes],
                lambda m: route_w_in[slot, m : m + 1, own_lanes],
            )

    for i in range(2):
        across[i].wait_recv()
        forward[i].start()
    for load in loads[conv_loads:stream_loads]:
        load.wait()
    swapped = remote(conv_in.at[pl.ds(1, columns - 1)], conv_in.at[pl.ds(1, columns - 1)], x_send, x_recv, tp_peer(1))
    swapped.wait_recv()

    squares = jnp.zeros((rows_own, 1), jnp.float32)
    for col in range(0, width, tile):
        cols = slice(col, col + tile)
        mixed = jnp.zeros((rows_own, tile), jnp.float32)
        for mask in range(columns):
            w_rows = pl.ds(pl.multiple_of(flipped(me_t, mask) * local, local), local)
            mixed = mixed + jnp.dot(conv_in[mask], ow[w_rows, cols], preferred_element_type=jnp.float32)
        part = residual[:, cols].astype(jnp.float32) + mixed.astype(jnp.bfloat16).astype(jnp.float32)
        stream[:, cols] = part
        squares = squares + jnp.sum(part * part, axis=-1, keepdims=True)
    scale = lax.rsqrt(squares / width + 1e-06)
    far_rows = []
    for h in range(halves):
        cols = slice(h * half, (h + 1) * half)
        normed[h] = (stream[:, cols] * scale * ffn_ref[:, cols]).astype(jnp.bfloat16)
        far_rows.append(remote(
            normed.at[h], rows_in.at[relay_slot, h], far_send.at[h], far_recv.at[relay_slot, h], (relay, me_t)
        ))
        far_rows[h].start()

    def packet(mask):
        return pl.ds(mask * capacity, capacity)

    others = pl.ds(capacity, near_slots - capacity)
    for h in range(halves):
        for col in range(0, half, tile):
            cols = slice(col, col + tile)
            outgoing[h, :, cols] = jnp.dot(
                picks[0], normed[h, :, cols], preferred_element_type=jnp.float32
            ).astype(jnp.bfloat16)
        for mask in range(near_n - 1, 0, -1):
            remote(
                outgoing.at[h, packet(mask)], arrived.at[h, packet(mask)], d_send, d_recv, sp_peer(mask)
            ).start()
        arrived[h, 0:capacity, :] = outgoing[h, 0:capacity, :]

    relay_masks = ((6, 7, 4, 5), (4, 5, 6, 7))

    def relayed(slot, m, h):
        return remote(
            relay_out.at[slot, h, packet(m)], arrived.at[h, packet(relay_masks[slot][m])],
            rd_send, e_recv, sp_peer(m),
        )

    def relay_half(slot, h):
        @pl.when(in_middle)
        def _():
            remote(
                normed.at[h], rows_in.at[slot, h], far_send.at[h], far_recv.at[slot, h], (relay, me_t)
            ).wait_recv()
            for col in range(0, half, tile):
                cols = slice(col, col + tile)
                relay_out[slot, h, :, cols] = jnp.dot(
                    picks[1 + slot], rows_in[slot, h, :, cols], preferred_element_type=jnp.float32
                ).astype(jnp.bfloat16)
            for m in (2, 3, 1):
                relayed(slot, m, h).start()
            place = relay_masks[slot][0] * capacity
            arrived[h, place : place + capacity, :] = relay_out[slot, h, 0:capacity, :]

    def landed(rows, recv):
        remote(arrived.at[:, rows], arrived.at[:, rows], d_send, recv, sp_peer(1)).wait_recv()

    for h in range(halves):
        relay_half(1, h)

    for load in loads[stream_loads:]:
        load.wait()
    for copy in beside:
        copy.wait_recv()
    across[2].wait_recv()
    forward[2].start()

    for h in range(halves):
        relay_half(0, h)

    landed(others, d_recv)

    near, far = slice(0, near_slots), slice(near_slots, 2 * near_slots)

    def act(w, rows):
        return sum(
            jnp.dot(arrived[h, rows, :], w[h * half : (h + 1) * half, :], preferred_element_type=jnp.float32)
            for h in range(halves)
        )

    def silu(v):
        return v / (1.0 + jnp.exp(-v))

    def hidden_units(mask, rows):
        g = wg if mask == 0 else wg_in.at[mask - 1]
        u = wu if mask == 0 else wu_in.at[mask - 1]
        hidden[mask, rows, :] = (silu(act(g, rows)) * act(u, rows)).astype(jnp.bfloat16)

    hidden_units(0, near)
    hidden_units(1, near)

    across[3].wait_recv()
    forward[3].start()

    @pl.when(in_middle)
    def _():
        landed(pl.ds(near_slots, 2 * capacity), e_recv)

    @pl.when(at_end)
    def _():
        landed(pl.ds(near_slots, 4 * capacity), e_recv)

    hidden_units(0, far)
    hidden_units(1, far)

    across[4].wait_recv()
    forward[4].start()

    for i in range(3):
        forward[i].wait_recv()
    for mask in (2, 3):
        for rows in (near, far):
            silu_gate[mask - 2, rows, :] = silu(act(wg_in.at[mask - 1], rows))

    across[5].wait_recv()
    forward[5].start()

    def finish_hidden(mask):
        for rows in (near, far):
            units = silu_gate[mask - 2, rows, :] * act(wu_in.at[mask - 1], rows)
            hidden[mask, rows, :] = units.astype(jnp.bfloat16)

    finish_hidden(2)

    for i in range(3, up_done):
        forward[i].wait_recv()

    finish_hidden(3)

    def to_relay(mask, m, slot, j):
        return remote(
            results.at[j, packet(mask)], relay_in.at[slot, j, packet(m)],
            rb_send, rb_recv.at[slot, j], sp_peer(m),
        )

    from_middle = ((7, 1, 0), (5, 1, 1))
    from_end = ((4, 2, 0), (6, 2, 1), (5, 3, 0), (7, 3, 1))
    kept = ((6, 0), (4, 1))
    give_back = {
        (mask, j): remote(
            results.at[j, packet(mask)], returned.at[j, packet(mask)],
            r_send, r_recv.at[j], sp_peer(mask),
        )
        for j in range(blocks) for mask in range(1, near_n)
    }

    def band_results(j):
        cols = slice(j * band, (j + 1) * band)
        across[up_done + j].wait_recv()
        forward[up_done + j].start()

        def down(mask):
            w = wd[:, cols] if mask == 0 else wd_in[mask - 1, :, cols]
            return jnp.dot(hidden[mask], w, preferred_element_type=jnp.float32)

        partial[...] = down(0) + down(1) + down(2)
        forward[up_done + j].wait_recv()
        results[j] = (partial[...] + down(3)).astype(jnp.bfloat16)

        @pl.when(in_middle)
        def _():
            for mask, m, slot in from_middle:
                to_relay(mask, m, slot, j).start()
            for mask, slot in kept:
                relay_in[slot, j, 0:capacity, :] = results[j, mask * capacity : (mask + 1) * capacity, :]

        @pl.when(at_end)
        def _():
            for mask, m, slot in from_end:
                to_relay(mask, m, slot, j).start()

        returned[j, 0:capacity, :] = results[j, 0:capacity, :]

    def direct(j, masks):
        for mask in masks:
            give_back[mask, j].start()

    def summed_up(slot, j):
        return remote(
            relay_sum.at[slot, j], far_in.at[j], sum_send, sum_recv.at[j],
            sp_peer((6, 4)[slot]),
        )

    def weighed(which, packets):
        return sum(
            shares[which, m][:, 0:1] * jnp.dot(tables[which, m], packets, preferred_element_type=jnp.float32)
            for m in range(top_count)
        )

    def relay_band(j):
        @pl.when(in_middle)
        def _():
            for slot in range(2):
                remote(
                    relay_in.at[slot, j, others], relay_in.at[slot, j, others],
                    rb_send, rb_recv.at[slot, j], sp_peer(1),
                ).wait_recv()
                relay_sum[slot, j] = weighed(1 + slot, relay_in[slot, j]).astype(jnp.bfloat16)
                summed_up(slot, j).start()

    early, lag = blocks // 4, blocks // 2
    for j in range(blocks):
        band_results(j)
        pl.when(in_middle)(functools.partial(direct, j, (3, 2)))
        if j < early:
            pl.when(at_end)(functools.partial(direct, j, (3, 2)))
        if j >= lag:
            relay_band(j - lag)
    for j in range(blocks):
        if j >= early:
            pl.when(at_end)(functools.partial(direct, j, (3, 2)))
        direct(j, (1,))
    for j in range(blocks - lag, blocks):
        relay_band(j)

    def finish(j):
        cols = slice(j * band, (j + 1) * band)
        remote(
            relay_sum.at[0, j], far_in.at[j], sum_send, sum_recv.at[j], (relay, me_t)
        ).wait_recv()
        remote(
            returned.at[j, others], returned.at[j, others], r_send, r_recv.at[j], sp_peer(1)
        ).wait_recv()
        total = stream[:, cols] + weighed(0, returned[j]) + far_in[j].astype(jnp.float32)
        out_ref[:, cols] = total.astype(jnp.bfloat16)

    for j in range(blocks // 2):
        finish(j)
    for j in range(blocks // 2, blocks):
        finish(j)

    def sent(ref, sem):
        remote(ref, ref, sem, sem, sp_peer(1)).wait_send()

    for copy in rim_copies + route_copies + far_rows:
        copy.wait_send()
    for sem in (y_send, f_send, c_send):
        sent(wg_in, sem)
    swapped.wait_send()
    sent(outgoing.at[:, others], d_send)
    sent(results.at[:, others], r_send)

    @pl.when(in_middle)
    def _():
        sent(relay_out.at[:, :, others], rd_send)
        sent(relay_sum, sum_send)
        sent(results.at[:, pl.ds(0, 2 * capacity)], rb_send)

    @pl.when(at_end)
    def _():
        sent(results.at[:, pl.ds(0, 4 * capacity)], rb_send)


def shards(*args):
    (residual, conv_value, conv_gate, segments, conv_weight, norm_gain, norm_shift, out_weight,
     ffn_gain, routes, route_weights, w_gate, w_up, w_down) = args
    tok_dev, local = conv_value.shape
    width = residual.shape[1]
    experts_n, columns = lax.axis_size("sp"), lax.axis_size("tp")
    top_count = routes.shape[1]
    capacity = max(2, 2 * tok_dev * top_count // (columns * experts_n))
    if capacity % 32 or columns != 4 or tok_dev != columns * 128 or experts_n != 8:
        return plain_shards(*args)
    rows_own = tok_dev // columns
    lanes = DC // CONV_GROUPS
    slot_total = experts_n * capacity
    near_slots = slot_total // 2
    halves, blocks = 2, 8
    half, band = width // halves, width // blocks
    bf16, f32 = jnp.bfloat16, jnp.float32
    vmem, dma = pltpu.VMEM, pltpu.SemaphoreType.DMA
    anywhere = pl.BlockSpec(memory_space=pl.ANY)
    operands = (
        residual, conv_value, conv_gate,
        segments.reshape(-1, lanes), conv_weight,
        norm_gain[None], norm_shift[None], out_weight, ffn_gain[None],
        routes.T, route_weights.T, w_gate[0], w_up[0], w_down[0],
    )
    return pl.pallas_call(
        functools.partial(layer_kernel, experts_n, columns, capacity, blocks),
        out_shape=pltpu.VMEM((rows_own, width), bf16),
        in_specs=[anywhere] * len(operands),
        out_specs=pl.BlockSpec(memory_space=pltpu.VMEM),
        scratch_shapes=[vmem(operand.shape, operand.dtype) for operand in operands] + [
            vmem((3, width, local), bf16), vmem((3, width, local), bf16), vmem((3, local, width), bf16),
            vmem((2, RIM, local), bf16), vmem((tok_dev // lanes, lanes), jnp.int32),
            vmem((RIM + tok_dev, lanes), f32), vmem((RIM + tok_dev, local), f32),
            vmem((RIM + rows_own, local), f32), vmem((RIM + rows_own, lanes), f32),
            vmem((tok_dev, local), bf16), vmem((columns, rows_own, local), bf16),
            vmem((rows_own, width), f32), vmem((halves, rows_own, half), bf16),
            vmem((halves, near_slots, half), bf16), vmem((halves, slot_total, half), bf16),
            vmem((2, halves, rows_own, half), bf16), vmem((2, halves, near_slots, half), bf16),
            vmem((columns, slot_total, local), bf16), vmem((2, slot_total, local), f32),
            vmem((slot_total, band), f32),
            vmem((blocks, slot_total, band), bf16), vmem((blocks, near_slots, band), bf16),
            vmem((2, blocks, near_slots, band), bf16), vmem((2, blocks, rows_own, band), bf16),
            vmem((blocks, rows_own, band), bf16),
            vmem((3, top_count, rows_own, near_slots), bf16), vmem((3, near_slots, rows_own), bf16),
            vmem((3, top_count, rows_own, rows_own), f32),
            vmem((2, top_count, tok_dev), routes.dtype), vmem((2, top_count, tok_dev), route_weights.dtype),
            dma((len(operands),)), dma, dma((6 + blocks,)), dma, dma((3,)),
            dma, dma((6 + blocks,)), dma((3,)), dma((3,)), dma, dma,
            dma((2,)), dma((2, 2)), dma((halves,)), dma((2, halves)),
            dma, dma, dma, dma,
            dma, dma((2, blocks)), dma, dma((blocks,)), dma, dma((blocks,)),
        ],
        compiler_params=pltpu.CompilerParams(
            collective_id=0, has_side_effects=True, vmem_limit_bytes=60 * 1024 * 1024
        ),
    )(*operands)


def solution(mesh):
    return jax.shard_map(
        shards,
        mesh=mesh,
        in_specs=(
            P(("sp", "tp"), None),
            P("sp", "tp"),
            P("sp", "tp"),
            P("sp"),
            P(None, "tp"),
            P("tp"),
            P("tp"),
            P(),
            P(),
            P("sp", None),
            P("sp", None),
            P("sp", None, "tp"),
            P("sp", None, "tp"),
            P("sp", "tp", None),
        ),
        out_specs=P(("sp", "tp"), None),
        check_vma=False,
    )
```

```python
import functools

import jax
import jax.numpy as jnp
from jax import lax
from jax.experimental import pallas as pl
from jax.experimental.pallas import tpu as pltpu
from jax.sharding import PartitionSpec as P

DC = 1024
CONV_GROUPS = 8
MESH = pl.DeviceIdType.MESH
RIM = 32


def passed_along(value, axis, steps):
    count = lax.axis_size(axis)
    initial, last = (max(0, -steps), min(count, count - steps))
    return lax.ppermute(value, axis, [(source, source + steps) for source in range(initial, last)])


def slot_numbers(block_routes, capacity, experts_n):
    route_pairs = block_routes.reshape(block_routes.shape[:-2] + (-1,))
    onehot = (route_pairs[..., None] == jnp.arange(experts_n, dtype=jnp.int32)).astype(jnp.int32)
    slot_rank = jnp.sum((jnp.cumsum(onehot, axis=-2) - onehot) * onehot, axis=-1)
    return (route_pairs * capacity + slot_rank).reshape(block_routes.shape)


def dispatch_matrix(slot_ids, slot_total):
    numbers = jnp.arange(slot_total, dtype=jnp.int32)[:, None, None]
    matches = jnp.any(numbers == slot_ids[..., None, :, :], axis=-1)
    return matches.astype(jnp.bfloat16)


def plain_shards(
    residual,
    conv_value,
    conv_gate,
    segments,
    conv_weight,
    norm_gain,
    norm_shift,
    out_weight,
    ffn_gain,
    routes,
    route_weights,
    w_gate,
    w_up,
    w_down,
):
    tok_dev, local_channels = conv_value.shape
    reach = conv_weight.shape[0] - 1
    whole_gate, whole_up = (
        lax.all_gather(w_gate[0], "tp", axis=1, tiled=True),
        lax.all_gather(w_up[0], "tp", axis=1, tiled=True),
    )
    whole_down = lax.all_gather(w_down[0], "tp", axis=0, tiled=True)
    gated = (conv_value.astype(jnp.float32) * jax.nn.sigmoid(conv_gate.astype(jnp.float32))).astype(
        jnp.bfloat16
    )
    rim_prev, seg_prev = passed_along(
        (gated[tok_dev - reach :], segments[tok_dev - reach :]), "sp", 1
    )
    extended = jnp.concatenate([rim_prev, gated], 0).astype(jnp.float32)
    seg_ext = jnp.concatenate([seg_prev, segments], 0)
    convolved = jnp.zeros((tok_dev, local_channels), jnp.float32)
    for offset in range(reach + 1):
        same_doc = (seg_ext[offset : offset + tok_dev] == segments)[:, None]
        convolved = convolved + jnp.where(
            same_doc, extended[offset : offset + tok_dev] * conv_weight[offset], 0.0
        )
    group_size = DC // CONV_GROUPS
    grouped = convolved.reshape(tok_dev, local_channels // group_size, group_size)
    group_mean = jnp.mean(grouped, axis=-1, keepdims=True)
    group_var = jnp.mean(jnp.square(grouped - group_mean), axis=-1, keepdims=True)
    scaled = ((grouped - group_mean) * lax.rsqrt(group_var + 1e-05)).reshape(
        tok_dev, local_channels
    ) * norm_gain + norm_shift
    conv_out = jax.nn.silu(scaled).astype(jnp.bfloat16)
    columns = lax.axis_size("tp")
    column = lax.axis_index("tp")
    rows_own = tok_dev // columns
    own_conv = lax.all_to_all(conv_out, "tp", split_axis=0, concat_axis=1, tiled=True)
    mixed = jnp.dot(own_conv, out_weight, preferred_element_type=jnp.float32)
    stream = residual.astype(jnp.float32) + lax.optimization_barrier(
        mixed.astype(jnp.bfloat16)
    ).astype(jnp.float32)
    normed = (
        stream * lax.rsqrt(jnp.mean(stream * stream, axis=-1, keepdims=True) + 1e-06) * ffn_gain
    ).astype(jnp.bfloat16)
    experts_n = lax.axis_size("sp")
    top_count = routes.shape[1]
    model_width = normed.shape[1]
    capacity = max(2, 2 * tok_dev * top_count // (columns * experts_n))
    slot_total = experts_n * capacity
    own_routes = lax.dynamic_slice_in_dim(routes, column * rows_own, rows_own, 0)
    own_weights = lax.dynamic_slice_in_dim(route_weights, column * rows_own, rows_own, 0)
    own_slots = slot_numbers(own_routes, capacity, experts_n)
    routing_table = dispatch_matrix(own_slots, slot_total)
    outgoing = jnp.dot(routing_table, normed, preferred_element_type=jnp.float32).astype(
        jnp.bfloat16
    )
    outgoing = outgoing.reshape(experts_n, capacity, model_width)
    arrived = lax.all_to_all(outgoing, "sp", split_axis=0, concat_axis=1, tiled=True).reshape(
        slot_total, model_width
    )
    gate_act = jnp.dot(arrived, whole_gate, preferred_element_type=jnp.float32)
    up_act = jnp.dot(arrived, whole_up, preferred_element_type=jnp.float32)
    hidden = (jax.nn.silu(gate_act) * up_act).astype(jnp.bfloat16)
    summed = jnp.dot(hidden, whole_down, preferred_element_type=jnp.float32)
    expert_out = summed.astype(jnp.bfloat16).reshape(experts_n, capacity, model_width)
    returned = lax.all_to_all(expert_out, "sp", split_axis=0, concat_axis=0, tiled=True).reshape(
        slot_total, model_width
    )
    combined = stream
    for member in range(top_count):
        chosen = jnp.take(returned, own_slots[:, member], axis=0).astype(jnp.float32)
        combined = combined + own_weights[:, member : member + 1] * chosen
    return combined.astype(jnp.bfloat16)


def flipped(index, mask):
    bit = 1
    while bit <= mask:
        if mask & bit:
            index = index + bit * (1 - 2 * ((index // bit) % 2))
        bit *= 2
    return index


def layer_kernel(
    experts_n, columns, capacity, widths,
    residual_hbm, value_hbm, gate_hbm, seg_hbm, conv_w_hbm, gain_hbm, shift_hbm, ow_hbm, ffn_hbm,
    routes_hbm, route_w_hbm, wg_hbm, wu_hbm, wd_hbm,
    out_ref,
    residual, value, gate, seg_ref, conv_w_ref, gain_ref, shift_ref, ow, ffn_ref, routes_ref, route_w_ref,
    wg, wu, wd, wg_in, wu_in, wd_in, rim, seg_in, seg_ext, ext, win, seg_win,
    conv_out, conv_in, stream, normed, outgoing, arrived, rows_in, relay_out, hidden, silu_gate, partial,
    results, returned, relay_in, relay_sum, far_in, help_in, pass_in, tables, picks, shares, routes_in, route_w_in,
    load_sem, y_send, y_recv, c_send, c_recv, f_send, f_recv, rim_send, rim_recv, x_send, x_recv,
    t_send, t_recv, far_send, far_recv, d_send, d_recv, e_recv, rd_send,
    rb_send, rb_recv, r_send, r_recv, sum_send, sum_recv, h_send, h_recv, p_recv, q_send,
):
    me_s, me_t = lax.axis_index("sp"), lax.axis_index("tp")
    tok_dev, local = value.shape
    width = residual.shape[1]
    rows_own = tok_dev // columns
    taps = conv_w_ref.shape[0]
    halves = normed.shape[0]
    half = width // halves
    blocks = len(widths)
    bands = [pl.ds(sum(widths[:j]), widths[j]) for j in range(blocks)]
    near_n = experts_n // 2
    near_slots = near_n * capacity
    next_s = (me_s + 1) % experts_n
    tile = 512
    group = DC // CONV_GROUPS
    level = me_s // 2
    levels = experts_n // 2
    in_middle = jnp.logical_or(level == levels // 2 - 1, level == levels // 2)
    at_end = jnp.logical_not(in_middle)

    def tp_peer(mask):
        return (me_s, flipped(me_t, mask))

    def sp_peer(mask):
        return (flipped(me_s, mask), me_t)

    loads = [
        pltpu.make_async_copy(src, dst, load_sem.at[i])
        for i, (src, dst) in enumerate((
            (value_hbm, value), (gate_hbm, gate), (seg_hbm, seg_ref), (conv_w_hbm, conv_w_ref),
            (gain_hbm, gain_ref), (shift_hbm, shift_ref), (routes_hbm, routes_ref), (route_w_hbm, route_w_ref),
            (residual_hbm, residual), (ow_hbm, ow), (ffn_hbm, ffn_ref),
            (wg_hbm, wg), (wu_hbm, wu), (wd_hbm, wd),
        ))
    ]
    conv_loads, stream_loads = 8, 11
    barrier = pltpu.get_barrier_semaphore()
    peers = [tp_peer(mask) for mask in range(1, columns)]
    peers += [sp_peer(mask) for mask in range(1, experts_n)]
    peers.append((flipped(me_s, 2), flipped(me_t, 2)))
    for peer in peers:
        pl.semaphore_signal(barrier, inc=1, device_id=peer, device_id_type=MESH)
    for load in loads:
        load.start()
    for load in loads[:conv_loads]:
        load.wait()
    pl.semaphore_wait(barrier, len(peers))

    def remote(src, dst, send, recv, peer):
        return pltpu.make_async_remote_copy(
            src_ref=src, dst_ref=dst, send_sem=send, recv_sem=recv,
            device_id=peer, device_id_type=MESH,
        )

    last = pl.ds(tok_dev - RIM, RIM)
    rim_copies = [
        remote(ref, dst, rim_send.at[i], rim_recv.at[i], (next_s, me_t))
        for i, (ref, dst) in enumerate(
            ((value.at[last], rim.at[0]), (gate.at[last], rim.at[1]), (seg_ref, seg_in))
        )
    ]
    for copy in rim_copies:
        copy.start()

    def across_piece(i, own, into, rows, cols):
        return (
            remote(own.at[rows, cols], into.at[1, rows, cols], y_send, y_recv.at[i], tp_peer(2)),
            remote(into.at[1, rows, cols], into.at[2, rows, cols], f_send, f_recv.at[i], tp_peer(1)),
        )

    every, first_rows, second_rows = pl.ds(0, local), width // 8, width // 16
    helped = help_in.shape[0] * help_in.shape[1]
    pieces = [
        (wg_hbm, wg_in, pl.ds(0, first_rows), every),
        (wg_hbm, wg_in, pl.ds(first_rows, second_rows), every),
        (wg_hbm, wg_in, pl.ds(first_rows + second_rows, width - first_rows - second_rows), every),
        (wu_hbm, wu_in, pl.ds(0, width // 2), every),
        (wu_hbm, wu_in, pl.ds(width // 2, width // 4), every),
        (wu_hbm, wu_in, pl.ds(3 * width // 4, width // 4 - helped), every),
        (wu_hbm, wu_in, pl.ds(width - helped, helped), every),
    ]
    up_done = len(pieces)
    detour = up_done - 1
    pieces += [(wd_hbm, wd_in, every, bands[j]) for j in range(blocks)]
    across, forward = zip(*[across_piece(i, *piece) for i, piece in enumerate(pieces)])
    beside = [
        remote(own, into.at[0], c_send, c_recv.at[i], tp_peer(1))
        for i, (own, into) in enumerate(((wg_hbm, wg_in), (wu_hbm, wu_in), (wd_hbm, wd_in)))
    ]
    across[0].start()
    parts = help_in.shape[0]

    def helper(k, back):
        rows = pl.ds(width - helped + k * (helped // parts), helped // parts)
        if back:
            return remote(help_in.at[k], wu_in.at[1, rows], h_send, y_recv.at[detour], sp_peer(2))
        return remote(
            wu_hbm.at[rows], help_in.at[k], y_send, h_recv.at[k], (flipped(me_s, 2), flipped(me_t, 2))
        )

    @pl.when(at_end)
    def _():
        for k in range(parts):
            helper(k, False).start()

    relay = jnp.where(in_middle, flipped(me_s, 6), flipped(me_s, 4))
    relay_slot = jnp.where(in_middle, 0, 1)
    route_copies = [
        remote(ref, dst.at[relay_slot], t_send.at[i], t_recv.at[relay_slot, i], (relay, me_t))
        for i, (ref, dst) in enumerate(((routes_ref, routes_in), (route_w_ref, route_w_in)))
    ]
    for copy in route_copies:
        copy.start()

    def gated_of(v, g):
        v, g = v.astype(jnp.float32), g.astype(jnp.float32)
        product = v * (1.0 / (1.0 + jnp.exp(-g)))
        return product.astype(jnp.bfloat16).astype(jnp.float32)

    def gate_rows(i, carry):
        row = pl.multiple_of(i * 64, 64)
        ext[pl.ds(row + RIM, 64), :] = gated_of(value[pl.ds(row, 64), :], gate[pl.ds(row, 64), :])
        return carry

    lax.fori_loop(0, tok_dev // 64, gate_rows, 0)
    lanes_n = seg_ref.shape[1]

    def column(row):
        return jnp.broadcast_to(row.astype(jnp.float32), (lanes_n, lanes_n)).T

    for i in range(seg_ref.shape[0]):
        seg_ext[RIM + i * lanes_n : RIM + (i + 1) * lanes_n, :] = column(seg_ref[i : i + 1, :])

    block = 64
    lead = RIM - (taps - 1)

    def conv_rows(row):
        win[...] = ext[pl.ds(row, RIM + rows_own), :]
        seg_win[...] = seg_ext[pl.ds(row, RIM + rows_own), :]
        for start in range(0, rows_own, block):
            own_seg = seg_win[start + RIM : start + RIM + block, :]
            sums = [jnp.zeros((block, group), jnp.float32) for _ in range(local // group)]
            for tap in range(taps):
                at = start + lead + tap
                same_doc = seg_win[at : at + block, :] == own_seg
                for g in range(local // group):
                    lanes = slice(g * group, (g + 1) * group)
                    term = win[at : at + block, lanes] * conv_w_ref[tap : tap + 1, lanes]
                    sums[g] = sums[g] + jnp.where(same_doc, term, 0.0)
            for g in range(local // group):
                lanes = slice(g * group, (g + 1) * group)
                mean = jnp.mean(sums[g], axis=-1, keepdims=True)
                centred = sums[g] - mean
                deviation = jnp.mean(centred * centred, axis=-1, keepdims=True)
                scaled = centred * lax.rsqrt(deviation + 1e-05) * gain_ref[:, lanes] + shift_ref[:, lanes]
                conv_out[pl.ds(row + start, block), lanes] = (scaled / (1.0 + jnp.exp(-scaled))).astype(jnp.bfloat16)

    low = me_t % 2
    masks = (3 - low, 2 + low, 1, 0)

    def conv_part(i):
        peer_row = pl.multiple_of((me_t ^ masks[i]) * rows_own, rows_own)
        conv_rows(peer_row)
        if i == 3:
            conv_in[0] = conv_out[pl.ds(peer_row, rows_own), :]
            return []
        copy = remote(
            conv_out.at[pl.ds(peer_row, rows_own)], conv_in.at[masks[i]], x_send, x_recv,
            (me_s, me_t ^ masks[i]),
        )
        copy.start()
        return [copy]

    conv_part(0)
    pl.when(at_end)(across[1].start)

    numbers = lax.broadcasted_iota(jnp.int32, (rows_own, lanes_n), 1).astype(jnp.float32)
    earlier = jnp.where(
        lax.broadcasted_iota(jnp.int32, (rows_own, rows_own), 0)
        > lax.broadcasted_iota(jnp.int32, (rows_own, rows_own), 1), 1.0, 0.0,
    ).astype(jnp.bfloat16)
    slot_places = lax.broadcasted_iota(jnp.int32, (rows_own, near_slots), 1)
    own_lanes = pl.ds(pl.multiple_of(me_t * rows_own, rows_own), rows_own)
    top_count = routes_ref.shape[0]

    def make_tables(which, route_row, weight_row):
        names = [column(route_row(m)) for m in range(top_count)]
        marks = [jnp.where(name == numbers, 1.0, 0.0) for name in names]
        counts = jnp.dot(earlier, sum(marks).astype(jnp.bfloat16), preferred_element_type=jnp.float32)
        total = jnp.zeros((rows_own, near_slots), jnp.float32)
        for m, mark in enumerate(marks):
            rank = jnp.sum(counts * mark, axis=-1, keepdims=True).astype(jnp.int32)
            slot = (names[m][:, 0:1].astype(jnp.int32) ^ me_s) * capacity + rank
            table = jnp.where(slot_places == slot, 1.0, 0.0)
            tables[which, m] = table.astype(jnp.bfloat16)
            total = total + table
            shares[which, m] = column(weight_row(m))
        picks[which] = total.T.astype(jnp.bfloat16)

    make_tables(
        0, lambda m: routes_ref[m : m + 1, own_lanes], lambda m: route_w_ref[m : m + 1, own_lanes]
    )

    for copy in rim_copies:
        copy.wait_recv()
    ext[pl.ds(0, RIM), :] = gated_of(rim[0], rim[1])
    before = column(seg_in[seg_ref.shape[0] - 1 : seg_ref.shape[0], :])[lanes_n - RIM :, :]
    seg_ext[0:RIM, :] = jnp.where(me_s == 0, -1.0, before)

    conv_part(1)
    for i in range(1, len(pieces)):
        if i == 1 or i == detour:
            pl.when(in_middle)(across[i].start)
        else:
            across[i].start()
    conv_part(2)
    for copy in beside:
        copy.start()
    conv_part(3)

    @pl.when(in_middle)
    def _():
        for slot in range(2):
            for i, ref in enumerate((routes_ref, route_w_ref)):
                dst = (routes_in, route_w_in)[i].at[slot]
                remote(ref, dst, t_send.at[i], t_recv.at[slot, i], (relay, me_t)).wait_recv()
            make_tables(
                1 + slot,
                lambda m: routes_in[slot, m : m + 1, own_lanes],
                lambda m: route_w_in[slot, m : m + 1, own_lanes],
            )

    @pl.when(in_middle)
    def _():
        for k in range(parts):
            helper(k, False).wait_recv()
            helper(k, True).start()

    def pass_first():
        for i in range(2):
            across[i].wait_recv()
            forward[i].start()

    pl.when(at_end)(pass_first)
    for load in loads[conv_loads:stream_loads]:
        load.wait()
    swapped = remote(conv_in.at[pl.ds(1, columns - 1)], conv_in.at[pl.ds(1, columns - 1)], x_send, x_recv, tp_peer(1))
    swapped.wait_recv()

    squares = jnp.zeros((rows_own, 1), jnp.float32)
    for col in range(0, width, tile):
        cols = slice(col, col + tile)
        mixed = jnp.zeros((rows_own, tile), jnp.float32)
        for mask in range(columns):
            w_rows = pl.ds(pl.multiple_of(flipped(me_t, mask) * local, local), local)
            mixed = mixed + jnp.dot(conv_in[mask], ow[w_rows, cols], preferred_element_type=jnp.float32)
        part = residual[:, cols].astype(jnp.float32) + mixed.astype(jnp.bfloat16).astype(jnp.float32)
        stream[:, cols] = part
        squares = squares + jnp.sum(part * part, axis=-1, keepdims=True)
    scale = lax.rsqrt(squares / width + 1e-06)
    far_rows = []
    for h in range(halves):
        cols = slice(h * half, (h + 1) * half)
        normed[h] = (stream[:, cols] * scale * ffn_ref[:, cols]).astype(jnp.bfloat16)
        far_rows.append(remote(
            normed.at[h], rows_in.at[relay_slot, h], far_send.at[h], far_recv.at[relay_slot, h], (relay, me_t)
        ))
        far_rows[h].start()

    def packet(mask):
        return pl.ds(mask * capacity, capacity)

    others = pl.ds(capacity, near_slots - capacity)
    for h in range(halves):
        for col in range(0, half, tile):
            cols = slice(col, col + tile)
            outgoing[h, :, cols] = jnp.dot(
                picks[0], normed[h, :, cols], preferred_element_type=jnp.float32
            ).astype(jnp.bfloat16)
        for mask in range(near_n - 1, 0, -1):
            remote(
                outgoing.at[h, packet(mask)], arrived.at[h, packet(mask)], d_send, d_recv, sp_peer(mask)
            ).start()
        arrived[h, 0:capacity, :] = outgoing[h, 0:capacity, :]

    relay_masks = ((6, 7, 4, 5), (4, 5, 6, 7))

    def relayed(slot, m, h):
        return remote(
            relay_out.at[slot, h, packet(m)], arrived.at[h, packet(relay_masks[slot][m])],
            rd_send, e_recv, sp_peer(m),
        )

    def relay_half(slot, h):
        @pl.when(in_middle)
        def _():
            remote(
                normed.at[h], rows_in.at[slot, h], far_send.at[h], far_recv.at[slot, h], (relay, me_t)
            ).wait_recv()
            for col in range(0, half, tile):
                cols = slice(col, col + tile)
                relay_out[slot, h, :, cols] = jnp.dot(
                    picks[1 + slot], rows_in[slot, h, :, cols], preferred_element_type=jnp.float32
                ).astype(jnp.bfloat16)
            for m in (2, 3, 1):
                relayed(slot, m, h).start()
            place = relay_masks[slot][0] * capacity
            arrived[h, place : place + capacity, :] = relay_out[slot, h, 0:capacity, :]

    def landed(rows, recv):
        remote(arrived.at[:, rows], arrived.at[:, rows], d_send, recv, sp_peer(1)).wait_recv()

    for h in range(halves):
        relay_half(1, h)

    for load in loads[stream_loads:]:
        load.wait()
    for copy in beside:
        copy.wait_recv()
    relay_half(0, 0)
    pl.when(in_middle)(pass_first)
    across[2].wait_recv()
    forward[2].start()

    def pass_detour():
        across[detour].wait_recv()
        forward[detour].start()

    pl.when(at_end)(pass_detour)

    for h in range(1, halves):
        relay_half(0, h)

    landed(others, d_recv)

    near, far = slice(0, near_slots), slice(near_slots, 2 * near_slots)

    def act(w, rows):
        return sum(
            jnp.dot(arrived[h, rows, :], w[h * half : (h + 1) * half, :], preferred_element_type=jnp.float32)
            for h in range(halves)
        )

    def silu(v):
        return v / (1.0 + jnp.exp(-v))

    def hidden_units(mask, rows):
        g = wg if mask == 0 else wg_in.at[mask - 1]
        u = wu if mask == 0 else wu_in.at[mask - 1]
        hidden[mask, rows, :] = (silu(act(g, rows)) * act(u, rows)).astype(jnp.bfloat16)

    hidden_units(0, near)
    hidden_units(1, near)

    across[3].wait_recv()
    forward[3].start()

    @pl.when(in_middle)
    def _():
        landed(pl.ds(near_slots, 2 * capacity), e_recv)

    @pl.when(at_end)
    def _():
        landed(pl.ds(near_slots, 4 * capacity), e_recv)

    hidden_units(0, far)
    hidden_units(1, far)

    across[4].wait_recv()
    forward[4].start()

    for i in range(3):
        forward[i].wait_recv()
    for mask in (2, 3):
        for rows in (near, far):
            silu_gate[mask - 2, rows, :] = silu(act(wg_in.at[mask - 1], rows))

    across[5].wait_recv()
    forward[5].start()
    pl.when(in_middle)(pass_detour)

    def finish_hidden(mask):
        for rows in (near, far):
            units = silu_gate[mask - 2, rows, :] * act(wu_in.at[mask - 1], rows)
            hidden[mask, rows, :] = units.astype(jnp.bfloat16)

    finish_hidden(2)

    for i in range(3, up_done):
        forward[i].wait_recv()

    finish_hidden(3)

    def to_relay(mask, m, slot, j):
        return remote(
            results.at[packet(mask), bands[j]], relay_in.at[slot, packet(m), bands[j]],
            rb_send, rb_recv.at[slot, j], sp_peer(m),
        )

    from_middle = ((7, 1, 0), (5, 1, 1))
    from_end = ((4, 2, 0), (6, 2, 1), (5, 3, 0), (7, 3, 1))
    kept = ((6, 0), (4, 1))
    give_back = {
        (mask, j): remote(
            results.at[packet(mask), bands[j]], returned.at[packet(mask), bands[j]],
            r_send, r_recv.at[j], sp_peer(mask),
        )
        for j in range(blocks) for mask in range(1, near_n)
    }

    def pass_on(j):
        return remote(
            results.at[packet(3), bands[j]], pass_in.at[:, bands[j]], r_send, p_recv, sp_peer(1)
        )

    def passed(j):
        return remote(
            pass_in.at[:, bands[j]], returned.at[packet(3), bands[j]], q_send, r_recv.at[j], sp_peer(2)
        )

    def band_results(j):
        cols, span = bands[j], slice(0, widths[j])
        across[up_done + j].wait_recv()
        forward[up_done + j].start()

        def down(mask):
            w = wd[:, cols] if mask == 0 else wd_in[mask - 1, :, cols]
            return jnp.dot(hidden[mask], w, preferred_element_type=jnp.float32)

        partial[:, span] = down(0) + down(1) + down(2)
        forward[up_done + j].wait_recv()
        results[:, cols] = (partial[:, span] + down(3)).astype(jnp.bfloat16)

        @pl.when(in_middle)
        def _():
            for mask, m, slot in from_middle:
                to_relay(mask, m, slot, j).start()
            for mask, slot in kept:
                relay_in[slot, 0:capacity, cols] = results[mask * capacity : (mask + 1) * capacity, cols]

        @pl.when(at_end)
        def _():
            for mask, m, slot in from_end:
                to_relay(mask, m, slot, j).start()
            pass_on(j).start()
            give_back[1, j].start()

        returned[0:capacity, cols] = results[0:capacity, cols]

    def direct(j, masks):
        for mask in masks:
            give_back[mask, j].start()

    def summed_up(slot, j):
        return remote(
            relay_sum.at[slot, :, bands[j]], far_in.at[:, bands[j]], sum_send, sum_recv.at[j],
            sp_peer((6, 4)[slot]),
        )

    def weighed(which, packets):
        return sum(
            shares[which, m][:, 0:1] * jnp.dot(tables[which, m], packets, preferred_element_type=jnp.float32)
            for m in range(top_count)
        )

    def relay_band(j):
        @pl.when(in_middle)
        def _():
            for slot in range(2):
                remote(
                    relay_in.at[slot, others, bands[j]], relay_in.at[slot, others, bands[j]],
                    rb_send, rb_recv.at[slot, j], sp_peer(1),
                ).wait_recv()
                relay_sum[slot, :, bands[j]] = weighed(1 + slot, relay_in[slot, :, bands[j]]).astype(jnp.bfloat16)
                summed_up(slot, j).start()

    early, summed, ends = blocks // 4, 0, [sum(widths[: j + 1]) for j in range(blocks)]
    for j in range(blocks):
        band_results(j)
        pl.when(in_middle)(functools.partial(direct, j, (3, 2)))
        if j < early:
            pl.when(at_end)(functools.partial(direct, j, (2,)))
        while ends[summed] + max(widths) <= ends[j]:
            relay_band(summed)
            summed += 1

    @pl.when(in_middle)
    def _():
        for j in range(blocks):
            direct(j, (1,))

    @pl.when(at_end)
    def _():
        for j in range(early, blocks):
            direct(j, (2,))
        remote(pass_in, pass_in, r_send, p_recv, sp_peer(1)).wait_recv()
        for j in range(blocks):
            passed(j).start()

    for j in range(summed, blocks):
        relay_band(j)

    def finish(j):
        cols = bands[j]
        remote(
            relay_sum.at[0, :, cols], far_in.at[:, cols], sum_send, sum_recv.at[j], (relay, me_t)
        ).wait_recv()
        remote(
            returned.at[others, cols], returned.at[others, cols], r_send, r_recv.at[j], sp_peer(1)
        ).wait_recv()
        total = stream[:, cols] + weighed(0, returned[:, cols]) + far_in[:, cols].astype(jnp.float32)
        out_ref[:, cols] = total.astype(jnp.bfloat16)

    for j in range(blocks // 2):
        finish(j)
    for j in range(blocks // 2, blocks):
        finish(j)

    def sent(ref, sem):
        remote(ref, ref, sem, sem, sp_peer(1)).wait_send()

    for copy in rim_copies + route_copies + far_rows:
        copy.wait_send()
    for sem in (y_send, f_send, c_send):
        sent(wg_in, sem)
    swapped.wait_send()
    sent(outgoing.at[:, others], d_send)
    sent(results.at[others, :], r_send)

    @pl.when(in_middle)
    def _():
        sent(relay_out.at[:, :, others], rd_send)
        sent(relay_sum, sum_send)
        sent(results.at[pl.ds(0, 2 * capacity), :], rb_send)
        sent(help_in, h_send)

    @pl.when(at_end)
    def _():
        sent(results.at[pl.ds(0, 4 * capacity), :], rb_send)
        sent(pass_in, q_send)


def shards(*args):
    (residual, conv_value, conv_gate, segments, conv_weight, norm_gain, norm_shift, out_weight,
     ffn_gain, routes, route_weights, w_gate, w_up, w_down) = args
    tok_dev, local = conv_value.shape
    width = residual.shape[1]
    experts_n, columns = lax.axis_size("sp"), lax.axis_size("tp")
    top_count = routes.shape[1]
    capacity = max(2, 2 * tok_dev * top_count // (columns * experts_n))
    if capacity % 32 or columns != 4 or tok_dev != columns * 128 or experts_n != 8:
        return plain_shards(*args)
    rows_own = tok_dev // columns
    lanes = DC // CONV_GROUPS
    slot_total = experts_n * capacity
    near_slots = slot_total // 2
    halves, fine = 2, width // 16
    widths = (fine, fine) + (2 * fine,) * 6 + (fine, fine)
    half, blocks = width // halves, len(widths)
    helped = 4 * (width // 32)
    bf16, f32 = jnp.bfloat16, jnp.float32
    vmem, dma = pltpu.VMEM, pltpu.SemaphoreType.DMA
    anywhere = pl.BlockSpec(memory_space=pl.ANY)
    operands = (
        residual, conv_value, conv_gate,
        segments.reshape(-1, lanes), conv_weight,
        norm_gain[None], norm_shift[None], out_weight, ffn_gain[None],
        routes.T, route_weights.T, w_gate[0], w_up[0], w_down[0],
    )
    return pl.pallas_call(
        functools.partial(layer_kernel, experts_n, columns, capacity, widths),
        out_shape=pltpu.VMEM((rows_own, width), bf16),
        in_specs=[anywhere] * len(operands),
        out_specs=pl.BlockSpec(memory_space=pltpu.VMEM),
        scratch_shapes=[vmem(operand.shape, operand.dtype) for operand in operands] + [
            vmem((3, width, local), bf16), vmem((3, width, local), bf16), vmem((3, local, width), bf16),
            vmem((2, RIM, local), bf16), vmem((tok_dev // lanes, lanes), jnp.int32),
            vmem((RIM + tok_dev, lanes), f32), vmem((RIM + tok_dev, local), f32),
            vmem((RIM + rows_own, local), f32), vmem((RIM + rows_own, lanes), f32),
            vmem((tok_dev, local), bf16), vmem((columns, rows_own, local), bf16),
            vmem((rows_own, width), f32), vmem((halves, rows_own, half), bf16),
            vmem((halves, near_slots, half), bf16), vmem((halves, slot_total, half), bf16),
            vmem((2, halves, rows_own, half), bf16), vmem((2, halves, near_slots, half), bf16),
            vmem((columns, slot_total, local), bf16), vmem((2, slot_total, local), f32),
            vmem((slot_total, 2 * fine), f32),
            vmem((slot_total, width), bf16), vmem((near_slots, width), bf16),
            vmem((2, near_slots, width), bf16), vmem((2, rows_own, width), bf16),
            vmem((rows_own, width), bf16), vmem((2, helped // 2, local), bf16), vmem((capacity, width), bf16),
            vmem((3, top_count, rows_own, near_slots), bf16), vmem((3, near_slots, rows_own), bf16),
            vmem((3, top_count, rows_own, rows_own), f32),
            vmem((2, top_count, tok_dev), routes.dtype), vmem((2, top_count, tok_dev), route_weights.dtype),
            dma((len(operands),)), dma, dma((7 + blocks,)), dma, dma((3,)),
            dma, dma((7 + blocks,)), dma((3,)), dma((3,)), dma, dma,
            dma((2,)), dma((2, 2)), dma((halves,)), dma((2, halves)),
            dma, dma, dma, dma,
            dma, dma((2, blocks)), dma, dma((blocks,)), dma, dma((blocks,)), dma, dma((2,)), dma, dma,
        ],
        compiler_params=pltpu.CompilerParams(
            collective_id=0, has_side_effects=True, vmem_limit_bytes=60 * 1024 * 1024
        ),
    )(*operands)


def solution(mesh):
    return jax.shard_map(
        shards,
        mesh=mesh,
        in_specs=(
            P(("sp", "tp"), None),
            P("sp", "tp"),
            P("sp", "tp"),
            P("sp"),
            P(None, "tp"),
            P("tp"),
            P("tp"),
            P(),
            P(),
            P("sp", None),
            P("sp", None),
            P("sp", None, "tp"),
            P("sp", None, "tp"),
            P("sp", "tp", None),
        ),
        out_specs=P(("sp", "tp"), None),
        check_vma=False,
    )
```

```python
import functools

import jax
import jax.numpy as jnp
from jax import lax
from jax.experimental import pallas as pl
from jax.experimental.pallas import tpu as pltpu
from jax.sharding import PartitionSpec as P

DC = 1024
CONV_GROUPS = 8
MESH = pl.DeviceIdType.MESH
RIM = 32


def passed_along(value, axis, steps):
    count = lax.axis_size(axis)
    initial, last = (max(0, -steps), min(count, count - steps))
    return lax.ppermute(value, axis, [(source, source + steps) for source in range(initial, last)])


def slot_numbers(block_routes, capacity, experts_n):
    route_pairs = block_routes.reshape(block_routes.shape[:-2] + (-1,))
    onehot = (route_pairs[..., None] == jnp.arange(experts_n, dtype=jnp.int32)).astype(jnp.int32)
    slot_rank = jnp.sum((jnp.cumsum(onehot, axis=-2) - onehot) * onehot, axis=-1)
    return (route_pairs * capacity + slot_rank).reshape(block_routes.shape)


def dispatch_matrix(slot_ids, slot_total):
    numbers = jnp.arange(slot_total, dtype=jnp.int32)[:, None, None]
    matches = jnp.any(numbers == slot_ids[..., None, :, :], axis=-1)
    return matches.astype(jnp.bfloat16)


def plain_shards(
    residual,
    conv_value,
    conv_gate,
    segments,
    conv_weight,
    norm_gain,
    norm_shift,
    out_weight,
    ffn_gain,
    routes,
    route_weights,
    w_gate,
    w_up,
    w_down,
):
    tok_dev, local_channels = conv_value.shape
    reach = conv_weight.shape[0] - 1
    whole_gate, whole_up = (
        lax.all_gather(w_gate[0], "tp", axis=1, tiled=True),
        lax.all_gather(w_up[0], "tp", axis=1, tiled=True),
    )
    whole_down = lax.all_gather(w_down[0], "tp", axis=0, tiled=True)
    gated = (conv_value.astype(jnp.float32) * jax.nn.sigmoid(conv_gate.astype(jnp.float32))).astype(
        jnp.bfloat16
    )
    rim_prev, seg_prev = passed_along(
        (gated[tok_dev - reach :], segments[tok_dev - reach :]), "sp", 1
    )
    extended = jnp.concatenate([rim_prev, gated], 0).astype(jnp.float32)
    seg_ext = jnp.concatenate([seg_prev, segments], 0)
    convolved = jnp.zeros((tok_dev, local_channels), jnp.float32)
    for offset in range(reach + 1):
        same_doc = (seg_ext[offset : offset + tok_dev] == segments)[:, None]
        convolved = convolved + jnp.where(
            same_doc, extended[offset : offset + tok_dev] * conv_weight[offset], 0.0
        )
    group_size = DC // CONV_GROUPS
    grouped = convolved.reshape(tok_dev, local_channels // group_size, group_size)
    group_mean = jnp.mean(grouped, axis=-1, keepdims=True)
    group_var = jnp.mean(jnp.square(grouped - group_mean), axis=-1, keepdims=True)
    scaled = ((grouped - group_mean) * lax.rsqrt(group_var + 1e-05)).reshape(
        tok_dev, local_channels
    ) * norm_gain + norm_shift
    conv_out = jax.nn.silu(scaled).astype(jnp.bfloat16)
    columns = lax.axis_size("tp")
    column = lax.axis_index("tp")
    rows_own = tok_dev // columns
    own_conv = lax.all_to_all(conv_out, "tp", split_axis=0, concat_axis=1, tiled=True)
    mixed = jnp.dot(own_conv, out_weight, preferred_element_type=jnp.float32)
    stream = residual.astype(jnp.float32) + lax.optimization_barrier(
        mixed.astype(jnp.bfloat16)
    ).astype(jnp.float32)
    normed = (
        stream * lax.rsqrt(jnp.mean(stream * stream, axis=-1, keepdims=True) + 1e-06) * ffn_gain
    ).astype(jnp.bfloat16)
    experts_n = lax.axis_size("sp")
    top_count = routes.shape[1]
    model_width = normed.shape[1]
    capacity = max(2, 2 * tok_dev * top_count // (columns * experts_n))
    slot_total = experts_n * capacity
    own_routes = lax.dynamic_slice_in_dim(routes, column * rows_own, rows_own, 0)
    own_weights = lax.dynamic_slice_in_dim(route_weights, column * rows_own, rows_own, 0)
    own_slots = slot_numbers(own_routes, capacity, experts_n)
    routing_table = dispatch_matrix(own_slots, slot_total)
    outgoing = jnp.dot(routing_table, normed, preferred_element_type=jnp.float32).astype(
        jnp.bfloat16
    )
    outgoing = outgoing.reshape(experts_n, capacity, model_width)
    arrived = lax.all_to_all(outgoing, "sp", split_axis=0, concat_axis=1, tiled=True).reshape(
        slot_total, model_width
    )
    gate_act = jnp.dot(arrived, whole_gate, preferred_element_type=jnp.float32)
    up_act = jnp.dot(arrived, whole_up, preferred_element_type=jnp.float32)
    hidden = (jax.nn.silu(gate_act) * up_act).astype(jnp.bfloat16)
    summed = jnp.dot(hidden, whole_down, preferred_element_type=jnp.float32)
    expert_out = summed.astype(jnp.bfloat16).reshape(experts_n, capacity, model_width)
    returned = lax.all_to_all(expert_out, "sp", split_axis=0, concat_axis=0, tiled=True).reshape(
        slot_total, model_width
    )
    combined = stream
    for member in range(top_count):
        chosen = jnp.take(returned, own_slots[:, member], axis=0).astype(jnp.float32)
        combined = combined + own_weights[:, member : member + 1] * chosen
    return combined.astype(jnp.bfloat16)


def flipped(index, mask):
    bit = 1
    while bit <= mask:
        if mask & bit:
            index = index + bit * (1 - 2 * ((index // bit) % 2))
        bit *= 2
    return index


def layer_kernel(
    experts_n, columns, capacity, widths,
    residual_hbm, value_hbm, gate_hbm, seg_hbm, conv_w_hbm, gain_hbm, shift_hbm, ow_hbm, ffn_hbm,
    routes_hbm, route_w_hbm, wg_hbm, wu_hbm, wd_hbm,
    out_ref,
    residual, value, gate, seg_ref, conv_w_ref, gain_ref, shift_ref, ow, ffn_ref, routes_ref, route_w_ref,
    wg, wu, wd, wg_in, wu_in, wd_in, rim, seg_in, seg_ext, ext, win, seg_win,
    conv_out, conv_in, stream, normed, outgoing, arrived, rows_in, relay_out, hidden, silu_gate, partial,
    results, returned, relay_in, relay_sum, far_in, help_in, pass_in, through_in, tables, picks, shares, routes_in, route_w_in,
    load_sem, y_send, y_recv, c_send, c_recv, f_send, f_recv, rim_send, rim_recv, x_send, x_recv,
    t_send, t_recv, far_send, far_recv, d_send, d_recv, e_recv, rd_send,
    rb_send, rb_recv, r_send, r_recv, sum_send, sum_recv, h_send, h_recv, p_recv, q_send, v_recv,
):
    me_s, me_t = lax.axis_index("sp"), lax.axis_index("tp")
    tok_dev, local = value.shape
    width = residual.shape[1]
    rows_own = tok_dev // columns
    taps = conv_w_ref.shape[0]
    halves = normed.shape[0]
    half = width // halves
    blocks = len(widths)
    bands = [pl.ds(sum(widths[:j]), widths[j]) for j in range(blocks)]
    near_n = experts_n // 2
    near_slots = near_n * capacity
    next_s = (me_s + 1) % experts_n
    tile = 512
    group = DC // CONV_GROUPS
    level = me_s // 2
    levels = experts_n // 2
    in_middle = jnp.logical_or(level == levels // 2 - 1, level == levels // 2)
    at_end = jnp.logical_not(in_middle)

    def tp_peer(mask):
        return (me_s, flipped(me_t, mask))

    def sp_peer(mask):
        return (flipped(me_s, mask), me_t)

    loads = [
        pltpu.make_async_copy(src, dst, load_sem.at[i])
        for i, (src, dst) in enumerate((
            (value_hbm, value), (gate_hbm, gate), (seg_hbm, seg_ref), (conv_w_hbm, conv_w_ref),
            (gain_hbm, gain_ref), (shift_hbm, shift_ref), (routes_hbm, routes_ref), (route_w_hbm, route_w_ref),
            (residual_hbm, residual), (ow_hbm, ow), (ffn_hbm, ffn_ref),
            (wg_hbm, wg), (wu_hbm, wu), (wd_hbm, wd),
        ))
    ]
    conv_loads, stream_loads = 8, 11
    barrier = pltpu.get_barrier_semaphore()
    peers = [tp_peer(mask) for mask in range(1, columns)]
    peers += [sp_peer(mask) for mask in range(1, experts_n)]
    peers.append((flipped(me_s, 2), flipped(me_t, 2)))
    for peer in peers:
        pl.semaphore_signal(barrier, inc=1, device_id=peer, device_id_type=MESH)
    for load in loads:
        load.start()
    for load in loads[:conv_loads]:
        load.wait()
    pl.semaphore_wait(barrier, len(peers))

    def remote(src, dst, send, recv, peer):
        return pltpu.make_async_remote_copy(
            src_ref=src, dst_ref=dst, send_sem=send, recv_sem=recv,
            device_id=peer, device_id_type=MESH,
        )

    last = pl.ds(tok_dev - RIM, RIM)
    rim_copies = [
        remote(ref, dst, rim_send.at[i], rim_recv.at[i], (next_s, me_t))
        for i, (ref, dst) in enumerate(
            ((value.at[last], rim.at[0]), (gate.at[last], rim.at[1]), (seg_ref, seg_in))
        )
    ]
    for copy in rim_copies:
        copy.start()

    def across_piece(i, own, into, rows, cols):
        return (
            remote(own.at[rows, cols], into.at[1, rows, cols], y_send, y_recv.at[i], tp_peer(2)),
            remote(into.at[1, rows, cols], into.at[2, rows, cols], f_send, f_recv.at[i], tp_peer(1)),
        )

    every, first_rows, second_rows = pl.ds(0, local), width // 8, width // 16
    helped = help_in.shape[0] * help_in.shape[1]
    pieces = [
        (wg_hbm, wg_in, pl.ds(0, first_rows), every),
        (wg_hbm, wg_in, pl.ds(first_rows, second_rows), every),
        (wg_hbm, wg_in, pl.ds(first_rows + second_rows, width - first_rows - second_rows), every),
        (wu_hbm, wu_in, pl.ds(0, width // 2), every),
        (wu_hbm, wu_in, pl.ds(width // 2, width // 4), every),
        (wu_hbm, wu_in, pl.ds(3 * width // 4, width // 4 - helped), every),
        (wu_hbm, wu_in, pl.ds(width - helped, helped), every),
    ]
    up_done = len(pieces)
    detour = up_done - 1
    pieces += [(wd_hbm, wd_in, every, bands[j]) for j in range(blocks)]
    across, forward = zip(*[across_piece(i, *piece) for i, piece in enumerate(pieces)])
    beside = [
        remote(own, into.at[0], c_send, c_recv.at[i], tp_peer(1))
        for i, (own, into) in enumerate(((wg_hbm, wg_in), (wu_hbm, wu_in), (wd_hbm, wd_in)))
    ]
    pl.when(at_end)(across[0].start)
    pl.when(in_middle)(across[1].start)
    parts = help_in.shape[0]

    def helper(k, back):
        rows = pl.ds(width - helped + k * (helped // parts), helped // parts)
        if back:
            return remote(help_in.at[k], wu_in.at[1, rows], h_send, y_recv.at[detour], sp_peer(2))
        return remote(
            wu_hbm.at[rows], help_in.at[k], y_send, h_recv.at[k], (flipped(me_s, 2), flipped(me_t, 2))
        )

    @pl.when(at_end)
    def _():
        for k in range(parts):
            helper(k, False).start()

    relay = jnp.where(in_middle, flipped(me_s, 6), flipped(me_s, 4))
    relay_slot = jnp.where(in_middle, 0, 1)
    route_copies = [
        remote(ref, dst.at[relay_slot], t_send.at[i], t_recv.at[relay_slot, i], (relay, me_t))
        for i, (ref, dst) in enumerate(((routes_ref, routes_in), (route_w_ref, route_w_in)))
    ]
    for copy in route_copies:
        copy.start()

    def gated_of(v, g):
        v, g = v.astype(jnp.float32), g.astype(jnp.float32)
        product = v * (1.0 / (1.0 + jnp.exp(-g)))
        return product.astype(jnp.bfloat16).astype(jnp.float32)

    def gate_rows(i, carry):
        row = pl.multiple_of(i * 64, 64)
        ext[pl.ds(row + RIM, 64), :] = gated_of(value[pl.ds(row, 64), :], gate[pl.ds(row, 64), :])
        return carry

    lax.fori_loop(0, tok_dev // 64, gate_rows, 0)
    lanes_n = seg_ref.shape[1]

    def column(row):
        return jnp.broadcast_to(row.astype(jnp.float32), (lanes_n, lanes_n)).T

    for i in range(seg_ref.shape[0]):
        seg_ext[RIM + i * lanes_n : RIM + (i + 1) * lanes_n, :] = column(seg_ref[i : i + 1, :])

    block = 64
    lead = RIM - (taps - 1)

    def conv_rows(row):
        win[...] = ext[pl.ds(row, RIM + rows_own), :]
        seg_win[...] = seg_ext[pl.ds(row, RIM + rows_own), :]
        for start in range(0, rows_own, block):
            own_seg = seg_win[start + RIM : start + RIM + block, :]
            sums = [jnp.zeros((block, group), jnp.float32) for _ in range(local // group)]
            for tap in range(taps):
                at = start + lead + tap
                same_doc = seg_win[at : at + block, :] == own_seg
                for g in range(local // group):
                    lanes = slice(g * group, (g + 1) * group)
                    term = win[at : at + block, lanes] * conv_w_ref[tap : tap + 1, lanes]
                    sums[g] = sums[g] + jnp.where(same_doc, term, 0.0)
            for g in range(local // group):
                lanes = slice(g * group, (g + 1) * group)
                mean = jnp.mean(sums[g], axis=-1, keepdims=True)
                centred = sums[g] - mean
                deviation = jnp.mean(centred * centred, axis=-1, keepdims=True)
                scaled = centred * lax.rsqrt(deviation + 1e-05) * gain_ref[:, lanes] + shift_ref[:, lanes]
                conv_out[pl.ds(row + start, block), lanes] = (scaled / (1.0 + jnp.exp(-scaled))).astype(jnp.bfloat16)

    low = me_t % 2
    masks = (3 - low, 2 + low, 1, 0)

    def conv_part(i):
        peer_row = pl.multiple_of((me_t ^ masks[i]) * rows_own, rows_own)
        conv_rows(peer_row)
        if i == 3:
            conv_in[0] = conv_out[pl.ds(peer_row, rows_own), :]
            return []
        copy = remote(
            conv_out.at[pl.ds(peer_row, rows_own)], conv_in.at[masks[i]], x_send, x_recv,
            (me_s, me_t ^ masks[i]),
        )
        copy.start()
        return [copy]

    conv_part(0)
    pl.when(at_end)(across[1].start)

    numbers = lax.broadcasted_iota(jnp.int32, (rows_own, lanes_n), 1).astype(jnp.float32)
    earlier = jnp.where(
        lax.broadcasted_iota(jnp.int32, (rows_own, rows_own), 0)
        > lax.broadcasted_iota(jnp.int32, (rows_own, rows_own), 1), 1.0, 0.0,
    ).astype(jnp.bfloat16)
    slot_places = lax.broadcasted_iota(jnp.int32, (rows_own, near_slots), 1)
    own_lanes = pl.ds(pl.multiple_of(me_t * rows_own, rows_own), rows_own)
    top_count = routes_ref.shape[0]

    def make_tables(which, route_row, weight_row):
        names = [column(route_row(m)) for m in range(top_count)]
        marks = [jnp.where(name == numbers, 1.0, 0.0) for name in names]
        counts = jnp.dot(earlier, sum(marks).astype(jnp.bfloat16), preferred_element_type=jnp.float32)
        total = jnp.zeros((rows_own, near_slots), jnp.float32)
        for m, mark in enumerate(marks):
            rank = jnp.sum(counts * mark, axis=-1, keepdims=True).astype(jnp.int32)
            slot = (names[m][:, 0:1].astype(jnp.int32) ^ me_s) * capacity + rank
            table = jnp.where(slot_places == slot, 1.0, 0.0)
            tables[which, m] = table.astype(jnp.bfloat16)
            total = total + table
            shares[which, m] = column(weight_row(m))
        picks[which] = total.T.astype(jnp.bfloat16)

    make_tables(
        0, lambda m: routes_ref[m : m + 1, own_lanes], lambda m: route_w_ref[m : m + 1, own_lanes]
    )

    for copy in rim_copies:
        copy.wait_recv()
    ext[pl.ds(0, RIM), :] = gated_of(rim[0], rim[1])
    before = column(seg_in[seg_ref.shape[0] - 1 : seg_ref.shape[0], :])[lanes_n - RIM :, :]
    seg_ext[0:RIM, :] = jnp.where(me_s == 0, -1.0, before)

    conv_part(1)
    for i in (0, *range(2, len(pieces))):
        if i == 0 or i == detour:
            pl.when(in_middle)(across[i].start)
        else:
            across[i].start()
    conv_part(2)
    for copy in beside:
        copy.start()
    conv_part(3)

    @pl.when(in_middle)
    def _():
        for slot in range(2):
            for i, ref in enumerate((routes_ref, route_w_ref)):
                dst = (routes_in, route_w_in)[i].at[slot]
                remote(ref, dst, t_send.at[i], t_recv.at[slot, i], (relay, me_t)).wait_recv()
            make_tables(
                1 + slot,
                lambda m: routes_in[slot, m : m + 1, own_lanes],
                lambda m: route_w_in[slot, m : m + 1, own_lanes],
            )

    @pl.when(in_middle)
    def _():
        for k in range(parts):
            helper(k, False).wait_recv()
            helper(k, True).start()

    def pass_first():
        for i in range(2):
            across[i].wait_recv()
            forward[i].start()

    pl.when(at_end)(pass_first)
    for load in loads[conv_loads:stream_loads]:
        load.wait()
    swapped = remote(conv_in.at[pl.ds(1, columns - 1)], conv_in.at[pl.ds(1, columns - 1)], x_send, x_recv, tp_peer(1))
    swapped.wait_recv()

    squares = jnp.zeros((rows_own, 1), jnp.float32)
    for col in range(0, width, tile):
        cols = slice(col, col + tile)
        mixed = jnp.zeros((rows_own, tile), jnp.float32)
        for mask in range(columns):
            w_rows = pl.ds(pl.multiple_of(flipped(me_t, mask) * local, local), local)
            mixed = mixed + jnp.dot(conv_in[mask], ow[w_rows, cols], preferred_element_type=jnp.float32)
        part = residual[:, cols].astype(jnp.float32) + mixed.astype(jnp.bfloat16).astype(jnp.float32)
        stream[:, cols] = part
        squares = squares + jnp.sum(part * part, axis=-1, keepdims=True)
    scale = lax.rsqrt(squares / width + 1e-06)
    far_rows = []
    for h in range(halves):
        cols = slice(h * half, (h + 1) * half)
        normed[h] = (stream[:, cols] * scale * ffn_ref[:, cols]).astype(jnp.bfloat16)
        far_rows.append(remote(
            normed.at[h], rows_in.at[relay_slot, h], far_send.at[h], far_recv.at[relay_slot, h], (relay, me_t)
        ))
        far_rows[h].start()

    def packet(mask):
        return pl.ds(mask * capacity, capacity)

    others = pl.ds(capacity, near_slots - capacity)
    for h in range(halves):
        for col in range(0, half, tile):
            cols = slice(col, col + tile)
            outgoing[h, :, cols] = jnp.dot(
                picks[0], normed[h, :, cols], preferred_element_type=jnp.float32
            ).astype(jnp.bfloat16)
        for mask in range(near_n - 1, 0, -1):
            remote(
                outgoing.at[h, packet(mask)], arrived.at[h, packet(mask)], d_send, d_recv, sp_peer(mask)
            ).start()
        arrived[h, 0:capacity, :] = outgoing[h, 0:capacity, :]

    relay_masks = ((6, 7, 4, 5), (4, 5, 6, 7))

    def relayed(slot, m, h):
        return remote(
            relay_out.at[slot, h, packet(m)], arrived.at[h, packet(relay_masks[slot][m])],
            rd_send, e_recv, sp_peer(m),
        )

    def relay_half(slot, h):
        @pl.when(in_middle)
        def _():
            remote(
                normed.at[h], rows_in.at[slot, h], far_send.at[h], far_recv.at[slot, h], (relay, me_t)
            ).wait_recv()
            for col in range(0, half, tile):
                cols = slice(col, col + tile)
                relay_out[slot, h, :, cols] = jnp.dot(
                    picks[1 + slot], rows_in[slot, h, :, cols], preferred_element_type=jnp.float32
                ).astype(jnp.bfloat16)
            for m in (2, 3, 1):
                relayed(slot, m, h).start()
            place = relay_masks[slot][0] * capacity
            arrived[h, place : place + capacity, :] = relay_out[slot, h, 0:capacity, :]

    def landed(rows, recv):
        remote(arrived.at[:, rows], arrived.at[:, rows], d_send, recv, sp_peer(1)).wait_recv()

    for h in range(halves):
        relay_half(1, h)

    for load in loads[stream_loads:]:
        load.wait()
    for copy in beside:
        copy.wait_recv()
    relay_half(0, 0)
    pl.when(in_middle)(pass_first)
    across[2].wait_recv()
    forward[2].start()

    def pass_detour():
        across[detour].wait_recv()
        forward[detour].start()

    pl.when(at_end)(pass_detour)

    for h in range(1, halves):
        relay_half(0, h)

    landed(others, d_recv)

    near, far = slice(0, near_slots), slice(near_slots, 2 * near_slots)

    def act(w, rows):
        return sum(
            jnp.dot(arrived[h, rows, :], w[h * half : (h + 1) * half, :], preferred_element_type=jnp.float32)
            for h in range(halves)
        )

    def silu(v):
        return v / (1.0 + jnp.exp(-v))

    def hidden_units(mask, rows):
        g = wg if mask == 0 else wg_in.at[mask - 1]
        u = wu if mask == 0 else wu_in.at[mask - 1]
        hidden[mask, rows, :] = (silu(act(g, rows)) * act(u, rows)).astype(jnp.bfloat16)

    hidden_units(0, near)
    hidden_units(1, near)

    across[3].wait_recv()
    forward[3].start()

    for i in range(3):
        forward[i].wait_recv()

    def gate_units(rows):
        for mask in (2, 3):
            silu_gate[mask - 2, rows, :] = silu(act(wg_in.at[mask - 1], rows))

    gate_units(near)

    @pl.when(in_middle)
    def _():
        landed(pl.ds(near_slots, 2 * capacity), e_recv)

    @pl.when(at_end)
    def _():
        landed(pl.ds(near_slots, 4 * capacity), e_recv)

    hidden_units(0, far)
    hidden_units(1, far)

    across[4].wait_recv()
    forward[4].start()

    gate_units(far)

    across[5].wait_recv()
    forward[5].start()
    pl.when(in_middle)(pass_detour)

    def finish_hidden(mask):
        for rows in (near, far):
            units = silu_gate[mask - 2, rows, :] * act(wu_in.at[mask - 1], rows)
            hidden[mask, rows, :] = units.astype(jnp.bfloat16)

    finish_hidden(2)

    for i in range(3, up_done):
        forward[i].wait_recv()

    across[up_done].wait_recv()
    forward[up_done].start()

    finish_hidden(3)

    def to_relay(mask, m, slot, j):
        return remote(
            results.at[packet(mask), bands[j]], relay_in.at[slot, packet(m), bands[j]],
            rb_send, rb_recv.at[slot, j], sp_peer(m),
        )

    from_middle = ((7, 1, 0), (5, 1, 1))
    from_end, by_partner = ((4, 2, 0), (6, 2, 1), (7, 3, 1)), (5, 3, 0)
    kept = ((6, 0), (4, 1))
    give_back = {
        (mask, j): remote(
            results.at[packet(mask), bands[j]], returned.at[packet(mask), bands[j]],
            r_send, r_recv.at[j], sp_peer(mask),
        )
        for j in range(blocks) for mask in range(1, near_n)
    }

    def pass_on(j):
        return remote(
            results.at[packet(3), bands[j]], pass_in.at[:, bands[j]], r_send, p_recv, sp_peer(1)
        )

    def passed(j):
        return remote(
            pass_in.at[:, bands[j]], returned.at[packet(3), bands[j]], q_send, r_recv.at[j], sp_peer(2)
        )

    def through(j):
        return remote(
            results.at[packet(by_partner[0]), bands[j]], through_in.at[:, bands[j]],
            rb_send, v_recv.at[j], sp_peer(1),
        )

    def pass_through(j):
        through(j).wait_recv()
        _, m, slot = by_partner
        remote(
            through_in.at[:, bands[j]], relay_in.at[slot, packet(m), bands[j]],
            q_send, rb_recv.at[slot, j], sp_peer(2),
        ).start()

    def band_results(j):
        cols, span = bands[j], slice(0, widths[j])
        if j:
            across[up_done + j].wait_recv()
            forward[up_done + j].start()

        def down(mask):
            w = wd[:, cols] if mask == 0 else wd_in[mask - 1, :, cols]
            return jnp.dot(hidden[mask], w, preferred_element_type=jnp.float32)

        partial[:, span] = down(0) + down(1) + down(2)
        forward[up_done + j].wait_recv()
        results[:, cols] = (partial[:, span] + down(3)).astype(jnp.bfloat16)

        @pl.when(in_middle)
        def _():
            for mask, m, slot in from_middle:
                to_relay(mask, m, slot, j).start()
            for mask, slot in kept:
                relay_in[slot, 0:capacity, cols] = results[mask * capacity : (mask + 1) * capacity, cols]

        @pl.when(at_end)
        def _():
            through(j).start()
            for mask, m, slot in from_end:
                to_relay(mask, m, slot, j).start()
            pass_on(j).start()
            give_back[1, j].start()

        returned[0:capacity, cols] = results[0:capacity, cols]

    def direct(j, masks):
        for mask in masks:
            give_back[mask, j].start()

    def summed_up(slot, j):
        return remote(
            relay_sum.at[slot, :, bands[j]], far_in.at[:, bands[j]], sum_send, sum_recv.at[j],
            sp_peer((6, 4)[slot]),
        )

    def weighed(which, packets):
        return sum(
            shares[which, m][:, 0:1] * jnp.dot(tables[which, m], packets, preferred_element_type=jnp.float32)
            for m in range(top_count)
        )

    def relay_band(j):
        @pl.when(in_middle)
        def _():
            for slot in range(2):
                remote(
                    relay_in.at[slot, others, bands[j]], relay_in.at[slot, others, bands[j]],
                    rb_send, rb_recv.at[slot, j], sp_peer(1),
                ).wait_recv()
                relay_sum[slot, :, bands[j]] = weighed(1 + slot, relay_in[slot, :, bands[j]]).astype(jnp.bfloat16)
                summed_up(slot, j).start()

    early, summed, ends = blocks // 2, 0, [sum(widths[: j + 1]) for j in range(blocks)]
    forwarded = 0
    for j in range(blocks):
        band_results(j)
        while ends[forwarded] + max(widths) <= ends[j]:
            pl.when(at_end)(functools.partial(pass_through, forwarded))
            forwarded += 1
        pl.when(in_middle)(functools.partial(direct, j, (3, 2)))
        if j < early:
            pl.when(at_end)(functools.partial(direct, j, (2,)))
        while ends[summed] + max(widths) <= ends[j]:
            relay_band(summed)
            summed += 1

    @pl.when(in_middle)
    def _():
        for j in range(blocks):
            direct(j, (1,))

    @pl.when(at_end)
    def _():
        for j in range(forwarded, blocks):
            pass_through(j)
        for j in range(early, blocks):
            direct(j, (2,))
        remote(pass_in, pass_in, r_send, p_recv, sp_peer(1)).wait_recv()
        for j in range(blocks):
            passed(j).start()

    for j in range(summed, blocks):
        relay_band(j)

    def finish(j):
        cols = bands[j]
        remote(
            relay_sum.at[0, :, cols], far_in.at[:, cols], sum_send, sum_recv.at[j], (relay, me_t)
        ).wait_recv()
        remote(
            returned.at[others, cols], returned.at[others, cols], r_send, r_recv.at[j], sp_peer(1)
        ).wait_recv()
        total = stream[:, cols] + weighed(0, returned[:, cols]) + far_in[:, cols].astype(jnp.float32)
        out_ref[:, cols] = total.astype(jnp.bfloat16)

    for j in range(blocks // 2):
        finish(j)
    for j in range(blocks // 2, blocks):
        finish(j)

    def sent(ref, sem):
        remote(ref, ref, sem, sem, sp_peer(1)).wait_send()

    for copy in rim_copies + route_copies + far_rows:
        copy.wait_send()
    for sem in (y_send, f_send, c_send):
        sent(wg_in, sem)
    swapped.wait_send()
    sent(outgoing.at[:, others], d_send)
    sent(results.at[others, :], r_send)

    @pl.when(in_middle)
    def _():
        sent(relay_out.at[:, :, others], rd_send)
        sent(relay_sum, sum_send)
        sent(results.at[pl.ds(0, 2 * capacity), :], rb_send)
        sent(help_in, h_send)

    @pl.when(at_end)
    def _():
        sent(results.at[pl.ds(0, 4 * capacity), :], rb_send)
        sent(results.at[pl.ds(0, 2 * capacity), :], q_send)


def shards(*args):
    (residual, conv_value, conv_gate, segments, conv_weight, norm_gain, norm_shift, out_weight,
     ffn_gain, routes, route_weights, w_gate, w_up, w_down) = args
    tok_dev, local = conv_value.shape
    width = residual.shape[1]
    experts_n, columns = lax.axis_size("sp"), lax.axis_size("tp")
    top_count = routes.shape[1]
    capacity = max(2, 2 * tok_dev * top_count // (columns * experts_n))
    if capacity % 32 or columns != 4 or tok_dev != columns * 128 or experts_n != 8:
        return plain_shards(*args)
    rows_own = tok_dev // columns
    lanes = DC // CONV_GROUPS
    slot_total = experts_n * capacity
    near_slots = slot_total // 2
    halves, fine = 2, width // 16
    widths = (fine, fine) + (2 * fine,) * 6 + (fine, fine)
    half, blocks = width // halves, len(widths)
    helped = 4 * (width // 32)
    bf16, f32 = jnp.bfloat16, jnp.float32
    vmem, dma = pltpu.VMEM, pltpu.SemaphoreType.DMA
    anywhere = pl.BlockSpec(memory_space=pl.ANY)
    operands = (
        residual, conv_value, conv_gate,
        segments.reshape(-1, lanes), conv_weight,
        norm_gain[None], norm_shift[None], out_weight, ffn_gain[None],
        routes.T, route_weights.T, w_gate[0], w_up[0], w_down[0],
    )
    return pl.pallas_call(
        functools.partial(layer_kernel, experts_n, columns, capacity, widths),
        out_shape=pltpu.VMEM((rows_own, width), bf16),
        in_specs=[anywhere] * len(operands),
        out_specs=pl.BlockSpec(memory_space=pltpu.VMEM),
        scratch_shapes=[vmem(operand.shape, operand.dtype) for operand in operands] + [
            vmem((3, width, local), bf16), vmem((3, width, local), bf16), vmem((3, local, width), bf16),
            vmem((2, RIM, local), bf16), vmem((tok_dev // lanes, lanes), jnp.int32),
            vmem((RIM + tok_dev, lanes), f32), vmem((RIM + tok_dev, local), f32),
            vmem((RIM + rows_own, local), f32), vmem((RIM + rows_own, lanes), f32),
            vmem((tok_dev, local), bf16), vmem((columns, rows_own, local), bf16),
            vmem((rows_own, width), f32), vmem((halves, rows_own, half), bf16),
            vmem((halves, near_slots, half), bf16), vmem((halves, slot_total, half), bf16),
            vmem((2, halves, rows_own, half), bf16), vmem((2, halves, near_slots, half), bf16),
            vmem((columns, slot_total, local), bf16), vmem((2, slot_total, local), f32),
            vmem((slot_total, 2 * fine), f32),
            vmem((slot_total, width), bf16), vmem((near_slots, width), bf16),
            vmem((2, near_slots, width), bf16), vmem((2, rows_own, width), bf16),
            vmem((rows_own, width), bf16), vmem((2, helped // 2, local), bf16), vmem((capacity, width), bf16),
            vmem((capacity, width), bf16),
            vmem((3, top_count, rows_own, near_slots), bf16), vmem((3, near_slots, rows_own), bf16),
            vmem((3, top_count, rows_own, rows_own), f32),
            vmem((2, top_count, tok_dev), routes.dtype), vmem((2, top_count, tok_dev), route_weights.dtype),
            dma((len(operands),)), dma, dma((7 + blocks,)), dma, dma((3,)),
            dma, dma((7 + blocks,)), dma((3,)), dma((3,)), dma, dma,
            dma((2,)), dma((2, 2)), dma((halves,)), dma((2, halves)),
            dma, dma, dma, dma,
            dma, dma((2, blocks)), dma, dma((blocks,)), dma, dma((blocks,)), dma, dma((2,)), dma, dma, dma((blocks,)),
        ],
        compiler_params=pltpu.CompilerParams(
            collective_id=0, has_side_effects=True, vmem_limit_bytes=60 * 1024 * 1024
        ),
    )(*operands)


def solution(mesh):
    return jax.shard_map(
        shards,
        mesh=mesh,
        in_specs=(
            P(("sp", "tp"), None),
            P("sp", "tp"),
            P("sp", "tp"),
            P("sp"),
            P(None, "tp"),
            P("tp"),
            P("tp"),
            P(),
            P(),
            P("sp", None),
            P("sp", None),
            P("sp", None, "tp"),
            P("sp", None, "tp"),
            P("sp", "tp", None),
        ),
        out_specs=P(("sp", "tp"), None),
        check_vma=False,
    )
```

```python
import functools

import jax
import jax.numpy as jnp
from jax import lax
from jax.experimental import pallas as pl
from jax.experimental.pallas import tpu as pltpu
from jax.sharding import PartitionSpec as P

DC = 1024
CONV_GROUPS = 8
MESH = pl.DeviceIdType.MESH
RIM = 32


def passed_along(value, axis, steps):
    count = lax.axis_size(axis)
    initial, last = (max(0, -steps), min(count, count - steps))
    return lax.ppermute(value, axis, [(source, source + steps) for source in range(initial, last)])


def slot_numbers(block_routes, capacity, experts_n):
    route_pairs = block_routes.reshape(block_routes.shape[:-2] + (-1,))
    onehot = (route_pairs[..., None] == jnp.arange(experts_n, dtype=jnp.int32)).astype(jnp.int32)
    slot_rank = jnp.sum((jnp.cumsum(onehot, axis=-2) - onehot) * onehot, axis=-1)
    return (route_pairs * capacity + slot_rank).reshape(block_routes.shape)


def dispatch_matrix(slot_ids, slot_total):
    numbers = jnp.arange(slot_total, dtype=jnp.int32)[:, None, None]
    matches = jnp.any(numbers == slot_ids[..., None, :, :], axis=-1)
    return matches.astype(jnp.bfloat16)


def plain_shards(
    residual,
    conv_value,
    conv_gate,
    segments,
    conv_weight,
    norm_gain,
    norm_shift,
    out_weight,
    ffn_gain,
    routes,
    route_weights,
    w_gate,
    w_up,
    w_down,
):
    tok_dev, local_channels = conv_value.shape
    reach = conv_weight.shape[0] - 1
    whole_gate, whole_up = (
        lax.all_gather(w_gate[0], "tp", axis=1, tiled=True),
        lax.all_gather(w_up[0], "tp", axis=1, tiled=True),
    )
    whole_down = lax.all_gather(w_down[0], "tp", axis=0, tiled=True)
    gated = (conv_value.astype(jnp.float32) * jax.nn.sigmoid(conv_gate.astype(jnp.float32))).astype(
        jnp.bfloat16
    )
    rim_prev, seg_prev = passed_along(
        (gated[tok_dev - reach :], segments[tok_dev - reach :]), "sp", 1
    )
    extended = jnp.concatenate([rim_prev, gated], 0).astype(jnp.float32)
    seg_ext = jnp.concatenate([seg_prev, segments], 0)
    convolved = jnp.zeros((tok_dev, local_channels), jnp.float32)
    for offset in range(reach + 1):
        same_doc = (seg_ext[offset : offset + tok_dev] == segments)[:, None]
        convolved = convolved + jnp.where(
            same_doc, extended[offset : offset + tok_dev] * conv_weight[offset], 0.0
        )
    group_size = DC // CONV_GROUPS
    grouped = convolved.reshape(tok_dev, local_channels // group_size, group_size)
    group_mean = jnp.mean(grouped, axis=-1, keepdims=True)
    group_var = jnp.mean(jnp.square(grouped - group_mean), axis=-1, keepdims=True)
    scaled = ((grouped - group_mean) * lax.rsqrt(group_var + 1e-05)).reshape(
        tok_dev, local_channels
    ) * norm_gain + norm_shift
    conv_out = jax.nn.silu(scaled).astype(jnp.bfloat16)
    columns = lax.axis_size("tp")
    column = lax.axis_index("tp")
    rows_own = tok_dev // columns
    own_conv = lax.all_to_all(conv_out, "tp", split_axis=0, concat_axis=1, tiled=True)
    mixed = jnp.dot(own_conv, out_weight, preferred_element_type=jnp.float32)
    stream = residual.astype(jnp.float32) + lax.optimization_barrier(
        mixed.astype(jnp.bfloat16)
    ).astype(jnp.float32)
    normed = (
        stream * lax.rsqrt(jnp.mean(stream * stream, axis=-1, keepdims=True) + 1e-06) * ffn_gain
    ).astype(jnp.bfloat16)
    experts_n = lax.axis_size("sp")
    top_count = routes.shape[1]
    model_width = normed.shape[1]
    capacity = max(2, 2 * tok_dev * top_count // (columns * experts_n))
    slot_total = experts_n * capacity
    own_routes = lax.dynamic_slice_in_dim(routes, column * rows_own, rows_own, 0)
    own_weights = lax.dynamic_slice_in_dim(route_weights, column * rows_own, rows_own, 0)
    own_slots = slot_numbers(own_routes, capacity, experts_n)
    routing_table = dispatch_matrix(own_slots, slot_total)
    outgoing = jnp.dot(routing_table, normed, preferred_element_type=jnp.float32).astype(
        jnp.bfloat16
    )
    outgoing = outgoing.reshape(experts_n, capacity, model_width)
    arrived = lax.all_to_all(outgoing, "sp", split_axis=0, concat_axis=1, tiled=True).reshape(
        slot_total, model_width
    )
    gate_act = jnp.dot(arrived, whole_gate, preferred_element_type=jnp.float32)
    up_act = jnp.dot(arrived, whole_up, preferred_element_type=jnp.float32)
    hidden = (jax.nn.silu(gate_act) * up_act).astype(jnp.bfloat16)
    summed = jnp.dot(hidden, whole_down, preferred_element_type=jnp.float32)
    expert_out = summed.astype(jnp.bfloat16).reshape(experts_n, capacity, model_width)
    returned = lax.all_to_all(expert_out, "sp", split_axis=0, concat_axis=0, tiled=True).reshape(
        slot_total, model_width
    )
    combined = stream
    for member in range(top_count):
        chosen = jnp.take(returned, own_slots[:, member], axis=0).astype(jnp.float32)
        combined = combined + own_weights[:, member : member + 1] * chosen
    return combined.astype(jnp.bfloat16)


def flipped(index, mask):
    bit = 1
    while bit <= mask:
        if mask & bit:
            index = index + bit * (1 - 2 * ((index // bit) % 2))
        bit *= 2
    return index


def layer_kernel(
    experts_n, columns, capacity, widths,
    residual_hbm, value_hbm, gate_hbm, seg_hbm, conv_w_hbm, gain_hbm, shift_hbm, ow_hbm, ffn_hbm,
    routes_hbm, route_w_hbm, wg_hbm, wu_hbm, wd_hbm,
    out_ref,
    residual, value, gate, seg_ref, conv_w_ref, gain_ref, shift_ref, ow, ffn_ref, routes_ref, route_w_ref,
    wg, wu, wd, wg_in, wu_in, wd_in, rim, seg_in, seg_ext, ext, win, seg_win,
    conv_out, conv_in, stream, normed, outgoing, arrived, rows_in, relay_out, hidden, silu_gate, partial,
    results, returned, relay_in, relay_sum, far_in, help_in, pass_in, through_in, tables, picks, shares, routes_in, route_w_in,
    load_sem, y_send, y_recv, c_send, c_recv, f_send, f_recv, rim_send, rim_recv, x_send, x_recv,
    t_send, t_recv, far_send, far_recv, d_send, d_recv, e_recv, rd_send,
    rb_send, rb_recv, r_send, r_recv, sum_send, sum_recv, h_send, h_recv, p_recv, q_send, v_recv,
):
    me_s, me_t = lax.axis_index("sp"), lax.axis_index("tp")
    tok_dev, local = value.shape
    width = residual.shape[1]
    rows_own = tok_dev // columns
    taps = conv_w_ref.shape[0]
    halves = normed.shape[0]
    half = width // halves
    blocks = len(widths)
    bands = [pl.ds(sum(widths[:j]), widths[j]) for j in range(blocks)]
    near_n = experts_n // 2
    near_slots = near_n * capacity
    next_s = (me_s + 1) % experts_n
    tile = 512
    group = DC // CONV_GROUPS
    level = me_s // 2
    levels = experts_n // 2
    in_middle = jnp.logical_or(level == levels // 2 - 1, level == levels // 2)
    at_end = jnp.logical_not(in_middle)

    def tp_peer(mask):
        return (me_s, flipped(me_t, mask))

    def sp_peer(mask):
        return (flipped(me_s, mask), me_t)

    loads = [
        pltpu.make_async_copy(src, dst, load_sem.at[i])
        for i, (src, dst) in enumerate((
            (value_hbm, value), (gate_hbm, gate), (seg_hbm, seg_ref), (conv_w_hbm, conv_w_ref),
            (gain_hbm, gain_ref), (shift_hbm, shift_ref), (routes_hbm, routes_ref), (route_w_hbm, route_w_ref),
            (residual_hbm, residual), (ow_hbm, ow), (ffn_hbm, ffn_ref),
            (wg_hbm, wg), (wu_hbm, wu), (wd_hbm, wd),
        ))
    ]
    conv_loads, stream_loads = 8, 11
    barrier = pltpu.get_barrier_semaphore()
    peers = [tp_peer(mask) for mask in range(1, columns)]
    peers += [sp_peer(mask) for mask in range(1, experts_n)]
    peers.append((flipped(me_s, 2), flipped(me_t, 2)))
    for peer in peers:
        pl.semaphore_signal(barrier, inc=1, device_id=peer, device_id_type=MESH)
    for load in loads:
        load.start()
    for load in loads[:conv_loads]:
        load.wait()
    pl.semaphore_wait(barrier, len(peers))

    def remote(src, dst, send, recv, peer):
        return pltpu.make_async_remote_copy(
            src_ref=src, dst_ref=dst, send_sem=send, recv_sem=recv,
            device_id=peer, device_id_type=MESH,
        )

    last = pl.ds(tok_dev - RIM, RIM)
    rim_copies = [
        remote(ref, dst, rim_send.at[i], rim_recv.at[i], (next_s, me_t))
        for i, (ref, dst) in enumerate(
            ((value.at[last], rim.at[0]), (gate.at[last], rim.at[1]), (seg_ref, seg_in))
        )
    ]
    for copy in rim_copies:
        copy.start()

    def across_piece(i, own, into, rows, cols):
        return (
            remote(own.at[rows, cols], into.at[1, rows, cols], y_send, y_recv.at[i], tp_peer(2)),
            remote(into.at[1, rows, cols], into.at[2, rows, cols], f_send, f_recv.at[i], tp_peer(1)),
        )

    every, first_rows, second_rows = pl.ds(0, local), width // 8, width // 16
    helped = help_in.shape[0] * help_in.shape[1]
    pieces = [
        (wg_hbm, wg_in, pl.ds(0, first_rows), every),
        (wg_hbm, wg_in, pl.ds(first_rows, second_rows), every),
        (wg_hbm, wg_in, pl.ds(first_rows + second_rows, width - first_rows - second_rows), every),
        (wu_hbm, wu_in, pl.ds(0, width // 2), every),
        (wu_hbm, wu_in, pl.ds(width // 2, width // 4), every),
        (wu_hbm, wu_in, pl.ds(3 * width // 4, width // 4 - helped), every),
        (wu_hbm, wu_in, pl.ds(width - helped, helped), every),
    ]
    up_done = len(pieces)
    detour = up_done - 1
    pieces += [(wd_hbm, wd_in, every, bands[j]) for j in range(blocks)]
    across, forward = zip(*[across_piece(i, *piece) for i, piece in enumerate(pieces)])
    beside = [
        remote(own, into.at[0], c_send, c_recv.at[i], tp_peer(1))
        for i, (own, into) in enumerate(((wg_hbm, wg_in), (wu_hbm, wu_in), (wd_hbm, wd_in)))
    ]
    pl.when(at_end)(across[0].start)
    pl.when(in_middle)(across[1].start)
    parts = help_in.shape[0]

    def helper(k, back):
        rows = pl.ds(width - helped + k * (helped // parts), helped // parts)
        if back:
            return remote(help_in.at[k], wu_in.at[1, rows], h_send, y_recv.at[detour], sp_peer(2))
        return remote(
            wu_hbm.at[rows], help_in.at[k], y_send, h_recv.at[k], (flipped(me_s, 2), flipped(me_t, 2))
        )

    @pl.when(at_end)
    def _():
        for k in range(parts):
            helper(k, False).start()

    relay = jnp.where(in_middle, flipped(me_s, 6), flipped(me_s, 4))
    relay_slot = jnp.where(in_middle, 0, 1)
    route_copies = [
        remote(ref, dst.at[relay_slot], t_send.at[i], t_recv.at[relay_slot, i], (relay, me_t))
        for i, (ref, dst) in enumerate(((routes_ref, routes_in), (route_w_ref, route_w_in)))
    ]
    for copy in route_copies:
        copy.start()

    def gated_of(v, g):
        v, g = v.astype(jnp.float32), g.astype(jnp.float32)
        product = v * (1.0 / (1.0 + jnp.exp(-g)))
        return product.astype(jnp.bfloat16).astype(jnp.float32)

    def gate_rows(i, carry):
        row = pl.multiple_of(i * 64, 64)
        ext[pl.ds(row + RIM, 64), :] = gated_of(value[pl.ds(row, 64), :], gate[pl.ds(row, 64), :])
        return carry

    lax.fori_loop(0, tok_dev // 64, gate_rows, 0)
    lanes_n = seg_ref.shape[1]

    def column(row):
        return jnp.broadcast_to(row.astype(jnp.float32), (lanes_n, lanes_n)).T

    for i in range(seg_ref.shape[0]):
        seg_ext[RIM + i * lanes_n : RIM + (i + 1) * lanes_n, :] = column(seg_ref[i : i + 1, :])

    block = 64
    lead = RIM - (taps - 1)

    def conv_rows(row):
        win[...] = ext[pl.ds(row, RIM + rows_own), :]
        seg_win[...] = seg_ext[pl.ds(row, RIM + rows_own), :]
        for start in range(0, rows_own, block):
            own_seg = seg_win[start + RIM : start + RIM + block, :]
            sums = [jnp.zeros((block, group), jnp.float32) for _ in range(local // group)]
            for tap in range(taps):
                at = start + lead + tap
                same_doc = seg_win[at : at + block, :] == own_seg
                for g in range(local // group):
                    lanes = slice(g * group, (g + 1) * group)
                    term = win[at : at + block, lanes] * conv_w_ref[tap : tap + 1, lanes]
                    sums[g] = sums[g] + jnp.where(same_doc, term, 0.0)
            for g in range(local // group):
                lanes = slice(g * group, (g + 1) * group)
                mean = jnp.mean(sums[g], axis=-1, keepdims=True)
                centred = sums[g] - mean
                deviation = jnp.mean(centred * centred, axis=-1, keepdims=True)
                scaled = centred * lax.rsqrt(deviation + 1e-05) * gain_ref[:, lanes] + shift_ref[:, lanes]
                conv_out[pl.ds(row + start, block), lanes] = (scaled / (1.0 + jnp.exp(-scaled))).astype(jnp.bfloat16)

    low = me_t % 2
    masks = (3 - low, 2 + low, 1, 0)

    def conv_part(i):
        peer_row = pl.multiple_of((me_t ^ masks[i]) * rows_own, rows_own)
        conv_rows(peer_row)
        if i == 3:
            conv_in[0] = conv_out[pl.ds(peer_row, rows_own), :]
            return []
        copy = remote(
            conv_out.at[pl.ds(peer_row, rows_own)], conv_in.at[masks[i]], x_send, x_recv,
            (me_s, me_t ^ masks[i]),
        )
        copy.start()
        return [copy]

    conv_part(0)
    pl.when(at_end)(across[1].start)

    numbers = lax.broadcasted_iota(jnp.int32, (rows_own, lanes_n), 1).astype(jnp.float32)
    earlier = jnp.where(
        lax.broadcasted_iota(jnp.int32, (rows_own, rows_own), 0)
        > lax.broadcasted_iota(jnp.int32, (rows_own, rows_own), 1), 1.0, 0.0,
    ).astype(jnp.bfloat16)
    slot_places = lax.broadcasted_iota(jnp.int32, (rows_own, near_slots), 1)
    own_lanes = pl.ds(pl.multiple_of(me_t * rows_own, rows_own), rows_own)
    top_count = routes_ref.shape[0]

    def make_tables(which, route_row, weight_row):
        names = [column(route_row(m)) for m in range(top_count)]
        marks = [jnp.where(name == numbers, 1.0, 0.0) for name in names]
        counts = jnp.dot(earlier, sum(marks).astype(jnp.bfloat16), preferred_element_type=jnp.float32)
        total = jnp.zeros((rows_own, near_slots), jnp.float32)
        for m, mark in enumerate(marks):
            rank = jnp.sum(counts * mark, axis=-1, keepdims=True).astype(jnp.int32)
            slot = (names[m][:, 0:1].astype(jnp.int32) ^ me_s) * capacity + rank
            table = jnp.where(slot_places == slot, 1.0, 0.0)
            tables[which, m] = table.astype(jnp.bfloat16)
            total = total + table
            shares[which, m] = column(weight_row(m))
        picks[which] = total.T.astype(jnp.bfloat16)

    make_tables(
        0, lambda m: routes_ref[m : m + 1, own_lanes], lambda m: route_w_ref[m : m + 1, own_lanes]
    )

    for copy in rim_copies:
        copy.wait_recv()
    ext[pl.ds(0, RIM), :] = gated_of(rim[0], rim[1])
    before = column(seg_in[seg_ref.shape[0] - 1 : seg_ref.shape[0], :])[lanes_n - RIM :, :]
    seg_ext[0:RIM, :] = jnp.where(me_s == 0, -1.0, before)

    conv_part(1)
    for i in (0, *range(2, len(pieces))):
        if i == 0 or i == detour:
            pl.when(in_middle)(across[i].start)
        else:
            across[i].start()
    conv_part(2)
    for copy in beside:
        copy.start()
    conv_part(3)

    @pl.when(in_middle)
    def _():
        for slot in range(2):
            for i, ref in enumerate((routes_ref, route_w_ref)):
                dst = (routes_in, route_w_in)[i].at[slot]
                remote(ref, dst, t_send.at[i], t_recv.at[slot, i], (relay, me_t)).wait_recv()
            make_tables(
                1 + slot,
                lambda m: routes_in[slot, m : m + 1, own_lanes],
                lambda m: route_w_in[slot, m : m + 1, own_lanes],
            )

    @pl.when(in_middle)
    def _():
        for k in range(parts):
            helper(k, False).wait_recv()
            helper(k, True).start()

    def pass_first():
        for i in range(2):
            across[i].wait_recv()
            forward[i].start()

    pl.when(at_end)(pass_first)
    for load in loads[conv_loads:stream_loads]:
        load.wait()
    swapped = remote(conv_in.at[pl.ds(1, columns - 1)], conv_in.at[pl.ds(1, columns - 1)], x_send, x_recv, tp_peer(1))
    swapped.wait_recv()

    squares = jnp.zeros((rows_own, 1), jnp.float32)
    for col in range(0, width, tile):
        cols = slice(col, col + tile)
        mixed = jnp.zeros((rows_own, tile), jnp.float32)
        for mask in range(columns):
            w_rows = pl.ds(pl.multiple_of(flipped(me_t, mask) * local, local), local)
            mixed = mixed + jnp.dot(conv_in[mask], ow[w_rows, cols], preferred_element_type=jnp.float32)
        part = residual[:, cols].astype(jnp.float32) + mixed.astype(jnp.bfloat16).astype(jnp.float32)
        stream[:, cols] = part
        squares = squares + jnp.sum(part * part, axis=-1, keepdims=True)
    scale = lax.rsqrt(squares / width + 1e-06)
    far_rows = []
    for h in range(halves):
        cols = slice(h * half, (h + 1) * half)
        normed[h] = (stream[:, cols] * scale * ffn_ref[:, cols]).astype(jnp.bfloat16)
        far_rows.append(remote(
            normed.at[h], rows_in.at[relay_slot, h], far_send.at[h], far_recv.at[relay_slot, h], (relay, me_t)
        ))
        far_rows[h].start()

    def packet(mask):
        return pl.ds(mask * capacity, capacity)

    others = pl.ds(capacity, near_slots - capacity)
    for h in range(halves):
        for col in range(0, half, tile):
            cols = slice(col, col + tile)
            outgoing[h, :, cols] = jnp.dot(
                picks[0], normed[h, :, cols], preferred_element_type=jnp.float32
            ).astype(jnp.bfloat16)
        for mask in range(near_n - 1, 0, -1):
            remote(
                outgoing.at[h, packet(mask)], arrived.at[h, packet(mask)], d_send, d_recv, sp_peer(mask)
            ).start()
        arrived[h, 0:capacity, :] = outgoing[h, 0:capacity, :]

    relay_masks = ((6, 7, 4, 5), (4, 5, 6, 7))

    def relayed(slot, m, h):
        return remote(
            relay_out.at[slot, h, packet(m)], arrived.at[h, packet(relay_masks[slot][m])],
            rd_send, e_recv, sp_peer(m),
        )

    def relay_half(slot, h):
        @pl.when(in_middle)
        def _():
            remote(
                normed.at[h], rows_in.at[slot, h], far_send.at[h], far_recv.at[slot, h], (relay, me_t)
            ).wait_recv()
            for col in range(0, half, tile):
                cols = slice(col, col + tile)
                relay_out[slot, h, :, cols] = jnp.dot(
                    picks[1 + slot], rows_in[slot, h, :, cols], preferred_element_type=jnp.float32
                ).astype(jnp.bfloat16)
            for m in (2, 3, 1):
                relayed(slot, m, h).start()
            place = relay_masks[slot][0] * capacity
            arrived[h, place : place + capacity, :] = relay_out[slot, h, 0:capacity, :]

    def landed(rows, recv):
        remote(arrived.at[:, rows], arrived.at[:, rows], d_send, recv, sp_peer(1)).wait_recv()

    for h in range(halves):
        relay_half(1, h)

    for load in loads[stream_loads:]:
        load.wait()
    for copy in beside:
        copy.wait_recv()
    relay_half(0, 0)
    pl.when(in_middle)(pass_first)
    across[2].wait_recv()
    forward[2].start()

    def pass_detour():
        across[detour].wait_recv()
        forward[detour].start()

    pl.when(at_end)(pass_detour)

    for h in range(1, halves):
        relay_half(0, h)

    landed(others, d_recv)

    near, far = slice(0, near_slots), slice(near_slots, 2 * near_slots)

    def act(w, rows):
        return sum(
            jnp.dot(arrived[h, rows, :], w[h * half : (h + 1) * half, :], preferred_element_type=jnp.float32)
            for h in range(halves)
        )

    def silu(v):
        return v / (1.0 + jnp.exp(-v))

    def hidden_units(mask, rows):
        g = wg if mask == 0 else wg_in.at[mask - 1]
        u = wu if mask == 0 else wu_in.at[mask - 1]
        hidden[mask, rows, :] = (silu(act(g, rows)) * act(u, rows)).astype(jnp.bfloat16)

    hidden_units(0, near)
    hidden_units(1, near)

    across[3].wait_recv()
    forward[3].start()

    for i in range(3):
        forward[i].wait_recv()

    def gate_units(rows):
        for mask in (2, 3):
            silu_gate[mask - 2, rows, :] = silu(act(wg_in.at[mask - 1], rows))

    gate_units(near)

    @pl.when(in_middle)
    def _():
        landed(pl.ds(near_slots, 2 * capacity), e_recv)

    @pl.when(at_end)
    def _():
        landed(pl.ds(near_slots, 4 * capacity), e_recv)

    hidden_units(0, far)
    hidden_units(1, far)

    across[4].wait_recv()
    forward[4].start()

    gate_units(far)

    across[5].wait_recv()
    forward[5].start()
    pl.when(in_middle)(pass_detour)

    def finish_hidden(mask):
        for rows in (near, far):
            units = silu_gate[mask - 2, rows, :] * act(wu_in.at[mask - 1], rows)
            hidden[mask, rows, :] = units.astype(jnp.bfloat16)

    finish_hidden(2)

    for i in range(3, up_done):
        forward[i].wait_recv()

    across[up_done].wait_recv()
    forward[up_done].start()

    finish_hidden(3)

    def to_relay(mask, m, slot, j):
        return remote(
            results.at[packet(mask), bands[j]], relay_in.at[slot, packet(m), bands[j]],
            rb_send, rb_recv.at[slot, j], sp_peer(m),
        )

    from_middle = ((7, 1, 0), (5, 1, 1))
    from_end, by_partner = ((4, 2, 0), (6, 2, 1), (7, 3, 1)), (5, 3, 0)
    kept = ((6, 0), (4, 1))
    give_back = {
        (mask, j): remote(
            results.at[packet(mask), bands[j]], returned.at[packet(mask), bands[j]],
            r_send, r_recv.at[j], sp_peer(mask),
        )
        for j in range(blocks) for mask in range(1, near_n)
    }

    def pass_on(j):
        return remote(
            results.at[packet(3), bands[j]], pass_in.at[:, bands[j]], r_send, p_recv, sp_peer(1)
        )

    def passed(j):
        return remote(
            pass_in.at[:, bands[j]], returned.at[packet(3), bands[j]], q_send, r_recv.at[j], sp_peer(2)
        )

    def through(j):
        return remote(
            results.at[packet(by_partner[0]), bands[j]], through_in.at[:, bands[j]],
            rb_send, v_recv.at[j], sp_peer(1),
        )

    def pass_through(j):
        through(j).wait_recv()
        _, m, slot = by_partner
        remote(
            through_in.at[:, bands[j]], relay_in.at[slot, packet(m), bands[j]],
            q_send, rb_recv.at[slot, j], sp_peer(2),
        ).start()

    def band_results(j):
        cols, span = bands[j], slice(0, widths[j])
        if j:
            across[up_done + j].wait_recv()
            forward[up_done + j].start()

        def down(mask):
            w = wd[:, cols] if mask == 0 else wd_in[mask - 1, :, cols]
            return jnp.dot(hidden[mask], w, preferred_element_type=jnp.float32)

        partial[:, span] = down(0) + down(1) + down(2)
        forward[up_done + j].wait_recv()
        results[:, cols] = (partial[:, span] + down(3)).astype(jnp.bfloat16)

        @pl.when(in_middle)
        def _():
            for mask, m, slot in from_middle:
                to_relay(mask, m, slot, j).start()
            for mask, slot in kept:
                relay_in[slot, 0:capacity, cols] = results[mask * capacity : (mask + 1) * capacity, cols]

        @pl.when(at_end)
        def _():
            through(j).start()
            for mask, m, slot in from_end:
                to_relay(mask, m, slot, j).start()
            pass_on(j).start()
            give_back[1, j].start()

        returned[0:capacity, cols] = results[0:capacity, cols]

    def direct(j, masks):
        for mask in masks:
            give_back[mask, j].start()

    def summed_up(slot, j):
        return remote(
            relay_sum.at[slot, :, bands[j]], far_in.at[:, bands[j]], sum_send, sum_recv.at[j],
            sp_peer((6, 4)[slot]),
        )

    def weighed(which, packets):
        return sum(
            shares[which, m][:, 0:1] * jnp.dot(tables[which, m], packets, preferred_element_type=jnp.float32)
            for m in range(top_count)
        )

    def relay_band(j):
        @pl.when(in_middle)
        def _():
            for slot in (1, 0):
                remote(
                    relay_in.at[slot, others, bands[j]], relay_in.at[slot, others, bands[j]],
                    rb_send, rb_recv.at[slot, j], sp_peer(1),
                ).wait_recv()
                relay_sum[slot, :, bands[j]] = weighed(1 + slot, relay_in[slot, :, bands[j]]).astype(jnp.bfloat16)
                summed_up(slot, j).start()

    early, summed, ends = blocks // 2, 0, [sum(widths[: j + 1]) for j in range(blocks)]
    forwarded = 0
    for j in range(blocks):
        band_results(j)
        while ends[forwarded] + max(widths) <= ends[j]:
            pl.when(at_end)(functools.partial(pass_through, forwarded))
            forwarded += 1
        pl.when(in_middle)(functools.partial(direct, j, (3, 2)))
        if j >= 3:
            pl.when(in_middle)(functools.partial(direct, j - 3, (1,)))
        if j < early:
            pl.when(at_end)(functools.partial(direct, j, (2,)))
        while ends[summed] + max(widths) <= ends[j]:
            relay_band(summed)
            summed += 1

    @pl.when(in_middle)
    def _():
        for j in range(blocks - 3, blocks):
            direct(j, (1,))

    @pl.when(at_end)
    def _():
        for j in range(forwarded, blocks):
            pass_through(j)
        for j in range(early, blocks):
            direct(j, (2,))
        remote(pass_in, pass_in, r_send, p_recv, sp_peer(1)).wait_recv()
        for j in range(blocks):
            passed(j).start()

    for j in range(summed, blocks):
        relay_band(j)

    def finish(j):
        cols = bands[j]
        remote(
            relay_sum.at[0, :, cols], far_in.at[:, cols], sum_send, sum_recv.at[j], (relay, me_t)
        ).wait_recv()
        remote(
            returned.at[others, cols], returned.at[others, cols], r_send, r_recv.at[j], sp_peer(1)
        ).wait_recv()
        total = stream[:, cols] + weighed(0, returned[:, cols]) + far_in[:, cols].astype(jnp.float32)
        out_ref[:, cols] = total.astype(jnp.bfloat16)

    for j in range(blocks // 2):
        finish(j)
    for j in range(blocks // 2, blocks):
        finish(j)

    def sent(ref, sem):
        remote(ref, ref, sem, sem, sp_peer(1)).wait_send()

    for copy in rim_copies + route_copies + far_rows:
        copy.wait_send()
    for sem in (y_send, f_send, c_send):
        sent(wg_in, sem)
    swapped.wait_send()
    sent(outgoing.at[:, others], d_send)
    sent(results.at[others, :], r_send)

    @pl.when(in_middle)
    def _():
        sent(relay_out.at[:, :, others], rd_send)
        sent(relay_sum, sum_send)
        sent(results.at[pl.ds(0, 2 * capacity), :], rb_send)
        sent(help_in, h_send)

    @pl.when(at_end)
    def _():
        sent(results.at[pl.ds(0, 4 * capacity), :], rb_send)
        sent(results.at[pl.ds(0, 2 * capacity), :], q_send)


def shards(*args):
    (residual, conv_value, conv_gate, segments, conv_weight, norm_gain, norm_shift, out_weight,
     ffn_gain, routes, route_weights, w_gate, w_up, w_down) = args
    tok_dev, local = conv_value.shape
    width = residual.shape[1]
    experts_n, columns = lax.axis_size("sp"), lax.axis_size("tp")
    top_count = routes.shape[1]
    capacity = max(2, 2 * tok_dev * top_count // (columns * experts_n))
    if capacity % 32 or columns != 4 or tok_dev != columns * 128 or experts_n != 8:
        return plain_shards(*args)
    rows_own = tok_dev // columns
    lanes = DC // CONV_GROUPS
    slot_total = experts_n * capacity
    near_slots = slot_total // 2
    halves, fine = 2, width // 16
    widths = (fine, fine) + (2 * fine,) * 6 + (fine, fine)
    half, blocks = width // halves, len(widths)
    helped = 4 * (width // 32)
    bf16, f32 = jnp.bfloat16, jnp.float32
    vmem, dma = pltpu.VMEM, pltpu.SemaphoreType.DMA
    anywhere = pl.BlockSpec(memory_space=pl.ANY)
    operands = (
        residual, conv_value, conv_gate,
        segments.reshape(-1, lanes), conv_weight,
        norm_gain[None], norm_shift[None], out_weight, ffn_gain[None],
        routes.T, route_weights.T, w_gate[0], w_up[0], w_down[0],
    )
    return pl.pallas_call(
        functools.partial(layer_kernel, experts_n, columns, capacity, widths),
        out_shape=pltpu.VMEM((rows_own, width), bf16),
        in_specs=[anywhere] * len(operands),
        out_specs=pl.BlockSpec(memory_space=pltpu.VMEM),
        scratch_shapes=[vmem(operand.shape, operand.dtype) for operand in operands] + [
            vmem((3, width, local), bf16), vmem((3, width, local), bf16), vmem((3, local, width), bf16),
            vmem((2, RIM, local), bf16), vmem((tok_dev // lanes, lanes), jnp.int32),
            vmem((RIM + tok_dev, lanes), f32), vmem((RIM + tok_dev, local), f32),
            vmem((RIM + rows_own, local), f32), vmem((RIM + rows_own, lanes), f32),
            vmem((tok_dev, local), bf16), vmem((columns, rows_own, local), bf16),
            vmem((rows_own, width), f32), vmem((halves, rows_own, half), bf16),
            vmem((halves, near_slots, half), bf16), vmem((halves, slot_total, half), bf16),
            vmem((2, halves, rows_own, half), bf16), vmem((2, halves, near_slots, half), bf16),
            vmem((columns, slot_total, local), bf16), vmem((2, slot_total, local), f32),
            vmem((slot_total, 2 * fine), f32),
            vmem((slot_total, width), bf16), vmem((near_slots, width), bf16),
            vmem((2, near_slots, width), bf16), vmem((2, rows_own, width), bf16),
            vmem((rows_own, width), bf16), vmem((2, helped // 2, local), bf16), vmem((capacity, width), bf16),
            vmem((capacity, width), bf16),
            vmem((3, top_count, rows_own, near_slots), bf16), vmem((3, near_slots, rows_own), bf16),
            vmem((3, top_count, rows_own, rows_own), f32),
            vmem((2, top_count, tok_dev), routes.dtype), vmem((2, top_count, tok_dev), route_weights.dtype),
            dma((len(operands),)), dma, dma((7 + blocks,)), dma, dma((3,)),
            dma, dma((7 + blocks,)), dma((3,)), dma((3,)), dma, dma,
            dma((2,)), dma((2, 2)), dma((halves,)), dma((2, halves)),
            dma, dma, dma, dma,
            dma, dma((2, blocks)), dma, dma((blocks,)), dma, dma((blocks,)), dma, dma((2,)), dma, dma, dma((blocks,)),
        ],
        compiler_params=pltpu.CompilerParams(
            collective_id=0, has_side_effects=True, vmem_limit_bytes=60 * 1024 * 1024
        ),
    )(*operands)


def solution(mesh):
    return jax.shard_map(
        shards,
        mesh=mesh,
        in_specs=(
            P(("sp", "tp"), None),
            P("sp", "tp"),
            P("sp", "tp"),
            P("sp"),
            P(None, "tp"),
            P("tp"),
            P("tp"),
            P(),
            P(),
            P("sp", None),
            P("sp", None),
            P("sp", None, "tp"),
            P("sp", None, "tp"),
            P("sp", "tp", None),
        ),
        out_specs=P(("sp", "tp"), None),
        check_vma=False,
    )
```
